32 devices in a mesh: sp: 4 (over z), tp: 4 (over y, x), dp: 2 (over core).
Axes of the slice: x: 2, y: 2, z: 4, core: 2. Of those that a mesh axis runs over, the one named last changes fastest.
Arguments:
- latent: bfloat16 [2048, 2048], P(('dp', 'sp', 'tp')), parts along dimension 0, may hold values from -6 to 6
- context: bfloat16 [512, 2048], P(('dp', 'sp')), parts along dimension 0, may hold values from -6 to 6
- cond: bfloat16 [4096], P(('dp', 'sp')), parts along dimension 0, may hold values from -6 to 6
- context_cond: bfloat16 [2048], P('sp'), may hold values from -6 to 6
- norm_gain: float32 [2048], replicated, may hold values from 0.1 to 1.9
- mod_shift: bfloat16 [2048, 2048], P('sp', 'tp'), may hold values from -0.125 to 0.125
- mod_scale: bfloat16 [2048, 2048], P('sp', 'tp'), may hold values from -0.125 to 0.125
- mod_gate: bfloat16 [2048, 2048], P('sp', 'tp'), may hold values from -0.125 to 0.125
- w_query: bfloat16 [2048, 1024], P(None, 'tp'), may hold values from -0.125 to 0.125
- w_key: bfloat16 [2048, 1024], P(None, 'tp'), may hold values from -0.125 to 0.125
- w_value: bfloat16 [2048, 1024], P(None, 'tp'), may hold values from -0.125 to 0.125
- query_gain: float32 [64], replicated, may hold values from 1.4 to 2.2
- key_gain: float32 [64], replicated, may hold values from 0.1 to 1.9
- mix_lambda: float32 [8], P('tp'), may hold values from 0.3 to 0.8
- context_lift: float32 [8], P('tp'), may hold values from 1.5 to 2.5
- value_gain: float32 [128], replicated, may hold values from 0.1 to 1.9
- w_out: bfloat16 [1024, 2048], P('tp'), may hold values from -0.1875 to 0.1875
Outputs:
- output: bfloat16 [2048, 2048], P(('dp', 'sp', 'tp')), parts along dimension 0
The draws below stay inside these ranges and needn't reach their ends.
There are 2 independent parts, one for each index of `dp`. The reference program is written for one: setup_inputs(seed, part) draws one part's arguments, and reference() takes and returns one part's arrays. A program takes and returns all parts, laid end to end along the dimension named above; an argument that names none is the same for every part. Nothing has to cross between parts.
All inputs are finite; a program needn't handle non-finite values.
Results may differ from the reference program's by a relative error of at most 0.006.
Values may be sent and summed in bfloat16 or wider, within the bound.
A program may use at most 64 MiB of HBM per device.

```python
import jax
import jax.numpy as jnp
from jax import lax

D = 2048
HEADS = 8
HEAD_DIM = 64
VALUE_DIM = 128
GRID = 64
CTX = 256
LENGTH = 1024


def levels(key, shape, split, low, largest):
    loudness, own = 1.0, jax.random.fold_in(key, 6)
    for dim, parts in split:
        steps = jnp.exp(jax.random.uniform(jax.random.fold_in(own, dim), (parts,), jnp.float32, low / len(split), largest / len(split)))
        loudness = loudness * jnp.repeat(steps, shape[dim] // parts).reshape([-1 if axis == dim else 1 for axis in range(len(shape))])
    return loudness


def noise(stream_key, extent, width, limit, cuts=(), kind=jnp.bfloat16):
    array = jax.random.normal(stream_key, extent, jnp.float32) * width
    if len(cuts) > 0:
        array = levels(stream_key, extent, cuts, -0.22, 0.18) * array
    return jnp.clip(array, min=-limit, max=limit).astype(kind)


def setup_inputs(seed: int = 0, part: int = 0) -> dict:
    seeds = jax.random.split(jax.random.key(seed), 18)
    part_keys = jax.random.split(jax.random.fold_in(seeds[17], part), 18)
    return {
        "latent": noise(part_keys[0], (LENGTH, D), 1.0, 6.0, ((0, 16),)),
        "context": noise(part_keys[1], (CTX, D), 1.0, 6.0, ((0, 4),)),
        "cond": noise(part_keys[2], (D,), 1.0, 6.0, ((0, 4),)),
        "context_cond": noise(seeds[3], (D,), 1.0, 6.0, ((0, 4),)),
        "norm_gain": jnp.clip(1.0 + 0.18 * jax.random.normal(seeds[4], (D,), jnp.float32), 0.1, 1.9),
        "mod_shift": noise(seeds[5], (D, D), D ** -0.5, 0.125, ((0, 4), (1, 4))),
        "mod_scale": noise(seeds[6], (D, D), D ** -0.5, 0.125, ((0, 4), (1, 4))),
        "mod_gate": noise(seeds[7], (D, D), D ** -0.5, 0.125, ((0, 4), (1, 4))),
        "w_query": noise(seeds[8], (D, 2 * HEADS * HEAD_DIM), D ** -0.5, 0.125, ((1, 4),)),
        "w_key": noise(seeds[9], (D, 2 * HEADS * HEAD_DIM), D ** -0.5, 0.125, ((1, 4),)),
        "w_value": noise(seeds[10], (D, HEADS * VALUE_DIM), D ** -0.5, 0.125, ((1, 4),)),
        "query_gain": jnp.clip(jax.random.uniform(seeds[11], (HEAD_DIM,), jnp.float32, 1.4, 2.2), 1.4, 2.2),
        "key_gain": jnp.clip(1.0 + 0.18 * jax.random.normal(seeds[12], (HEAD_DIM,), jnp.float32), 0.1, 1.9),
        "mix_lambda": jnp.clip(0.3 + 0.5 * jax.random.uniform(seeds[13], (HEADS,), jnp.float32) ** levels(seeds[13], (HEADS,), ((0, 4),), -0.2, 0.2), 0.3, 0.8),
        "context_lift": jnp.clip(1.5 + 1.0 * jax.random.uniform(seeds[14], (HEADS,), jnp.float32) ** levels(seeds[14], (HEADS,), ((0, 4),), -0.2, 0.2), 1.5, 2.5),
        "value_gain": jnp.clip(1.0 + 0.18 * jax.random.normal(seeds[15], (VALUE_DIM,), jnp.float32), 0.1, 1.9),
        "w_out": noise(seeds[16], (HEADS * VALUE_DIM, D), (HEADS * VALUE_DIM) ** -0.5, 0.1875, ((0, 4),)),
    }


token_eps = 0.01
head_eps = 0.001
rope_base = 10000.0
head_factor = 0.8

def modulated_norm(row_block, gain_vector, shift_vector, scale_vector):
    values = row_block.astype(jnp.float32)
    inverse = lax.rsqrt(lax.optimization_barrier(jnp.mean(values * values, axis=-1, keepdims=True)) + token_eps)
    return (values * inverse * gain_vector * (1.0 + scale_vector) + shift_vector).astype(jnp.bfloat16)

def head_norm(values, gain_vector):
    inverse = lax.rsqrt(lax.optimization_barrier(jnp.mean(values * values, axis=-1, keepdims=True)) + token_eps)
    return values * inverse * gain_vector

def rotate(values, positions):
    quarter = values.shape[-1] // 4
    inverse = rope_base ** (-jnp.arange(quarter, dtype=jnp.float32) / quarter)
    grid_row = (positions // GRID).astype(jnp.float32)
    grid_col = (positions % GRID).astype(jnp.float32)
    angles = jnp.stack([grid_row[:, None] * inverse, grid_col[:, None] * inverse], axis=1)
    cosine_table = jnp.cos(angles)[:, None, None]
    sine_table = jnp.sin(angles)[:, None, None]
    halves = values.reshape(values.shape[:3] + (2, 2, quarter))
    front_half = halves[..., 0, :]
    back_half = halves[..., 1, :]
    turned = jnp.stack([front_half * cosine_table - back_half * sine_table, back_half * cosine_table + front_half * sine_table], axis=-2)
    return turned.reshape(values.shape)

def project_heads(row_block, weight, gain_vector, positions, factor):
    row_count = row_block.shape[0]
    head_width = gain_vector.shape[0]
    product = jnp.dot(row_block, weight, preferred_element_type=jnp.float32)
    shaped = head_norm(product.reshape(row_count, -1, 2, head_width), gain_vector)
    if positions is not None:
        shaped = rotate(shaped, positions)
    return (shaped * factor).astype(jnp.bfloat16).reshape(row_count, -1)

def attend_block(query_block, latent_keys, latent_values, context_keys, context_values, mix_lambda, context_lift, value_gain):
    head_count = mix_lambda.shape[0]
    head_width = latent_keys.shape[1] // (2 * head_count)
    shaped_query = query_block.astype(jnp.float32).reshape(query_block.shape[0], head_count, 2, head_width)

    def one_side(key_slab, value_slab, extra):
        shaped_keys = key_slab.astype(jnp.float32).reshape(key_slab.shape[0], head_count, 2, head_width)
        shaped_values = value_slab.astype(jnp.float32).reshape(value_slab.shape[0], head_count, -1)
        scores = jnp.einsum('qhmd,phmd->mhqp', shaped_query, shaped_keys) + extra
        weights = jnp.exp(scores)
        rounded = lax.optimization_barrier(weights.astype(jnp.bfloat16)).astype(jnp.float32)
        return (jnp.einsum('mhqp,phe->mhqe', rounded, shaped_values), lax.optimization_barrier(jnp.sum(weights, axis=-1)))
    latent_numer, latent_total = one_side(latent_keys, latent_values, jnp.float32(0.0))
    context_numer, context_total = one_side(context_keys, context_values, context_lift[None, :, None, None])
    ratios = (latent_numer + context_numer) / (latent_total + context_total)[..., None]
    mixed_heads = ratios[0] - mix_lambda[:, None, None] * ratios[1]
    inverse = lax.rsqrt(lax.optimization_barrier(jnp.mean(mixed_heads * mixed_heads, axis=-1, keepdims=True)) + head_eps)
    normalized = (mixed_heads * inverse * value_gain * head_factor).astype(jnp.bfloat16)
    return jnp.transpose(normalized, (1, 0, 2)).reshape(query_block.shape[0], -1)

def reference(latent, context, cond, context_cond, norm_gain, mod_shift, mod_scale, mod_gate, w_query, w_key, w_value, query_gain, key_gain, mix_lambda, context_lift, value_gain, w_out):
    cond_act = jax.nn.silu(cond.astype(jnp.float32)).astype(jnp.bfloat16)
    context_act = jax.nn.silu(context_cond.astype(jnp.float32)).astype(jnp.bfloat16)
    shift = jnp.dot(cond_act, mod_shift, preferred_element_type=jnp.float32)
    scale = jnp.dot(cond_act, mod_scale, preferred_element_type=jnp.float32)
    gate = jnp.dot(cond_act, mod_gate, preferred_element_type=jnp.float32)
    context_shift = jnp.dot(context_act, mod_shift, preferred_element_type=jnp.float32)
    context_scale = jnp.dot(context_act, mod_scale, preferred_element_type=jnp.float32)
    normed = modulated_norm(latent, norm_gain, shift, scale)
    context_normed = modulated_norm(context, norm_gain, context_shift, context_scale)
    length = latent.shape[0]
    positions = jnp.arange(length, dtype=jnp.int32)
    queries = project_heads(normed, w_query, query_gain, positions, HEAD_DIM ** (-0.5))
    latent_keys = project_heads(normed, w_key, key_gain, positions, 1.0)
    latent_values = jnp.dot(normed, w_value, preferred_element_type=jnp.float32).astype(jnp.bfloat16)
    context_keys = project_heads(context_normed, w_key, key_gain, None, 1.0)
    context_values = jnp.dot(context_normed, w_value, preferred_element_type=jnp.float32).astype(jnp.bfloat16)
    block_rows = 512 if length % 512 == 0 else length
    query_blocks = queries.reshape(length // block_rows, block_rows, -1)
    head_out = lax.map(lambda block_query: attend_block(block_query, latent_keys, latent_values, context_keys, context_values, mix_lambda, context_lift, value_gain), query_blocks).reshape(length, -1)
    mixture = jnp.dot(head_out, w_out, preferred_element_type=jnp.float32)
    return (latent.astype(jnp.float32) + gate * mixture).astype(jnp.bfloat16)
```

```python
import functools

import jax
import jax.numpy as jnp
import numpy as np
from jax import lax
from jax.experimental import pallas as pl
from jax.experimental.pallas import tpu as pltpu
from jax.sharding import PartitionSpec as P

GRID = 64
token_eps = 0.01
head_eps = 0.001
rope_base = 10000.0
head_factor = 0.8
MESH = pl.DeviceIdType.MESH
BF = jnp.bfloat16
F32 = jnp.float32


def rope_tables(length, width):
    quarter = width // 4
    inverse = (rope_base ** (-np.arange(quarter, dtype=np.float64) / quarter)).astype(np.float32)
    pos = np.arange(length)
    row = (pos // GRID).astype(np.float32)[:, None] * inverse
    col = (pos % GRID).astype(np.float32)[:, None] * inverse
    cos = np.concatenate([np.cos(row), np.cos(row), np.cos(col), np.cos(col)], axis=1)
    sin = np.concatenate([-np.sin(row), np.sin(row), -np.sin(col), np.sin(col)], axis=1)
    return np.tile(cos, (1, 2)).astype(np.float32), np.tile(sin, (1, 2)).astype(np.float32)


def kernel(n_sp, n_tp, n_dp, head_width, *refs):
    (
        lat_h, ctx_h, cond_h, cctx_h, gain_h, ms_h, msc_h, mg_h, wq_h, wk_h, wv_h,
        qg_h, kg_h, vg_h, lam_r, lift_r, wo_h, cos_h, sin_h,
        out_r,
        cond_r, cctx_r, gain_r, qg_r, kg_r, vg_r,
        lat, ctx, mw, wq, wk, wv, wo, cosv, sinv,
        act, part, mod_in, summed, mod_full, vecs, invs, normed, qown, qin, qm, kvl, kvr, acc, mine, ho, grp,
        loc, bs_lat, br_lat, bs_mod, br_mod, bs_mt, br_mt, bs_kv, br_kv, bs_wo, br_wo,
        bs_dd, br_dd, bs_ho, br_ho, bs_q, br_q,
    ) = refs
    s = lax.axis_index("sp")
    t = lax.axis_index("tp")
    d_ix = lax.axis_index("dp")
    core = lax.rem(d_ix, 2)
    partner = d_ix + 1 - 2 * core
    t_odd = lax.rem(t, 2)
    nbr1 = t + 1 - 2 * t_odd
    nbr2 = lax.rem(t + 2, 4)
    nbr3 = lax.rem(nbr1 + 2, 4)
    peers = (t, nbr1, nbr2, nbr3)
    e = lax.rem(s, 2)
    pair = s + 1 - 2 * e
    R = lat.shape[1]
    HR = R // 2
    C = ctx.shape[0]
    D = lat.shape[2]
    QW = wq.shape[1]
    n_head = QW // (2 * head_width)
    HW = 2 * head_width
    VW = wv.shape[1] // n_head
    ROWS = 4 * R

    def local(i, src, dst):
        c = pltpu.make_async_copy(src, dst, loc.at[i])
        c.start()
        return c

    l_lat = local(0, lat_h, lat.at[0])
    l_one = [local(11 + j, src, dst) for j, (src, dst) in enumerate(((cond_h, cond_r), (cctx_h, cctx_r)))]
    l_mod = [local(1 + j, h, mw.at[j]) for j, h in enumerate((ms_h, msc_h, mg_h))]

    bar = pltpu.get_barrier_semaphore()
    for k in range(1, n_sp):
        pl.semaphore_signal(bar, inc=1, device_id={"sp": lax.rem(s + k, n_sp)}, device_id_type=MESH)
    for k in range(1, 4):
        pl.semaphore_signal(bar, inc=1, device_id={"tp": peers[k]}, device_id_type=MESH)
        pl.semaphore_signal(
            bar, inc=1, device_id={"sp": pair, "tp": peers[k]}, device_id_type=MESH
        )
    pl.semaphore_signal(bar, inc=1, device_id={"dp": partner}, device_id_type=MESH)

    def remote(src, dst, ss, rs, where):
        return pltpu.make_async_remote_copy(
            src_ref=src, dst_ref=dst, send_sem=ss, recv_sem=rs, device_id=where, device_id_type=MESH
        )

    QR = HR // 2

    def lat_copy(i, src_slot, dst_slot, at, count, where):
        rows = pl.ds(at, count)
        return remote(lat.at[src_slot, rows], lat.at[dst_slot, rows], bs_lat.at[i], br_lat.at[i],
                      {"tp": where})

    x0 = lat_copy(0, 0, 1, 0, HR, nbr1)
    y1 = lat_copy(1, 0, 2, HR, HR, nbr2)
    x1 = [lat_copy(2 + j, 0, 1, HR + j * QR, QR, nbr1) for j in range(2)]
    y0 = [lat_copy(4 + j, 0, 2, j * QR, QR, nbr2) for j in range(2)]
    f0 = lat_copy(6, 1, 3, 0, HR, nbr2)
    f1 = lat_copy(7, 2, 3, HR, HR, nbr1)

    l_lat.wait()
    pl.semaphore_wait(bar, n_sp + 6)
    for c in (x0, y1, x1[0], y0[0]):
        c.start()

    act[...] = jnp.zeros_like(act)
    for row, ref in ((0, cond_r), (1, cctx_r)):
        l_one[row].wait()
        v = ref[...].astype(F32).reshape(1, -1)
        act[row : row + 1, :] = v / (1.0 + jnp.exp(-v))
    acts = act[...].astype(BF)
    part[...] = jnp.zeros_like(part)
    for j in range(3):
        l_mod[j].wait()
        res = jnp.dot(acts, mw[j], preferred_element_type=F32)
        part[2 * j : 2 * j + 2, :] = res[0:2]

    mod_copies = []
    for k in range(1, n_sp):
        c = remote(part, mod_in.at[k - 1], bs_mod.at[k - 1], br_mod.at[k - 1],
                   {"sp": lax.rem(s + k, n_sp)})
        c.start()
        mod_copies.append(c)

    l_ctx = local(4, ctx_h, ctx)
    l_wk = local(5, wk_h, wk)
    l_wv = local(6, wv_h, wv)
    l_cos = local(9, cos_h.at[pl.ds(s * ROWS, ROWS)], cosv)
    l_sin = local(10, sin_h.at[pl.ds(s * ROWS, ROWS)], sinv)
    l_one += [
        local(13 + j, src, dst)
        for j, (src, dst) in enumerate(((gain_h, gain_r), (qg_h, qg_r), (kg_h, kg_r), (vg_h, vg_r)))
    ]
    l_wq = local(7, wq_h, wq)
    l_wo = local(8, wo_h, wo.at[0])

    group = (
        lax.rem(lax.broadcasted_iota(jnp.int32, (2 * QW, QW), 0), QW) // head_width
        == lax.broadcasted_iota(jnp.int32, (2 * QW, QW), 1) // head_width
    )
    grp[...] = jnp.where(group, 1.0 / head_width, 0.0).astype(BF)

    l_ctx.wait()

    def inverse_rows(src, count, dst_at):
        for i in range(count // 16):
            v = src[i * 16 : (i + 1) * 16, :].astype(F32)
            inv = lax.rsqrt(jnp.mean(v * v, axis=-1, keepdims=True) + token_eps)
            invs[dst_at + i * 16 : dst_at + (i + 1) * 16, :] = jnp.broadcast_to(inv, (16, 128))

    inverse_rows(ctx, C, 0)
    inverse_rows(lat.at[0], R, C)

    total = part[...]
    for k in range(n_sp - 1):
        mod_copies[k].wait_recv()
        total = total + mod_in[k]
    summed[...] = total
    mod_full[t] = total
    tp_copies = []
    for k in range(1, 4):
        c = remote(summed, mod_full.at[t], bs_mt.at[k - 1], br_mt.at[k - 1], {"tp": peers[k]})
        c.start()
        tp_copies.append(c)
    x1[1].start()
    y0[1].start()
    x0.wait_recv()
    f0.start()
    y1.wait_recv()
    f1.start()

    HALF = wo.shape[1] // 2
    QUART = HALF // 2
    EIGHTH = QUART // 2

    def wo_rows(at, count):
        return pl.ds(pl.multiple_of(core * HALF + at, count), count)

    def wo_copy(i, src_slot, dst_slot, at, count, where):
        rows = wo_rows(at, count)
        return remote(wo.at[src_slot, rows], wo.at[dst_slot, rows], bs_wo.at[i], br_wo.at[i],
                      {"tp": where})

    def dd_copy(i, k, at, count):
        rows = wo_rows(at, count)
        return remote(wo.at[k, rows], wo.at[k, rows], bs_dd.at[i], br_dd.at[i], {"dp": partner})

    def dd_recv(i, k, at, count):
        rows = pl.ds(pl.multiple_of((1 - core) * HALF + at, count), count)
        return remote(wo.at[k, rows], wo.at[k, rows], bs_dd.at[i], br_dd.at[i], {"dp": partner})

    wx0 = wo_copy(0, 0, 1, 0, QUART, nbr1)
    wy1 = wo_copy(1, 0, 2, QUART, QUART, nbr2)
    wx1 = wo_copy(2, 0, 1, QUART, QUART, nbr1)
    wy0 = wo_copy(3, 0, 2, 0, QUART, nbr2)
    wf = [
        wo_copy(4, 1, 3, 0, EIGHTH, nbr2),
        wo_copy(5, 1, 3, EIGHTH, EIGHTH, nbr2),
        wo_copy(6, 2, 3, QUART, EIGHTH, nbr1),
        wo_copy(7, 2, 3, QUART + EIGHTH, EIGHTH, nbr1),
    ]
    dd_parts = [(0, 1, 0, HALF), (1, 2, 0, HALF), (2, 3, 0, EIGHTH), (3, 3, EIGHTH, EIGHTH),
                (4, 3, QUART, EIGHTH), (5, 3, QUART + EIGHTH, EIGHTH)]
    dd = [dd_copy(*d) for d in dd_parts]

    l_wo.wait()
    for c in (wx0, wy1, wx1, wy0):
        c.start()

    for k in range(1, 4):
        remote(summed, mod_full.at[peers[k]], bs_mt.at[k - 1], br_mt.at[k - 1],
               {"tp": peers[k]}).wait_recv()

    def full_row(j):
        return jnp.concatenate([mod_full[q, j : j + 1, :] for q in range(n_tp)], axis=1)

    for c in l_one[2:]:
        c.wait()
    gain = gain_r[...].reshape(1, -1)
    q_gain = qg_r[...].reshape(1, -1)
    q_gain = jnp.concatenate([q_gain, q_gain], axis=1)
    k_gain = kg_r[...].reshape(1, -1)
    k_gain = jnp.concatenate([k_gain, k_gain], axis=1)
    v_gain = vg_r[...].reshape(1, -1)
    vecs[0:1, :] = full_row(0)
    vecs[1:2, :] = full_row(1)
    vecs[2:3, :] = gain * (1.0 + full_row(2))
    vecs[3:4, :] = gain * (1.0 + full_row(3))
    vecs[4:5, :] = full_row(4)

    def norm_rows(src, row, count, dst_at):
        step = 16

        @pl.loop(0, count // step, unroll=True)
        def _(i):
            at = pl.multiple_of(i * step, step)
            v = src[pl.ds(at, step), :].astype(F32)
            inv = lax.rsqrt(jnp.mean(v * v, axis=-1, keepdims=True) + token_eps)
            normed[pl.ds(dst_at + at, step), :] = (
                v * inv * vecs[2 + row : 3 + row, :] + vecs[row : row + 1, :]
            ).astype(BF)

    def apply_rows(src, row, count, dst_at):
        for i in range(count // 16):
            v = src[i * 16 : (i + 1) * 16, :].astype(F32)
            at = slice(dst_at + i * 16, dst_at + (i + 1) * 16)
            normed[at, :] = (
                v * invs[at, 0:1] * vecs[2 + row : 3 + row, :] + vecs[row : row + 1, :]
            ).astype(BF)

    def head_norm(x):
        square = x * x
        high = square.astype(BF)
        low = (square - high.astype(F32)).astype(BF)
        mean = jnp.dot(jnp.concatenate([high, low], axis=1), grp[...], preferred_element_type=F32)
        return x * lax.rsqrt(mean + token_eps)

    def turn(y, cos, sin):
        lane = lax.broadcasted_iota(jnp.int32, y.shape, 1)
        front = lax.rem(lane, head_width // 2) < head_width // 4
        other = jnp.where(
            front,
            pltpu.roll(y, HW - head_width // 4, axis=1),
            pltpu.roll(y, head_width // 4, axis=1),
        )
        return y * cos + other * sin

    def project(first, count, plain):
        x = normed[first : first + count, :]
        kk = head_norm(jnp.dot(x, wk[...], preferred_element_type=F32))
        for h in range(n_head):
            y = kk[:, h * HW : (h + 1) * HW] * k_gain
            if plain:
                kvl[h, first : first + plain, 0:HW] = y[:plain].astype(BF)
            for at in range(plain, count, R):
                k = (first + at - C) // R
                pos = pl.ds(pl.multiple_of(peers[k] * R, R), R)
                kvl[h, first + at : first + at + R, 0:HW] = turn(
                    y[at : at + R], cosv[pos, :], sinv[pos, :]
                ).astype(BF)
        vv = jnp.dot(x, wv[...], preferred_element_type=F32).astype(BF)
        for h in range(n_head):
            kvl[h, first : first + count, HW:] = vv[:, h * VW : (h + 1) * VW]

    def project_queries():
        x = normed[C:, :]
        qq = head_norm(jnp.dot(x, wq[...], preferred_element_type=F32))
        for k in range(4):
            at = pl.ds(pl.multiple_of(peers[k] * R, R), R)
            cos, sin = cosv[at, :], sinv[at, :]
            for h in range(n_head):
                y = qq[k * R : (k + 1) * R, h * HW : (h + 1) * HW] * q_gain
                qown[h, k * R : (k + 1) * R, :] = (
                    turn(y, cos, sin) * (head_width ** -0.5)
                ).astype(BF)

    def split_maps(q, at):
        lane = lax.broadcasted_iota(jnp.int32, q.shape, 1)
        for m in range(2):
            qm[m, at : at + ROWS, :] = jnp.where(lane // head_width == m, q, jnp.zeros_like(q))

    chunks = ((0, C + R), (C + R, 2 * R), (C + 3 * R, R))

    def kv_copy(direction, dist, c, src, origin, where):
        at, count = chunks[c]
        i = (direction * (n_sp - 1) + dist - 1) * len(chunks) + c
        return remote(src.at[pl.ds(at, count)], kvr.at[origin, pl.ds(at, count)], bs_kv.at[i],
                      br_kv.at[i], {"sp": where})

    def side(direction, dist, c, act_on):
        sign = 1 - 2 * direction
        hop = 1 if dist == 1 else 2
        origin = s - sign * (dist - hop)
        where = s + sign * hop
        ok = jnp.logical_and(
            jnp.logical_and(origin >= 0, origin < n_sp),
            jnp.logical_and(where >= 0, where < n_sp),
        )

        @pl.when(ok)
        def _():
            if dist == 1:
                src = kvl.at[1 - e]
            elif dist == 2:
                src = kvl.at[e]
            else:
                src = kvr.at[origin]
            act_on(kv_copy(direction, dist, c, src, origin, where))

    def start(copy):
        copy.start()

    def drain(copy):
        copy.wait_send()

    def send_own(c):
        for dist in (1, 2):
            if dist < n_sp:
                for direction in (0, 1):
                    side(direction, dist, c, start)

    apply_rows(ctx, 1, C, 0)
    apply_rows(lat.at[0], 0, R, C)
    l_wk.wait()
    l_wv.wait()
    l_cos.wait()
    l_sin.wait()
    project(0, C + R, C)
    send_own(0)

    for c in [x1[0], x1[1], y0[0], y0[1]]:
        c.wait_recv()
    norm_rows(lat.at[1], 0, R, C + R)
    norm_rows(lat.at[2], 0, R, C + 2 * R)
    project(C + R, 2 * R, 0)
    send_own(1)
    f0.wait_recv()
    f1.wait_recv()
    norm_rows(lat.at[3], 0, R, C + 3 * R)
    project(C + 3 * R, R, 0)
    send_own(2)

    def arrive(dist, c):
        for direction in (0, 1):
            origin = s - dist if direction == 0 else s + dist
            here = origin >= 0 if direction == 0 else origin < n_sp

            @pl.when(here)
            def _():
                kv_copy(direction, dist, c, kvr.at[origin], origin, s).wait_recv()

            if dist + 2 < n_sp:
                side(direction, dist + 2, c, start)

    l_wq.wait()
    project_queries()
    q_copy = remote(qown.at[1 - e], qin, bs_q, br_q, {"sp": pair})
    q_copy.start()
    split_maps(qown[e], 0)
    arrive(1, 0)

    QB = 2 * R
    lift = lift_r[e]

    def attend(block, at, keys, start_row, count, first):
        k = block[at : at + keys, 0:HW]
        v = block[at : at + keys, HW:]
        vx = jnp.concatenate([v, jnp.ones_like(v)], axis=1)
        key = lax.broadcasted_iota(jnp.int32, (1, keys), 1)
        for m in range(2):
            for b in range(count // QB):
                rows = slice(start_row + b * QB, start_row + (b + 1) * QB)
                sc = lax.dot_general(
                    qm[m, rows, :], k, (((1,), (1,)), ((), ())), preferred_element_type=F32
                )
                if at < C:
                    sc = sc + jnp.where(key < C - at, lift, 0.0)
                p = jnp.exp(sc).astype(BF)
                add = jnp.dot(p, vx, preferred_element_type=F32)
                if first:
                    acc[m, rows, :] = add
                else:
                    acc[m, rows, :] += add

    def attend_arrived(dist, at, keys):
        @pl.when(s - dist >= 0)
        def _():
            attend(kvr.at[s - dist], at, keys, 0, 2 * ROWS, False)

        @pl.when(s + dist < n_sp)
        def _():
            attend(kvr.at[s + dist], at, keys, 0, 2 * ROWS, False)

    attend(kvl.at[e], 0, C + ROWS, 0, ROWS, True)
    for c in range(1, len(chunks)):
        arrive(1, c)
    wx0.wait_recv()
    wf[0].start()
    wf[1].start()
    wy1.wait_recv()
    wf[2].start()
    wf[3].start()
    q_copy.wait_recv()
    split_maps(qin[...], ROWS)
    attend(kvl.at[e], 0, C + ROWS, ROWS, ROWS, True)

    for dist in range(1, n_sp):
        last = dist == n_sp - 1
        if dist > 1:
            for c in range(len(chunks)):
                arrive(dist, c)
        attend_arrived(dist, 0, C + ROWS)
        if dist == 2 or (last and n_sp == 2):
            wx1.wait_recv()
            dd[0].start()
            wy0.wait_recv()
            dd[1].start()

    def ho_copy(q, k):
        i = q * 4 + k
        where = {"tp": peers[k]} if q == 0 else {"sp": pair, "tp": peers[k]}
        if q == 1 and k == 0:
            where = {"sp": pair}
        lanes = pl.ds(pl.multiple_of(e * VW, VW), VW)
        return remote(mine.at[q, k], ho.at[k, :, lanes], bs_ho.at[i], br_ho.at[i], where)

    for q, k in ((1, 3), (1, 1), (1, 2), (0, 3), (1, 0), (0, 1), (0, 2), (0, 0)):
        rows = slice((4 * q + k) * R, (4 * q + k + 1) * R)
        a0 = acc[0, rows, :]
        a1 = acc[1, rows, :]
        mixed = a0[:, :VW] / a0[:, VW:] - lam_r[e] * (a1[:, :VW] / a1[:, VW:])
        inv = lax.rsqrt(jnp.mean(mixed * mixed, axis=-1, keepdims=True) + head_eps)
        value = (mixed * inv * v_gain * head_factor).astype(BF)
        if q or k:
            mine[q, k, :, :] = value
            ho_copy(q, k).start()
        else:
            for h in range(2):
                @pl.when(e == h)
                def _():
                    ho[0, :, h * VW : (h + 1) * VW] = value

    for c, d in zip(wf, dd[2:]):
        c.wait_recv()
        d.start()

    for k in range(4):
        for i, part_k, at, count in dd_parts:
            if part_k == k:
                dd_recv(i, k, at, count).wait_recv()
        for q in range(2):
            if q or k:
                ho_copy(q, k).wait_recv()
        add = jnp.dot(ho[k], wo[k], preferred_element_type=F32)
        if k == 0:
            out_r[...] = add
        elif k < 3:
            out_r[...] += add
        else:
            out_r[...] = vecs[4:5, :] * (out_r[...] + add)

    for c in mod_copies + tp_copies + [x0, y1, *x1, *y0, f0, f1, wx0, wy1, wx1, wy0] + wf + dd:
        c.wait_send()
    q_copy.wait_send()
    for q in range(2):
        for k in range(4):
            if q or k:
                ho_copy(q, k).wait_send()
    for dist in range(1, n_sp):
        for c in range(len(chunks)):
            for direction in (0, 1):
                side(direction, dist, c, drain)


def on_device(n_sp, n_tp, n_dp, *args):
    (
        latent, context, cond, context_cond, norm_gain, mod_shift, mod_scale, mod_gate,
        w_query, w_key, w_value, query_gain, key_gain, mix_lambda, context_lift, value_gain, w_out,
    ) = args
    R, D = latent.shape
    C = context.shape[0]
    head_width = query_gain.shape[0]
    cos, sin = rope_tables(R * n_sp * n_tp, head_width)
    QW, VWALL = w_query.shape[1], w_value.shape[1]
    heads = mix_lambda.shape[0]
    ROWS = R * n_tp
    MC = mod_shift.shape[1]
    chunk_sems = 2 * max(n_sp - 1, 1) * 3
    vm = pl.BlockSpec(memory_space=pltpu.VMEM)
    anywhere = pl.BlockSpec(memory_space=pl.ANY)
    smem = pl.BlockSpec(memory_space=pltpu.SMEM)
    dma = pltpu.SemaphoreType.DMA
    update = pl.pallas_call(
        functools.partial(kernel, n_sp, n_tp, n_dp, head_width),
        out_shape=pltpu.VMEM((R, D), F32),
        in_specs=[anywhere] * 14 + [smem, smem]
        + [anywhere] * 3,
        out_specs=vm,
        scratch_shapes=[
            pltpu.VMEM(cond.shape, BF),
            pltpu.VMEM(context_cond.shape, BF),
            pltpu.VMEM(norm_gain.shape, F32),
            pltpu.VMEM(query_gain.shape, F32),
            pltpu.VMEM(key_gain.shape, F32),
            pltpu.VMEM(value_gain.shape, F32),
            pltpu.VMEM((4, R, D), BF),
            pltpu.VMEM((C, D), BF),
            pltpu.VMEM((3,) + mod_shift.shape, BF),
            pltpu.VMEM(w_query.shape, BF),
            pltpu.VMEM(w_key.shape, BF),
            pltpu.VMEM(w_value.shape, BF),
            pltpu.VMEM((4,) + w_out.shape, BF),
            pltpu.VMEM((ROWS, 2 * head_width), F32),
            pltpu.VMEM((ROWS, 2 * head_width), F32),
            pltpu.VMEM((8, mod_shift.shape[0]), F32),
            pltpu.VMEM((8, MC), F32),
            pltpu.VMEM((max(n_sp - 1, 1), 8, MC), F32),
            pltpu.VMEM((8, MC), F32),
            pltpu.VMEM((n_tp, 8, MC), F32),
            pltpu.VMEM((8, D), F32),
            pltpu.VMEM((C + R, 128), F32),
            pltpu.VMEM((C + ROWS, D), BF),
            pltpu.VMEM((heads, ROWS, 2 * head_width), BF),
            pltpu.VMEM((ROWS, 2 * head_width), BF),
            pltpu.VMEM((2, 2 * ROWS, 2 * head_width), BF),
            pltpu.VMEM((heads, C + ROWS, (QW + VWALL) // heads), BF),
            pltpu.VMEM((n_sp, C + ROWS, (QW + VWALL) // heads), BF),
            pltpu.VMEM((2, 2 * ROWS, 2 * VWALL // heads), F32),
            pltpu.VMEM((2, 4, R, VWALL // heads), BF),
            pltpu.VMEM((4, R, VWALL), BF),
            pltpu.VMEM((2 * QW, QW), BF),
            dma((17,)),
            dma((8,)), dma((8,)),
            dma((max(n_sp - 1, 1),)), dma((max(n_sp - 1, 1),)),
            dma((3,)), dma((3,)),
            dma((chunk_sems,)), dma((chunk_sems,)),
            dma((8,)), dma((8,)),
            dma((6,)), dma((6,)),
            dma((8,)), dma((8,)),
            dma(()), dma(()),
        ],
        compiler_params=pltpu.CompilerParams(
            collective_id=0, has_side_effects=True, vmem_limit_bytes=66_100_000
        ),
        name="block",
    )(
        latent, context, cond, context_cond, norm_gain, mod_shift, mod_scale,
        mod_gate, w_query, w_key, w_value, query_gain, key_gain, value_gain, mix_lambda, context_lift, w_out,
        jnp.asarray(cos), jnp.asarray(sin),
    )
    return (latent.astype(F32) + update).astype(latent.dtype)


def solution(mesh):
    placed = (
        P(("dp", "sp", "tp"), None),
        P(("dp", "sp"), None),
        P(("dp", "sp")),
        P("sp"),
        P(),
        P("sp", "tp"),
        P("sp", "tp"),
        P("sp", "tp"),
        P(None, "tp"),
        P(None, "tp"),
        P(None, "tp"),
        P(),
        P(),
        P("tp"),
        P("tp"),
        P(),
        P("tp", None),
    )
    sizes = mesh.shape
    return jax.shard_map(
        functools.partial(on_device, sizes["sp"], sizes["tp"], sizes["dp"]),
        mesh=mesh,
        in_specs=placed,
        out_specs=P(("dp", "sp", "tp"), None),
        check_vma=False,
    )
```

```python
import functools

import jax
import jax.numpy as jnp
import numpy as np
from jax import lax
from jax.experimental import pallas as pl
from jax.experimental.pallas import tpu as pltpu
from jax.sharding import PartitionSpec as P

GRID = 64
token_eps = 0.01
head_eps = 0.001
rope_base = 10000.0
head_factor = 0.8
MESH = pl.DeviceIdType.MESH
BF = jnp.bfloat16
F32 = jnp.float32


def rope_tables(length, width):
    quarter = width // 4
    inverse = (rope_base ** (-np.arange(quarter, dtype=np.float64) / quarter)).astype(np.float32)
    pos = np.arange(length)
    row = (pos // GRID).astype(np.float32)[:, None] * inverse
    col = (pos % GRID).astype(np.float32)[:, None] * inverse
    cos = np.concatenate([np.cos(row), np.cos(row), np.cos(col), np.cos(col)], axis=1)
    sin = np.concatenate([-np.sin(row), np.sin(row), -np.sin(col), np.sin(col)], axis=1)
    return np.tile(cos, (1, 2)).astype(np.float32), np.tile(sin, (1, 2)).astype(np.float32)


def kernel(n_sp, n_tp, n_dp, head_width, *refs):
    (
        lat_h, ctx_h, cond_h, cctx_h, gain_h, ms_h, msc_h, mg_h, wq_h, wk_h, wv_h,
        qg_h, kg_h, vg_h, lam_r, lift_r, wo_h, cos_h, sin_h,
        out_r,
        cond_r, cctx_r, gain_r, qg_r, kg_r, vg_r,
        own, lat, ctx, mw, wq, wkv, wo, turns,
        act, part, mod_in, summed, mod_full, vecs, normed, qown, qin, qm, kvl, kvr, kvc, acc,
        mine, ho, grp,
        loc, s_swap, r_swap, s_lat, r_lat, s_mod, r_mod, s_mt, r_mt, s_vec, r_vec, s_kv, r_kv,
        s_ctx, r_ctx, s_q, r_q, s_wo, r_wo, s_dd, r_dd, s_ho, r_ho,
    ) = refs
    s = lax.axis_index("sp")
    t = lax.axis_index("tp")
    d_ix = lax.axis_index("dp")
    core = lax.rem(d_ix, 2)
    partner = d_ix + 1 - 2 * core
    t_odd = lax.rem(t, 2)
    nbr1 = t + 1 - 2 * t_odd
    nbr2 = lax.rem(t + 2, 4)
    nbr3 = lax.rem(nbr1 + 2, 4)
    peers = (t, nbr1, nbr2, nbr3)
    H = n_sp // 2
    half = s // H
    base = half * H
    s_opp = lax.rem(s + H, n_sp)
    home = core == half
    away = jnp.not_equal(core, half)
    a = lax.rem(core + half, 2)
    block = s + a * (s_opp - s)
    other_block = s_opp + a * (s - s_opp)
    d_work = d_ix - core + half
    R, D = own.shape
    PR = R // 4
    C = ctx.shape[0]
    QW = wq.shape[1]
    n_head = QW // (2 * head_width)
    HW = 2 * head_width
    VW = wkv.shape[2] // n_head
    ROWS = 4 * R

    bar = pltpu.get_barrier_semaphore()
    greeted = [{"tp": peers[k]} for k in range(1, 4)] + [{"dp": partner}]
    for k in range(1, n_sp):
        there = lax.rem(s + k, n_sp)
        greeted += [{"sp": there}, {"dp": partner, "sp": there}]
    for where in greeted:
        pl.semaphore_signal(bar, inc=1, device_id=where, device_id_type=MESH)

    def local(i, src, dst):
        c = pltpu.make_async_copy(src, dst, loc.at[i])
        c.start()
        return c

    def remote(src, dst, ss, rs, where):
        return pltpu.make_async_remote_copy(
            src_ref=src, dst_ref=dst, send_sem=ss, recv_sem=rs, device_id=where, device_id_type=MESH
        )

    def drain(ref, sem):
        remote(ref, ref, sem, sem, {"dp": partner}).wait_recv()

    @pl.when(home)
    def _():
        local(0, lat_h, lat.at[0])

    @pl.when(away)
    def _():
        local(0, lat_h, own)

    l_one = [local(1, cond_h, cond_r), local(2, cctx_h, cctx_r)]
    for j, h in enumerate((ms_h, msc_h, mg_h)):
        local(3, h, mw.at[j])

    act[...] = jnp.zeros_like(act)
    for row, ref in ((0, cond_r), (1, cctx_r)):
        l_one[row].wait()
        v = ref[...].astype(F32).reshape(1, -1)
        act[row : row + 1, :] = v / (1.0 + jnp.exp(-v))
    acts = act[...].astype(BF)
    part[...] = jnp.zeros_like(part)
    drain(mw, loc.at[3])
    for j in range(3):
        res = jnp.dot(acts, mw[j], preferred_element_type=F32)
        part[2 * j : 2 * j + 2, :] = res[0:2]

    drain(own, loc.at[0])
    pl.semaphore_wait(bar, len(greeted))

    def mod_copy(k):
        return remote(part, mod_in.at[k - 1], s_mod, r_mod, {"sp": lax.rem(s + k, n_sp)})

    def piece(j):
        return pl.ds(j * PR, PR)

    def swap(j):
        return remote(own.at[piece(j)], lat.at[0, piece(j)], s_swap, r_swap.at[j],
                      {"dp": partner, "sp": s_opp})

    def along_x(j):
        return remote(lat.at[0, piece(j)], lat.at[1, piece(j)], s_lat, r_lat.at[j if j < 2 else 4],
                      {"tp": nbr1})

    def along_y(j):
        return remote(lat.at[0, piece(j)], lat.at[2, piece(j)], s_lat, r_lat.at[j if j > 1 else 4],
                      {"tp": nbr2})

    def onward(j):
        slot, where = (1, nbr2) if j < 2 else (2, nbr1)
        return remote(lat.at[slot, piece(j)], lat.at[3, piece(j)], s_lat, r_lat.at[5], {"tp": where})

    def pass_on(j):
        (along_x(j) if j < 2 else along_y(j)).wait_recv()
        onward(j).start()

    for k in range(1, n_sp):
        mod_copy(k).start()

    @pl.when(home)
    def _():
        for j in range(4):
            along_x(j).start()
            along_y((j + 2) % 4).start()

    @pl.when(away)
    def _():
        swap(0).start()
        swap(1).start()

    l_ctx = local(4, ctx_h, ctx)
    local(5, wk_h, wkv.at[0])
    local(5, wv_h, wkv.at[1])
    at_turns = pl.ds(pl.multiple_of(block * ROWS, ROWS), ROWS)
    local(6, cos_h.at[at_turns], turns.at[0])
    local(6, sin_h.at[at_turns], turns.at[1])
    l_small = [
        local(7 + j, src, dst)
        for j, (src, dst) in enumerate(((gain_h, gain_r), (qg_h, qg_r), (kg_h, kg_r), (vg_h, vg_r)))
    ]
    l_wq = local(11, wq_h, wq)
    l_wo = local(12, wo_h, wo.at[0])

    group = (
        lax.rem(lax.broadcasted_iota(jnp.int32, (2 * QW, QW), 0), QW) // head_width
        == lax.broadcasted_iota(jnp.int32, (2 * QW, QW), 1) // head_width
    )
    grp[...] = jnp.where(group, 1.0 / head_width, 0.0).astype(BF)
    for c in l_small:
        c.wait()
    gain = gain_r[...].reshape(1, -1)
    q_gain = qg_r[...].reshape(1, -1)
    q_gain = jnp.concatenate([q_gain, q_gain], axis=1)
    k_gain = kg_r[...].reshape(1, -1)
    k_gain = jnp.concatenate([k_gain, k_gain], axis=1)
    v_gain = vg_r[...].reshape(1, -1)

    drain(mod_in, r_mod)
    total = part[...]
    for k in range(n_sp - 1):
        total = total + mod_in[k]
    summed[...] = total
    mod_full[t] = total

    def mt_copy(k):
        return remote(summed, mod_full.at[t], s_mt, r_mt, {"tp": peers[k]})

    for k in range(1, 4):
        mt_copy(k).start()

    HALF = wo.shape[1] // 2
    QUART = HALF // 2
    EIGHTH = QUART // 2

    def wo_rows(at, count):
        return pl.ds(pl.multiple_of(core * HALF + at, count), count)

    def wo_copy(i, src_slot, dst_slot, at, count, where):
        rows = wo_rows(at, count)
        return remote(wo.at[src_slot, rows], wo.at[dst_slot, rows], s_wo, r_wo.at[i], {"tp": where})

    def dd_copy(i, k, at, count):
        rows = wo_rows(at, count)
        return remote(wo.at[k, rows], wo.at[k, rows], s_dd, r_dd.at[i], {"dp": partner})

    wx0 = wo_copy(0, 0, 1, 0, QUART, nbr1)
    wy1 = wo_copy(1, 0, 2, QUART, QUART, nbr2)
    wx1 = wo_copy(2, 0, 1, QUART, QUART, nbr1)
    wy0 = wo_copy(2, 0, 2, 0, QUART, nbr2)
    wf = [
        wo_copy(3, 1, 3, 0, EIGHTH, nbr2),
        wo_copy(4, 1, 3, EIGHTH, EIGHTH, nbr2),
        wo_copy(5, 2, 3, QUART, EIGHTH, nbr1),
        wo_copy(6, 2, 3, QUART + EIGHTH, EIGHTH, nbr1),
    ]
    dd = [dd_copy(0, 1, 0, HALF), dd_copy(1, 2, 0, HALF)] + [
        dd_copy(2, 3, i * EIGHTH, EIGHTH) for i in range(4)
    ]
    l_wo.wait()

    @pl.when(home)
    def _():
        for j in (0, 2, 1, 3):
            pass_on(j)
        for c in (wx0, wy1, wx1, wy0):
            c.start()

    @pl.when(away)
    def _():
        swap(2).start()
        swap(3).start()
        for j in range(4):
            swap(j).wait_recv()
            along_x(j).start()
            along_y(j).start()
        pass_on(0)
        pass_on(1)

    drain(mod_full.at[0:3], r_mt)

    def full_row(j):
        return jnp.concatenate([mod_full[q, j : j + 1, :] for q in range(n_tp)], axis=1)

    vecs[0, 0:1, :] = full_row(0)
    vecs[0, 1:2, :] = full_row(1)
    vecs[0, 2:3, :] = gain * (1.0 + full_row(2))
    vecs[0, 3:4, :] = gain * (1.0 + full_row(3))
    vecs[0, 4:8, :] = jnp.broadcast_to(full_row(4), (4, D))
    vec_copy = remote(vecs.at[0], vecs.at[1], s_vec, r_vec, {"dp": partner})

    @pl.when(home)
    def _():
        vec_copy.start()

    @pl.when(away)
    def _():
        vec_copy.wait_recv()

    def norm_rows(src, row, count, dst_at):
        step = 16

        @pl.loop(0, count // step, unroll=True)
        def _(i):
            at = pl.multiple_of(i * step, step)
            v = src[pl.ds(at, step), :].astype(F32)
            inv = lax.rsqrt(jnp.mean(v * v, axis=-1, keepdims=True) + token_eps)
            normed[pl.ds(dst_at + at, step), :] = (
                v * inv * vecs[a, 2 + row : 3 + row, :] + vecs[a, row : row + 1, :]
            ).astype(BF)

    def head_norm(x):
        square = x * x
        high = square.astype(BF)
        low = (square - high.astype(F32)).astype(BF)
        mean = jnp.dot(jnp.concatenate([high, low], axis=1), grp[...], preferred_element_type=F32)
        return x * lax.rsqrt(mean + token_eps)

    def turn(y, cos, sin):
        lane = lax.broadcasted_iota(jnp.int32, y.shape, 1)
        front = lax.rem(lane, head_width // 2) < head_width // 4
        other = jnp.where(
            front,
            pltpu.roll(y, HW - head_width // 4, axis=1),
            pltpu.roll(y, head_width // 4, axis=1),
        )
        return y * cos + other * sin

    def turns_of(k):
        at = pl.ds(pl.multiple_of(peers[k] * R, R), R)
        return turns[0, at, :], turns[1, at, :]

    def project(first, count, plain):
        x = normed[first : first + count, :]
        kk = head_norm(jnp.dot(x, wkv[0], preferred_element_type=F32))
        for h in range(n_head):
            y = kk[:, h * HW : (h + 1) * HW] * k_gain
            if plain:
                kvl[h, first : first + plain, 0:HW] = y[:plain].astype(BF)
            for at in range(plain, count, R):
                kvl[h, first + at : first + at + R, 0:HW] = turn(
                    y[at : at + R], *turns_of((first + at - C) // R)
                ).astype(BF)
        vv = jnp.dot(x, wkv[1], preferred_element_type=F32).astype(BF)
        for h in range(n_head):
            kvl[h, first : first + count, HW:] = vv[:, h * VW : (h + 1) * VW]

    def project_queries():
        x = normed[C:, :]
        qq = head_norm(jnp.dot(x, wq[...], preferred_element_type=F32))
        for k in range(4):
            for h in range(n_head):
                y = qq[k * R : (k + 1) * R, h * HW : (h + 1) * HW] * q_gain
                qown[h, k * R : (k + 1) * R, :] = (
                    turn(y, *turns_of(k)) * (head_width ** -0.5)
                ).astype(BF)

    def split_maps(q, at):
        lane = lax.broadcasted_iota(jnp.int32, q.shape, 1)
        for m in range(2):
            qm[m, at : at + ROWS, :] = jnp.where(lane // head_width == m, q, jnp.zeros_like(q))

    def kv_copy(j, head, at, count):
        there = base + lax.rem(s - base + j, H)
        i = 2 * j + a
        return remote(kvl.at[head, pl.ds(C + at, count)], kvr.at[block, pl.ds(at, count)], s_kv,
                      r_kv.at[i], {"dp": d_ix - core + head, "sp": there})

    def send_block(at, count):
        for j in range(1, H):
            for head in range(2):
                kv_copy(j, head, at, count).start()
        kv_copy(0, 1 - core, at, count).start()

    def ctx_copy(there, head):
        at = pl.ds(pl.multiple_of(s * C, C), C)
        return remote(kvl.at[head, pl.ds(0, C)], kvc.at[at], s_ctx, r_ctx,
                      {"dp": d_ix - core + head, "sp": there})

    def send_ctx():
        @pl.when(home)
        def _():
            for j in range(1, H):
                for head in range(2):
                    ctx_copy(base + lax.rem(s - base + j, H), head).start()
            ctx_copy(s, 1 - core).start()
            kvc[pl.ds(pl.multiple_of(s * C, C), C), :] = kvl[core, 0:C, :]

        @pl.when(away)
        def _():
            for j in range(H):
                for head in range(2):
                    ctx_copy(lax.rem(s_opp + j, H) + H - base, head).start()

    l_ctx.wait()
    norm_rows(ctx, 1, C, 0)
    norm_rows(lat.at[0], 0, R, C)
    drain(wkv, loc.at[5])
    drain(turns, loc.at[6])
    project(0, C + R, C)
    send_block(0, R)
    send_ctx()

    @pl.when(away)
    def _():
        pass_on(2)
        pass_on(3)
        for c in (wx0, wy1, wx1, wy0):
            c.start()

    drain(lat.at[1], r_lat.at[4])
    norm_rows(lat.at[1], 0, R, C + R)
    norm_rows(lat.at[2], 0, R, C + 2 * R)
    project(C + R, 2 * R, 0)
    send_block(R, 2 * R)
    drain(lat.at[3], r_lat.at[5])
    norm_rows(lat.at[3], 0, R, C + 3 * R)
    project(C + 3 * R, R, 0)
    send_block(3 * R, R)

    l_wq.wait()
    project_queries()
    q_copy = remote(qown.at[1 - core], qin, s_q, r_q, {"dp": partner})
    q_copy.start()
    split_maps(qown[core], 0)

    QB = 2 * R
    lift = lift_r[core]

    def attend(block, at, keys, start_row, count, first, plus):
        k = block[at : at + keys, 0:HW]
        v = block[at : at + keys, HW:]
        vx = jnp.concatenate([v, jnp.ones_like(v)], axis=1)
        for m in range(2):
            for b in range(count // QB):
                rows = slice(start_row + b * QB, start_row + (b + 1) * QB)
                sc = lax.dot_general(
                    qm[m, rows, :], k, (((1,), (1,)), ((), ())), preferred_element_type=F32
                )
                if plus is not None:
                    sc = sc + plus
                p = jnp.exp(sc).astype(BF)
                add = jnp.dot(p, vx, preferred_element_type=F32)
                if first:
                    acc[m, rows, :] = add
                else:
                    acc[m, rows, :] += add

    attend(kvl.at[core], C, ROWS, 0, ROWS, True, None)
    wx0.wait_recv()
    wf[0].start()
    wf[1].start()
    wy1.wait_recv()
    wf[2].start()
    wf[3].start()
    q_copy.wait_recv()
    split_maps(qin[...], ROWS)
    attend(kvl.at[core], C, ROWS, ROWS, ROWS, True, None)

    def attend_block(slot, i):
        drain(kvr.at[slot], r_kv.at[i])
        attend(kvr.at[slot], 0, ROWS, 0, 2 * ROWS, False, None)

    for j in range(1, H):
        attend_block(base + lax.rem(s - base + H - j, H), 2 * j)

    @pl.when(home)
    def _():
        drain(kvc.at[pl.ds(0, (n_sp - 1) * C)], r_ctx)

    @pl.when(away)
    def _():
        drain(kvc, r_ctx)

    attend(kvc, 0, n_sp * C, 0, 2 * ROWS, False, lift)
    attend_block(other_block, 1 - a)
    drain(wo.at[1, pl.ds(0, HALF)], r_wo.at[2])
    dd[0].start()
    dd[1].start()
    for j in range(1, H):
        attend_block(lax.rem(base + lax.rem(s - base + H - j, H) + H, n_sp), 2 * j + 1)

    def ho_copy(q, k):
        lanes = pl.ds(pl.multiple_of(core * VW, VW), VW)
        return remote(mine.at[4 * q + k], ho.at[k, :, lanes], s_ho, r_ho.at[k],
                      {"dp": d_work, "sp": other_block if q else block, "tp": peers[k]})

    for q, k in ((1, 3), (0, 3), (1, 1), (0, 1), (1, 2), (0, 2), (1, 0), (0, 0)):
        rows = slice((4 * q + k) * R, (4 * q + k + 1) * R)
        a0 = acc[0, rows, :]
        a1 = acc[1, rows, :]
        mixed = a0[:, :VW] / a0[:, VW:] - lam_r[core] * (a1[:, :VW] / a1[:, VW:])
        inv = lax.rsqrt(jnp.mean(mixed * mixed, axis=-1, keepdims=True) + head_eps)
        value = (mixed * inv * v_gain * head_factor).astype(BF)
        mine[4 * q + k, :, :] = value
        if q or k:
            ho_copy(q, k).start()
        else:
            @pl.when(away)
            def _():
                ho_copy(0, 0).start()

            for h in range(2):
                @pl.when(jnp.logical_and(home, core == h))
                def _():
                    ho[0, :, h * VW : (h + 1) * VW] = value

    for i in range(4):
        wf[i].wait_recv()
        dd[2 + i].start()

    @pl.when(home)
    def _():
        drain(mine.at[0], r_ho.at[0])

    @pl.when(away)
    def _():
        drain(ho.at[0], r_ho.at[0])

    for k in range(4):
        if k:
            drain(wo.at[k, pl.ds(0, HALF)], r_dd.at[k - 1])
            drain(ho.at[k], r_ho.at[k])
        add = jnp.dot(ho[k], wo[k], preferred_element_type=F32)
        if k == 0:
            out_r[...] = add
        elif k < 3:
            out_r[...] += add
        else:
            out_r[...] = vecs[0, 4:5, :] * (out_r[...] + add)

    def sent(ref, sem):
        remote(ref, ref, sem, sem, {"dp": partner}).wait_send()

    sent(mod_in, s_mod)
    sent(mod_full.at[0:3], s_mt)
    sent(lat.at[0:3], s_lat)
    sent(kvr.at[0 : n_sp - 1], s_kv)
    sent(wo.at[0:3, pl.ds(0, HALF)], s_wo)
    sent(wo.at[0:3, pl.ds(0, HALF)], s_dd)
    q_copy.wait_send()

    @pl.when(home)
    def _():
        vec_copy.wait_send()
        sent(kvc.at[pl.ds(0, (n_sp - 1) * C)], s_ctx)
        sent(mine.at[1:8], s_ho)

    @pl.when(away)
    def _():
        sent(own, s_swap)
        sent(kvc, s_ctx)
        sent(mine, s_ho)


def on_device(n_sp, n_tp, n_dp, *args):
    (
        latent, context, cond, context_cond, norm_gain, mod_shift, mod_scale, mod_gate,
        w_query, w_key, w_value, query_gain, key_gain, mix_lambda, context_lift, value_gain, w_out,
    ) = args
    R, D = latent.shape
    C = context.shape[0]
    head_width = query_gain.shape[0]
    cos, sin = rope_tables(R * n_sp * n_tp, head_width)
    QW, VWALL = w_query.shape[1], w_value.shape[1]
    heads = mix_lambda.shape[0]
    ROWS = R * n_tp
    HW = 2 * head_width
    KV = (QW + VWALL) // heads
    MC = mod_shift.shape[1]
    vm = pl.BlockSpec(memory_space=pltpu.VMEM)
    anywhere = pl.BlockSpec(memory_space=pl.ANY)
    smem = pl.BlockSpec(memory_space=pltpu.SMEM)
    dma = pltpu.SemaphoreType.DMA
    update = pl.pallas_call(
        functools.partial(kernel, n_sp, n_tp, n_dp, head_width),
        out_shape=pltpu.VMEM((R, D), F32),
        in_specs=[anywhere] * 14 + [smem, smem]
        + [anywhere] * 3,
        out_specs=vm,
        scratch_shapes=[
            pltpu.VMEM(cond.shape, BF),
            pltpu.VMEM(context_cond.shape, BF),
            pltpu.VMEM(norm_gain.shape, F32),
            pltpu.VMEM(query_gain.shape, F32),
            pltpu.VMEM(key_gain.shape, F32),
            pltpu.VMEM(value_gain.shape, F32),
            pltpu.VMEM((R, D), BF),
            pltpu.VMEM((4, R, D), BF),
            pltpu.VMEM((C, D), BF),
            pltpu.VMEM((3,) + mod_shift.shape, BF),
            pltpu.VMEM(w_query.shape, BF),
            pltpu.VMEM((2,) + w_key.shape, BF),
            pltpu.VMEM((4,) + w_out.shape, BF),
            pltpu.VMEM((2, ROWS, HW), F32),
            pltpu.VMEM((8, mod_shift.shape[0]), F32),
            pltpu.VMEM((8, MC), F32),
            pltpu.VMEM((n_sp - 1, 8, MC), F32),
            pltpu.VMEM((8, MC), F32),
            pltpu.VMEM((n_tp, 8, MC), F32),
            pltpu.VMEM((2, 8, D), F32),
            pltpu.VMEM((C + ROWS, D), BF),
            pltpu.VMEM((heads, ROWS, HW), BF),
            pltpu.VMEM((ROWS, HW), BF),
            pltpu.VMEM((2, 2 * ROWS, HW), BF),
            pltpu.VMEM((heads, C + ROWS, KV), BF),
            pltpu.VMEM((n_sp, ROWS, KV), BF),
            pltpu.VMEM((n_sp * C, KV), BF),
            pltpu.VMEM((2, 2 * ROWS, 2 * VWALL // heads), F32),
            pltpu.VMEM((8, R, VWALL // heads), BF),
            pltpu.VMEM((4, R, VWALL), BF),
            pltpu.VMEM((2 * QW, QW), BF),
            dma((13,)),
            dma(()), dma((4,)),
            dma(()), dma((6,)),
            dma(()), dma(()),
            dma(()), dma(()),
            dma(()), dma(()),
            dma(()), dma((n_sp,)),
            dma(()), dma(()),
            dma(()), dma(()),
            dma(()), dma((7,)),
            dma(()), dma((3,)),
            dma(()), dma((4,)),
        ],
        compiler_params=pltpu.CompilerParams(
            collective_id=0, has_side_effects=True, vmem_limit_bytes=66_100_000
        ),
        name="block",
    )(
        latent, context, cond, context_cond, norm_gain, mod_shift, mod_scale,
        mod_gate, w_query, w_key, w_value, query_gain, key_gain, value_gain, mix_lambda, context_lift, w_out,
        jnp.asarray(cos), jnp.asarray(sin),
    )
    return (latent.astype(F32) + update).astype(latent.dtype)


def solution(mesh):
    placed = (
        P(("dp", "sp", "tp"), None),
        P(("dp", "sp"), None),
        P(("dp", "sp")),
        P("sp"),
        P(),
        P("sp", "tp"),
        P("sp", "tp"),
        P("sp", "tp"),
        P(None, "tp"),
        P(None, "tp"),
        P(None, "tp"),
        P(),
        P(),
        P("tp"),
        P("tp"),
        P(),
        P("tp", None),
    )
    sizes = mesh.shape
    return jax.shard_map(
        functools.partial(on_device, sizes["sp"], sizes["tp"], sizes["dp"]),
        mesh=mesh,
        in_specs=placed,
        out_specs=P(("dp", "sp", "tp"), None),
        check_vma=False,
    )
```

```python
import functools

import jax
import jax.numpy as jnp
import numpy as np
from jax import lax
from jax.experimental import pallas as pl
from jax.experimental.pallas import tpu as pltpu
from jax.sharding import PartitionSpec as P

GRID = 64
token_eps = 0.01
head_eps = 0.001
rope_base = 10000.0
head_factor = 0.8
MESH = pl.DeviceIdType.MESH
BF = jnp.bfloat16
F32 = jnp.float32


def rope_tables(length, width):
    quarter = width // 4
    inverse = (rope_base ** (-np.arange(quarter, dtype=np.float64) / quarter)).astype(np.float32)
    pos = np.arange(length)
    row = (pos // GRID).astype(np.float32)[:, None] * inverse
    col = (pos % GRID).astype(np.float32)[:, None] * inverse
    cos = np.concatenate([np.cos(row), np.cos(row), np.cos(col), np.cos(col)], axis=1)
    sin = np.concatenate([-np.sin(row), np.sin(row), -np.sin(col), np.sin(col)], axis=1)
    return np.tile(cos, (1, 2)).astype(np.float32), np.tile(sin, (1, 2)).astype(np.float32)


def kernel(n_sp, n_tp, n_dp, head_width, *refs):
    (
        lat_h, ctx_h, cond_h, cctx_h, gain_h, ms_h, msc_h, mg_h, wq_h, wk_h, wv_h,
        qg_h, kg_h, vg_h, lam_r, lift_r, wo_h, cos_h, sin_h,
        out_r,
        cond_r, cctx_r, gain_r, qg_r, kg_r, vg_r,
        own, lat, ctx, mw, wq, wkv, wo, turns,
        act, part, mod_in, summed, mod_full, vecs, normed, qown, qin, qm, kvl, kvr, kvc, acc,
        mine, ho, grp,
        loc, s_swap, r_swap, s_lat, r_lat, s_mod, r_mod, s_mt, r_mt, s_vec, r_vec, s_kv, r_kv,
        s_ctx, r_ctx, s_q, r_q, s_wo, r_wo, s_wz, r_wz, s_dd, r_dd, s_ho, r_ho,
    ) = refs
    s = lax.axis_index("sp")
    t = lax.axis_index("tp")
    d_ix = lax.axis_index("dp")
    core = lax.rem(d_ix, 2)
    partner = d_ix + 1 - 2 * core
    t_odd = lax.rem(t, 2)
    nbr1 = t + 1 - 2 * t_odd
    nbr2 = lax.rem(t + 2, 4)
    nbr3 = lax.rem(nbr1 + 2, 4)
    peers = (t, nbr1, nbr2, nbr3)
    H = n_sp // 2
    half = s // H
    base = half * H
    s_opp = lax.rem(s + H, n_sp)
    home = core == half
    away = jnp.not_equal(core, half)
    a = lax.rem(core + half, 2)
    block = s + a * (s_opp - s)
    other_block = s_opp + a * (s - s_opp)
    d_work = d_ix - core + half
    e = lax.rem(s, 2)
    level = s + 1 - 2 * e
    R, D = own.shape
    PR = R // 4
    C = ctx.shape[0]
    QW = wq.shape[1]
    n_head = QW // (2 * head_width)
    HW = 2 * head_width
    VW = wkv.shape[2] // n_head
    ROWS = 4 * R

    bar = pltpu.get_barrier_semaphore()
    greeted = [{"tp": peers[k]} for k in range(1, 4)] + [{"dp": partner}]
    for k in range(1, n_sp):
        there = lax.rem(s + k, n_sp)
        greeted += [{"sp": there}, {"dp": partner, "sp": there}]
    for where in greeted:
        pl.semaphore_signal(bar, inc=1, device_id=where, device_id_type=MESH)

    def local(i, src, dst):
        c = pltpu.make_async_copy(src, dst, loc.at[i])
        c.start()
        return c

    def remote(src, dst, ss, rs, where):
        return pltpu.make_async_remote_copy(
            src_ref=src, dst_ref=dst, send_sem=ss, recv_sem=rs, device_id=where, device_id_type=MESH
        )

    def drain(ref, sem):
        remote(ref, ref, sem, sem, {"dp": partner}).wait_recv()

    @pl.when(home)
    def _():
        local(0, lat_h, lat.at[0])

    @pl.when(away)
    def _():
        local(0, lat_h, own)

    l_one = [local(1, cond_h, cond_r), local(2, cctx_h, cctx_r)]
    for j, h in enumerate((ms_h, msc_h, mg_h)):
        local(3, h, mw.at[j])

    act[...] = jnp.zeros_like(act)
    for row, ref in ((0, cond_r), (1, cctx_r)):
        l_one[row].wait()
        v = ref[...].astype(F32).reshape(1, -1)
        act[row : row + 1, :] = v / (1.0 + jnp.exp(-v))
    acts = act[...].astype(BF)
    part[...] = jnp.zeros_like(part)
    drain(mw, loc.at[3])
    l_wo = local(12, wo_h, wo.at[0])
    for j in range(3):
        res = jnp.dot(acts, mw[j], preferred_element_type=F32)
        part[2 * j : 2 * j + 2, :] = res[0:2]

    drain(own, loc.at[0])
    pl.semaphore_wait(bar, len(greeted))

    def mod_copy(k):
        return remote(part, mod_in.at[k - 1], s_mod, r_mod, {"sp": lax.rem(s + k, n_sp)})

    def piece(j):
        return pl.ds(j * PR, PR)

    def swap(j):
        return remote(own.at[piece(j)], lat.at[0, piece(j)], s_swap, r_swap.at[j],
                      {"dp": partner, "sp": s_opp})

    def along_x(j):
        return remote(lat.at[0, piece(j)], lat.at[1, piece(j)], s_lat, r_lat.at[j if j < 2 else 4],
                      {"tp": nbr1})

    def along_y(j):
        return remote(lat.at[0, piece(j)], lat.at[2, piece(j)], s_lat, r_lat.at[j if j > 1 else 4],
                      {"tp": nbr2})

    def onward(j):
        slot, where = (1, nbr2) if j < 2 else (2, nbr1)
        return remote(lat.at[slot, piece(j)], lat.at[3, piece(j)], s_lat, r_lat.at[5], {"tp": where})

    def pass_on(j):
        (along_x(j) if j < 2 else along_y(j)).wait_recv()
        onward(j).start()

    HALF = wo.shape[1] // 2
    QUART = HALF // 2
    SH = QUART // 4

    def wo_rows(at, count):
        return pl.ds(pl.multiple_of(core * HALF + at, SH), count)

    def wo_copy(i, src_slot, dst_slot, at, count, where):
        rows = wo_rows(at, count)
        return remote(wo.at[src_slot, rows], wo.at[dst_slot, rows], s_wo, r_wo.at[i], {"tp": where})

    def wz_copy(k, q):
        rows = wo_rows(q * QUART + (QUART - SH) * e, SH)
        return remote(wo.at[k, rows], wo.at[k, rows], s_wz, r_wz.at[k - 1], {"sp": level})

    def dd_copy(k, at, count):
        rows = wo_rows(at, count)
        return remote(wo.at[k, rows], wo.at[k, rows], s_dd, r_dd.at[k - 1], {"dp": partner})

    def lead(i, src, dst, q, where):
        return wo_copy(i, src, dst, q * QUART + (QUART - SH) * e, SH, where)

    def rest(i, src, dst, q, where):
        return wo_copy(i, src, dst, q * QUART + SH, QUART - 2 * SH, where)

    lead_x = [lead(0, 0, 1, 0, nbr1), lead(2, 0, 1, 1, nbr1)]
    lead_y = [lead(2, 0, 2, 0, nbr2), lead(1, 0, 2, 1, nbr2)]
    lead_f = [lead(6, 1, 3, 0, nbr2), lead(6, 2, 3, 1, nbr1)]
    rest_x = [rest(3, 0, 1, 0, nbr1), rest(5, 0, 1, 1, nbr1)]
    rest_y = [rest(5, 0, 2, 0, nbr2), rest(4, 0, 2, 1, nbr2)]
    rest_f = [rest(7, 1, 3, 0, nbr2), rest(8, 2, 3, 1, nbr1)]

    def start(*copies):
        for c in copies:
            c.start()

    def share_first():
        lead_x[0].wait_recv()
        wz_copy(1, 0).start()
        lead_y[1].wait_recv()
        wz_copy(2, 1).start()

    def share_second():
        drain(wo.at[1, pl.ds(0, 2 * SH)], r_wo.at[2])
        wz_copy(1, 1).start()
        wz_copy(2, 0).start()

    def share_far():
        wz_copy(3, 0).start()
        wz_copy(3, 1).start()

    def pass_rest():
        rest_x[0].wait_recv()
        rest_f[0].start()
        rest_y[1].wait_recv()
        rest_f[1].start()

    near_leads = (lead_x[0], lead_y[1], lead_x[1], lead_y[0])
    near_rests = (rest_x[0], rest_y[1], rest_x[1], rest_y[0])

    for k in range(1, n_sp):
        mod_copy(k).start()

    @pl.when(home)
    def _():
        for j in range(4):
            along_x(j).start()
            along_y((j + 2) % 4).start()

    @pl.when(away)
    def _():
        for j in range(4):
            swap(j).start()

    l_ctx = local(4, ctx_h, ctx)
    local(5, wk_h, wkv.at[0])
    local(5, wv_h, wkv.at[1])
    at_turns = pl.ds(pl.multiple_of(block * ROWS, ROWS), ROWS)
    local(6, cos_h.at[at_turns], turns.at[0])
    local(6, sin_h.at[at_turns], turns.at[1])
    l_small = [
        local(7 + j, src, dst)
        for j, (src, dst) in enumerate(((gain_h, gain_r), (qg_h, qg_r), (kg_h, kg_r), (vg_h, vg_r)))
    ]
    l_wq = local(11, wq_h, wq)

    l_wo.wait()

    @pl.when(away)
    def _():
        start(*near_leads)

    group = (
        lax.rem(lax.broadcasted_iota(jnp.int32, (2 * QW, QW), 0), QW) // head_width
        == lax.broadcasted_iota(jnp.int32, (2 * QW, QW), 1) // head_width
    )
    grp[...] = jnp.where(group, 1.0 / head_width, 0.0).astype(BF)
    for c in l_small:
        c.wait()
    gain = gain_r[...].reshape(1, -1)
    q_gain = qg_r[...].reshape(1, -1)
    q_gain = jnp.concatenate([q_gain, q_gain], axis=1)
    k_gain = kg_r[...].reshape(1, -1)
    k_gain = jnp.concatenate([k_gain, k_gain], axis=1)
    v_gain = vg_r[...].reshape(1, -1)

    drain(mod_in, r_mod)
    total = part[...]
    for k in range(n_sp - 1):
        total = total + mod_in[k]
    summed[...] = total
    mod_full[t] = total

    def mt_copy(k):
        return remote(summed, mod_full.at[t], s_mt, r_mt, {"tp": peers[k]})

    for k in range(1, 4):
        mt_copy(k).start()

    @pl.when(home)
    def _():
        for j in (0, 2, 1, 3):
            pass_on(j)
        start(*near_leads)

    @pl.when(away)
    def _():
        for j in range(4):
            swap(j).wait_recv()
            along_x(j).start()
            along_y(j).start()
            if j == 1:
                share_first()
                share_second()
        pass_on(0)
        pass_on(1)

    drain(mod_full.at[0:3], r_mt)

    def full_row(j):
        return jnp.concatenate([mod_full[q, j : j + 1, :] for q in range(n_tp)], axis=1)

    vecs[0, 0:1, :] = full_row(0)
    vecs[0, 1:2, :] = full_row(1)
    vecs[0, 2:3, :] = gain * (1.0 + full_row(2))
    vecs[0, 3:4, :] = gain * (1.0 + full_row(3))
    vecs[0, 4:8, :] = jnp.broadcast_to(full_row(4), (4, D))
    vec_copy = remote(vecs.at[0], vecs.at[1], s_vec, r_vec, {"dp": partner})

    @pl.when(home)
    def _():
        vec_copy.start()

    def norm_rows(src, row, count, dst_at, slot):
        step = 16

        @pl.loop(0, count // step, unroll=True)
        def _(i):
            at = pl.multiple_of(i * step, step)
            v = src[pl.ds(at, step), :].astype(F32)
            inv = lax.rsqrt(jnp.mean(v * v, axis=-1, keepdims=True) + token_eps)
            normed[pl.ds(dst_at + at, step), :] = (
                v * inv * vecs[slot, 2 + row : 3 + row, :] + vecs[slot, row : row + 1, :]
            ).astype(BF)

    def head_norm(x):
        square = x * x
        high = square.astype(BF)
        low = (square - high.astype(F32)).astype(BF)
        mean = jnp.dot(jnp.concatenate([high, low], axis=1), grp[...], preferred_element_type=F32)
        return x * lax.rsqrt(mean + token_eps)

    def turn(y, cos, sin):
        lane = lax.broadcasted_iota(jnp.int32, y.shape, 1)
        front = lax.rem(lane, head_width // 2) < head_width // 4
        other = jnp.where(
            front,
            pltpu.roll(y, HW - head_width // 4, axis=1),
            pltpu.roll(y, head_width // 4, axis=1),
        )
        return y * cos + other * sin

    def turns_of(k):
        at = pl.ds(pl.multiple_of(peers[k] * R, R), R)
        return turns[0, at, :], turns[1, at, :]

    def project(first, count, plain):
        x = normed[first : first + count, :]
        kk = head_norm(jnp.dot(x, wkv[0], preferred_element_type=F32))
        for h in range(n_head):
            y = kk[:, h * HW : (h + 1) * HW] * k_gain
            if plain:
                kvl[h, first : first + plain, 0:HW] = y[:plain].astype(BF)
            for at in range(plain, count, R):
                kvl[h, first + at : first + at + R, 0:HW] = turn(
                    y[at : at + R], *turns_of((first + at - C) // R)
                ).astype(BF)
        vv = jnp.dot(x, wkv[1], preferred_element_type=F32).astype(BF)
        for h in range(n_head):
            kvl[h, first : first + count, HW:] = vv[:, h * VW : (h + 1) * VW]

    def project_queries(first, last):
        x = normed[C + first * R : C + last * R, :]
        qq = head_norm(jnp.dot(x, wq[...], preferred_element_type=F32))
        for k in range(first, last):
            for h in range(n_head):
                y = qq[(k - first) * R : (k - first + 1) * R, h * HW : (h + 1) * HW] * q_gain
                qown[h, k * R : (k + 1) * R, :] = (
                    turn(y, *turns_of(k)) * (head_width ** -0.5)
                ).astype(BF)

    def split_maps(q, at):
        lane = lax.broadcasted_iota(jnp.int32, q.shape, 1)
        for m in range(2):
            qm[m, at : at + ROWS, :] = jnp.where(lane // head_width == m, q, jnp.zeros_like(q))

    def kv_copy(j, head, at, count):
        there = base + lax.rem(s - base + j, H)
        i = 2 * j + a
        return remote(kvl.at[head, pl.ds(C + at, count)], kvr.at[block, pl.ds(at, count)], s_kv,
                      r_kv.at[i], {"dp": d_ix - core + head, "sp": there})

    def send_block(at, count):
        for j in range(1, H):
            for head in range(2):
                kv_copy(j, head, at, count).start()
        kv_copy(0, 1 - core, at, count).start()

    def ctx_copy(there, head):
        at = pl.ds(pl.multiple_of(s * C, C), C)
        return remote(kvl.at[head, pl.ds(0, C)], kvc.at[at], s_ctx, r_ctx,
                      {"dp": d_ix - core + head, "sp": there})

    def send_ctx():
        @pl.when(home)
        def _():
            for j in range(1, H):
                for head in range(2):
                    ctx_copy(base + lax.rem(s - base + j, H), head).start()
            ctx_copy(s, 1 - core).start()
            kvc[pl.ds(pl.multiple_of(s * C, C), C), :] = kvl[core, 0:C, :]

        @pl.when(away)
        def _():
            for j in range(H):
                for head in range(2):
                    ctx_copy(lax.rem(s_opp + j, H) + H - base, head).start()

    l_ctx.wait()
    norm_rows(ctx, 1, C, 0, 0)
    drain(wkv, loc.at[5])
    drain(turns, loc.at[6])

    @pl.when(home)
    def _():
        norm_rows(lat.at[0], 0, R, C, 0)
        project(0, C + R, C)
        send_block(0, R)
        send_ctx()
        drain(lat.at[1], r_lat.at[4])
        norm_rows(lat.at[1], 0, R, C + R, 0)
        norm_rows(lat.at[2], 0, R, C + 2 * R, 0)
        project(C + R, 2 * R, 0)
        send_block(R, 2 * R)

    @pl.when(away)
    def _():
        project(0, C, C)
        send_ctx()
        pass_on(2)
        pass_on(3)
        start(*lead_f, *near_rests)
        vec_copy.wait_recv()
        norm_rows(lat.at[0], 0, R, C, 1)
        drain(lat.at[1], r_lat.at[4])
        norm_rows(lat.at[1], 0, R, C + R, 1)
        norm_rows(lat.at[2], 0, R, C + 2 * R, 1)
        project(C, 3 * R, 0)
        send_block(0, 3 * R)

    l_wq.wait()
    project_queries(0, 3)
    drain(lat.at[3], r_lat.at[5])
    norm_rows(lat.at[3], 0, R, C + 3 * R, a)
    project(C + 3 * R, R, 0)
    send_block(3 * R, R)

    project_queries(3, 4)
    q_copy = remote(qown.at[1 - core], qin, s_q, r_q, {"dp": partner})
    q_copy.start()
    split_maps(qown[core], 0)

    QB = 2 * R
    lift = lift_r[core]

    def attend(block, at, keys, start_row, count, first, plus):
        k = block[at : at + keys, 0:HW]
        v = block[at : at + keys, HW:]
        vx = jnp.concatenate([v, jnp.ones_like(v)], axis=1)
        for m in range(2):
            for b in range(count // QB):
                rows = slice(start_row + b * QB, start_row + (b + 1) * QB)
                sc = lax.dot_general(
                    qm[m, rows, :], k, (((1,), (1,)), ((), ())), preferred_element_type=F32
                )
                if plus is not None:
                    sc = sc + plus
                p = jnp.exp(sc).astype(BF)
                add = jnp.dot(p, vx, preferred_element_type=F32)
                if first:
                    acc[m, rows, :] = add
                else:
                    acc[m, rows, :] += add

    @pl.when(home)
    def _():
        share_first()
        start(*lead_f)

    @pl.when(jnp.logical_and(home, core == 0))
    def _():
        start(*near_rests)

    attend(kvl.at[core], C, ROWS, 0, ROWS, True, None)

    @pl.when(jnp.logical_and(home, core == 1))
    def _():
        drain(wo.at[3, pl.ds(0, 2 * SH)], r_wo.at[6])
        start(*near_rests)

    q_copy.wait_recv()
    split_maps(qin[...], ROWS)
    attend(kvl.at[core], C, ROWS, ROWS, ROWS, True, None)

    pass_rest()

    @pl.when(home)
    def _():
        share_second()

    @pl.when(jnp.logical_or(away, core == 0))
    def _():
        drain(wo.at[3, pl.ds(0, 2 * SH)], r_wo.at[6])

    share_far()

    def attend_block(slot, i):
        drain(kvr.at[slot], r_kv.at[i])
        attend(kvr.at[slot], 0, ROWS, 0, 2 * ROWS, False, None)

    for j in range(1, H):
        attend_block(base + lax.rem(s - base + H - j, H), 2 * j)

    @pl.when(home)
    def _():
        drain(kvc.at[pl.ds(0, (n_sp - 1) * C)], r_ctx)

    @pl.when(away)
    def _():
        drain(kvc, r_ctx)

    attend(kvc, 0, n_sp * C, 0, 2 * ROWS, False, lift)
    attend_block(other_block, 1 - a)
    for j in range(1, H):
        attend_block(lax.rem(base + lax.rem(s - base + H - j, H) + H, n_sp), 2 * j + 1)

    def ho_copy(q, k):
        lanes = pl.ds(pl.multiple_of(k * n_head * VW + core * VW, VW), VW)
        return remote(mine.at[q, pl.ds(k * R, R)], ho.at[:, lanes], s_ho, r_ho.at[k],
                      {"dp": d_work, "sp": block + q * (other_block - block), "tp": peers[k]})

    for q in (1 - a, a):
        rows = pl.ds(pl.multiple_of(q * ROWS, ROWS), ROWS)
        a0 = acc[0, rows, :]
        a1 = acc[1, rows, :]
        mixed = a0[:, :VW] / a0[:, VW:] - lam_r[core] * (a1[:, :VW] / a1[:, VW:])
        inv = lax.rsqrt(jnp.mean(mixed * mixed, axis=-1, keepdims=True) + head_eps)
        mine[q, :, :] = (mixed * inv * v_gain * head_factor).astype(BF)
        for k in (3, 1, 2):
            ho_copy(q, k).start()
        if q is not a:
            ho_copy(q, 0).start()

    @pl.when(away)
    def _():
        ho_copy(a, 0).start()

    for h in range(2):
        @pl.when(jnp.logical_and(home, core == h))
        def _():
            ho[:, h * VW : (h + 1) * VW] = mine[0, 0:R, :]

    drain(wo.at[1, pl.ds(0, 2 * (QUART - 2 * SH))], r_wo.at[5])
    for k in range(1, 3):
        drain(wo.at[k, pl.ds(0, 2 * SH)], r_wz.at[k - 1])
        dd_copy(k, 0, HALF).start()
    drain(wo.at[3, pl.ds(0, 2 * SH)], r_wz.at[2])
    for q in range(2):
        dd_copy(3, q * QUART, SH).start()
        dd_copy(3, (q + 1) * QUART - SH, SH).start()
    for q in range(2):
        rest_f[q].wait_recv()
        dd_copy(3, q * QUART + SH, QUART - 2 * SH).start()

    for k in range(1, 4):
        drain(wo.at[k, pl.ds(0, HALF)], r_dd.at[k - 1])
        drain(mine.at[0, pl.ds(0, 2 * R)], r_ho.at[k])

    @pl.when(home)
    def _():
        drain(mine.at[0, pl.ds(0, R)], r_ho.at[0])

    @pl.when(away)
    def _():
        drain(mine.at[0, pl.ds(0, 2 * R)], r_ho.at[0])

    weights = wo[...].reshape(-1, D)
    out_r[...] = vecs[0, 4:5, :] * jnp.dot(ho[...], weights, preferred_element_type=F32)

    def sent(ref, sem):
        remote(ref, ref, sem, sem, {"dp": partner}).wait_send()

    sent(mod_in, s_mod)
    sent(mod_full.at[0:3], s_mt)
    sent(lat.at[0:3], s_lat)
    sent(kvr.at[0 : n_sp - 1], s_kv)
    sent(wo.at[0:3, pl.ds(0, 2 * (QUART - SH))], s_wo)
    sent(wo.at[0:3, pl.ds(0, 2 * SH)], s_wz)
    sent(wo.at[0:3, pl.ds(0, HALF)], s_dd)
    q_copy.wait_send()

    @pl.when(home)
    def _():
        vec_copy.wait_send()
        sent(kvc.at[pl.ds(0, (n_sp - 1) * C)], s_ctx)
        sent(qm.at[0, pl.ds(0, 7 * R)], s_ho)

    @pl.when(away)
    def _():
        sent(own, s_swap)
        sent(kvc, s_ctx)
        sent(mine, s_ho)


def on_device(n_sp, n_tp, n_dp, *args):
    (
        latent, context, cond, context_cond, norm_gain, mod_shift, mod_scale, mod_gate,
        w_query, w_key, w_value, query_gain, key_gain, mix_lambda, context_lift, value_gain, w_out,
    ) = args
    R, D = latent.shape
    C = context.shape[0]
    head_width = query_gain.shape[0]
    cos, sin = rope_tables(R * n_sp * n_tp, head_width)
    QW, VWALL = w_query.shape[1], w_value.shape[1]
    heads = mix_lambda.shape[0]
    ROWS = R * n_tp
    HW = 2 * head_width
    KV = (QW + VWALL) // heads
    MC = mod_shift.shape[1]
    vm = pl.BlockSpec(memory_space=pltpu.VMEM)
    anywhere = pl.BlockSpec(memory_space=pl.ANY)
    smem = pl.BlockSpec(memory_space=pltpu.SMEM)
    dma = pltpu.SemaphoreType.DMA
    update = pl.pallas_call(
        functools.partial(kernel, n_sp, n_tp, n_dp, head_width),
        out_shape=pltpu.VMEM((R, D), F32),
        in_specs=[anywhere] * 14 + [smem, smem]
        + [anywhere] * 3,
        out_specs=vm,
        scratch_shapes=[
            pltpu.VMEM(cond.shape, BF),
            pltpu.VMEM(context_cond.shape, BF),
            pltpu.VMEM(norm_gain.shape, F32),
            pltpu.VMEM(query_gain.shape, F32),
            pltpu.VMEM(key_gain.shape, F32),
            pltpu.VMEM(value_gain.shape, F32),
            pltpu.VMEM((R, D), BF),
            pltpu.VMEM((4, R, D), BF),
            pltpu.VMEM((C, D), BF),
            pltpu.VMEM((3,) + mod_shift.shape, BF),
            pltpu.VMEM(w_query.shape, BF),
            pltpu.VMEM((2,) + w_key.shape, BF),
            pltpu.VMEM((4,) + w_out.shape, BF),
            pltpu.VMEM((2, ROWS, HW), F32),
            pltpu.VMEM((8, mod_shift.shape[0]), F32),
            pltpu.VMEM((8, MC), F32),
            pltpu.VMEM((n_sp - 1, 8, MC), F32),
            pltpu.VMEM((8, MC), F32),
            pltpu.VMEM((n_tp, 8, MC), F32),
            pltpu.VMEM((2, 8, D), F32),
            pltpu.VMEM((C + ROWS, D), BF),
            pltpu.VMEM((heads, ROWS, HW), BF),
            pltpu.VMEM((ROWS, HW), BF),
            pltpu.VMEM((2, 2 * ROWS, HW), BF),
            pltpu.VMEM((heads, C + ROWS, KV), BF),
            pltpu.VMEM((n_sp, ROWS, KV), BF),
            pltpu.VMEM((n_sp * C, KV), BF),
            pltpu.VMEM((2, 2 * ROWS, 2 * VWALL // heads), F32),
            pltpu.VMEM((2, ROWS, VWALL // heads), BF),
            pltpu.VMEM((R, n_tp * VWALL), BF),
            pltpu.VMEM((2 * QW, QW), BF),
            dma((13,)),
            dma(()), dma((4,)),
            dma(()), dma((6,)),
            dma(()), dma(()),
            dma(()), dma(()),
            dma(()), dma(()),
            dma(()), dma((n_sp,)),
            dma(()), dma(()),
            dma(()), dma(()),
            dma(()), dma((9,)),
            dma(()), dma((3,)),
            dma(()), dma((3,)),
            dma(()), dma((4,)),
        ],
        compiler_params=pltpu.CompilerParams(
            collective_id=0, has_side_effects=True, vmem_limit_bytes=66_100_000
        ),
        name="block",
    )(
        latent, context, cond, context_cond, norm_gain, mod_shift, mod_scale,
        mod_gate, w_query, w_key, w_value, query_gain, key_gain, value_gain, mix_lambda, context_lift, w_out,
        jnp.asarray(cos), jnp.asarray(sin),
    )
    return (latent.astype(F32) + update).astype(latent.dtype)


def solution(mesh):
    placed = (
        P(("dp", "sp", "tp"), None),
        P(("dp", "sp"), None),
        P(("dp", "sp")),
        P("sp"),
        P(),
        P("sp", "tp"),
        P("sp", "tp"),
        P("sp", "tp"),
        P(None, "tp"),
        P(None, "tp"),
        P(None, "tp"),
        P(),
        P(),
        P("tp"),
        P("tp"),
        P(),
        P("tp", None),
    )
    sizes = mesh.shape
    return jax.shard_map(
        functools.partial(on_device, sizes["sp"], sizes["tp"], sizes["dp"]),
        mesh=mesh,
        in_specs=placed,
        out_specs=P(("dp", "sp", "tp"), None),
        check_vma=False,
    )
```

```python
import functools

import jax
import jax.numpy as jnp
import numpy as np
from jax import lax
from jax.experimental import pallas as pl
from jax.experimental.pallas import tpu as pltpu
from jax.sharding import PartitionSpec as P

GRID = 64
token_eps = 0.01
head_eps = 0.001
rope_base = 10000.0
head_factor = 0.8
MESH = pl.DeviceIdType.MESH
BF = jnp.bfloat16
F32 = jnp.float32


def rope_tables(length, width):
    quarter = width // 4
    inverse = (rope_base ** (-np.arange(quarter, dtype=np.float64) / quarter)).astype(np.float32)
    pos = np.arange(length)
    row = (pos // GRID).astype(np.float32)[:, None] * inverse
    col = (pos % GRID).astype(np.float32)[:, None] * inverse
    cos = np.concatenate([np.cos(row), np.cos(row), np.cos(col), np.cos(col)], axis=1)
    sin = np.concatenate([-np.sin(row), np.sin(row), -np.sin(col), np.sin(col)], axis=1)
    return np.tile(cos, (1, 2)).astype(np.float32), np.tile(sin, (1, 2)).astype(np.float32)


def kernel(n_sp, n_tp, n_dp, head_width, *refs):
    (
        lat_h, ctx_h, cond_h, cctx_h, gain_h, ms_h, msc_h, mg_h, wq_h, wk_h, wv_h,
        qg_h, kg_h, vg_h, lam_r, lift_r, wo_h, cos_h, sin_h,
        out_r,
        cond_r, cctx_r, gain_r, qg_r, kg_r, vg_r,
        own, lat, ctx, mw, wq, wkv, wo, turns,
        act, part, mod_in, summed, mod_full, vecs, normed, qown, qin, qm, kvl, kvr, kvc, acc,
        mine, ho, grp,
        loc, s_swap, r_swap, s_lat, r_lat, s_mod, r_mod, s_mt, r_mt, s_vec, r_vec, s_kv, r_kv,
        s_ctx, r_ctx, s_q, r_q, s_wo, r_wo, s_wz, r_wz, s_dd, r_dd, s_ho, r_ho,
    ) = refs
    s = lax.axis_index("sp")
    t = lax.axis_index("tp")
    d_ix = lax.axis_index("dp")
    core = lax.rem(d_ix, 2)
    partner = d_ix + 1 - 2 * core
    t_odd = lax.rem(t, 2)
    nbr1 = t + 1 - 2 * t_odd
    nbr2 = lax.rem(t + 2, 4)
    nbr3 = lax.rem(nbr1 + 2, 4)
    peers = (t, nbr1, nbr2, nbr3)
    H = n_sp // 2
    half = s // H
    base = half * H
    s_opp = lax.rem(s + H, n_sp)
    home = core == half
    away = jnp.not_equal(core, half)
    a = lax.rem(core + half, 2)
    block = s + a * (s_opp - s)
    other_block = s_opp + a * (s - s_opp)
    d_work = d_ix - core + half
    e = lax.rem(s, 2)
    level = s + 1 - 2 * e
    R, D = own.shape
    PR = R // 4
    C = ctx.shape[0]
    QW = wq.shape[1]
    n_head = QW // (2 * head_width)
    HW = 2 * head_width
    VW = wkv.shape[2] // n_head
    ROWS = 4 * R

    bar = pltpu.get_barrier_semaphore()
    greeted = [{"tp": peers[k]} for k in range(1, 4)] + [{"dp": partner}]
    for k in range(1, n_sp):
        there = lax.rem(s + k, n_sp)
        greeted += [{"sp": there}, {"dp": partner, "sp": there}]
    for where in greeted:
        pl.semaphore_signal(bar, inc=1, device_id=where, device_id_type=MESH)

    def local(i, src, dst):
        c = pltpu.make_async_copy(src, dst, loc.at[i])
        c.start()
        return c

    def remote(src, dst, ss, rs, where):
        return pltpu.make_async_remote_copy(
            src_ref=src, dst_ref=dst, send_sem=ss, recv_sem=rs, device_id=where, device_id_type=MESH
        )

    def drain(ref, sem):
        remote(ref, ref, sem, sem, {"dp": partner}).wait_recv()

    @pl.when(home)
    def _():
        local(0, lat_h, lat.at[0])

    @pl.when(away)
    def _():
        local(0, lat_h, own)

    l_one = [local(1, cond_h, cond_r), local(2, cctx_h, cctx_r)]
    for j, h in enumerate((ms_h, msc_h, mg_h)):
        local(3, h, mw.at[j])

    act[...] = jnp.zeros_like(act)
    for row, ref in ((0, cond_r), (1, cctx_r)):
        l_one[row].wait()
        v = ref[...].astype(F32).reshape(1, -1)
        act[row : row + 1, :] = v / (1.0 + jnp.exp(-v))
    acts = act[...].astype(BF)
    part[...] = jnp.zeros_like(part)
    drain(mw, loc.at[3])
    l_wo = local(12, wo_h, wo.at[0])
    for j in range(3):
        res = jnp.dot(acts, mw[j], preferred_element_type=F32)
        part[2 * j : 2 * j + 2, :] = res[0:2]

    drain(own, loc.at[0])
    pl.semaphore_wait(bar, len(greeted))

    def mod_copy(k):
        return remote(part, mod_in.at[k - 1], s_mod, r_mod, {"sp": lax.rem(s + k, n_sp)})

    def piece(j):
        return pl.ds(j * PR, PR)

    def swap(j):
        return remote(own.at[piece(j)], lat.at[0, piece(j)], s_swap, r_swap.at[j],
                      {"dp": partner, "sp": s_opp})

    def along_x(j):
        return remote(lat.at[0, piece(j)], lat.at[1, piece(j)], s_lat, r_lat.at[j if j < 2 else 4],
                      {"tp": nbr1})

    def along_y(j):
        return remote(lat.at[0, piece(j)], lat.at[2, piece(j)], s_lat, r_lat.at[j if j > 1 else 4],
                      {"tp": nbr2})

    def onward(j):
        slot, where = (1, nbr2) if j < 2 else (2, nbr1)
        return remote(lat.at[slot, piece(j)], lat.at[3, piece(j)], s_lat, r_lat.at[5], {"tp": where})

    def pass_on(j):
        (along_x(j) if j < 2 else along_y(j)).wait_recv()
        onward(j).start()

    HALF = wo.shape[1] // 2
    QUART = HALF // 2
    SH = QUART // 4

    def wo_rows(at, count):
        return pl.ds(pl.multiple_of(core * HALF + at, SH), count)

    def wo_copy(i, src_slot, dst_slot, at, count, where):
        rows = wo_rows(at, count)
        return remote(wo.at[src_slot, rows], wo.at[dst_slot, rows], s_wo, r_wo.at[i], {"tp": where})

    def wz_copy(k, q):
        rows = wo_rows(q * QUART + (QUART - SH) * e, SH)
        return remote(wo.at[k, rows], wo.at[k, rows], s_wz, r_wz.at[k - 1], {"sp": level})

    def dd_copy(k, at, count):
        rows = wo_rows(at, count)
        return remote(wo.at[k, rows], wo.at[k, rows], s_dd, r_dd.at[k - 1], {"dp": partner})

    def lead(i, src, dst, q, where):
        return wo_copy(i, src, dst, q * QUART + (QUART - SH) * e, SH, where)

    def rest(i, src, dst, q, where):
        return wo_copy(i, src, dst, q * QUART + SH, QUART - 2 * SH, where)

    lead_x = [lead(0, 0, 1, 0, nbr1), lead(2, 0, 1, 1, nbr1)]
    lead_y = [lead(2, 0, 2, 0, nbr2), lead(1, 0, 2, 1, nbr2)]
    lead_f = [lead(6, 1, 3, 0, nbr2), lead(6, 2, 3, 1, nbr1)]
    rest_x = [rest(3, 0, 1, 0, nbr1), rest(5, 0, 1, 1, nbr1)]
    rest_y = [rest(5, 0, 2, 0, nbr2), rest(4, 0, 2, 1, nbr2)]
    rest_f = [rest(7, 1, 3, 0, nbr2), rest(8, 2, 3, 1, nbr1)]

    def start(*copies):
        for c in copies:
            c.start()

    def share_first():
        lead_x[0].wait_recv()
        wz_copy(1, 0).start()
        lead_y[1].wait_recv()
        wz_copy(2, 1).start()

    def share_second():
        drain(wo.at[1, pl.ds(0, 2 * SH)], r_wo.at[2])
        wz_copy(1, 1).start()
        wz_copy(2, 0).start()

    def share_far():
        wz_copy(3, 0).start()
        wz_copy(3, 1).start()

    def pass_rest():
        rest_x[0].wait_recv()
        rest_f[0].start()
        rest_y[1].wait_recv()
        rest_f[1].start()

    near_leads = (lead_x[0], lead_y[1], lead_x[1], lead_y[0])
    near_rests = (rest_x[0], rest_y[1], rest_x[1], rest_y[0])

    for k in range(1, n_sp):
        mod_copy(k).start()

    @pl.when(home)
    def _():
        for j in range(4):
            along_x(j).start()
            along_y((j + 2) % 4).start()

    @pl.when(away)
    def _():
        for j in range(4):
            swap(j).start()

    l_ctx = local(4, ctx_h, ctx)
    local(5, wk_h, wkv.at[0])
    local(5, wv_h, wkv.at[1])
    at_turns = pl.ds(pl.multiple_of(block * ROWS, ROWS), ROWS)
    local(6, cos_h.at[at_turns], turns.at[0])
    local(6, sin_h.at[at_turns], turns.at[1])
    l_small = [
        local(7 + j, src, dst)
        for j, (src, dst) in enumerate(((gain_h, gain_r), (qg_h, qg_r), (kg_h, kg_r), (vg_h, vg_r)))
    ]
    l_wq = local(11, wq_h, wq)

    l_wo.wait()

    @pl.when(away)
    def _():
        start(*near_leads)

    group = (
        lax.rem(lax.broadcasted_iota(jnp.int32, (2 * QW, QW), 0), QW) // head_width
        == lax.broadcasted_iota(jnp.int32, (2 * QW, QW), 1) // head_width
    )
    grp[...] = jnp.where(group, 1.0 / head_width, 0.0).astype(BF)
    for c in l_small:
        c.wait()
    gain = gain_r[...].reshape(1, -1)
    q_gain = qg_r[...].reshape(1, -1)
    q_gain = jnp.concatenate([q_gain, q_gain], axis=1)
    k_gain = kg_r[...].reshape(1, -1)
    k_gain = jnp.concatenate([k_gain, k_gain], axis=1)
    v_gain = vg_r[...].reshape(1, -1)

    drain(mod_in, r_mod)
    total = part[...]
    for k in range(n_sp - 1):
        total = total + mod_in[k]
    summed[...] = total
    mod_full[t] = total

    def mt_copy(k):
        return remote(summed, mod_full.at[t], s_mt, r_mt, {"tp": peers[k]})

    for k in range(1, 4):
        mt_copy(k).start()

    @pl.when(home)
    def _():
        for j in (0, 2, 1, 3):
            pass_on(j)

    @pl.when(jnp.logical_and(home, core == 1))
    def _():
        start(*near_leads)

    @pl.when(away)
    def _():
        for j in range(4):
            swap(j).wait_recv()
            along_x(j).start()
            along_y(j).start()
            if j == 1:
                share_first()
                share_second()
        pass_on(0)
        pass_on(1)

    drain(mod_full.at[0:3], r_mt)

    def full_row(j):
        return jnp.concatenate([mod_full[q, j : j + 1, :] for q in range(n_tp)], axis=1)

    vecs[0, 0:1, :] = full_row(0)
    vecs[0, 1:2, :] = full_row(1)
    vecs[0, 2:3, :] = gain * (1.0 + full_row(2))
    vecs[0, 3:4, :] = gain * (1.0 + full_row(3))
    vecs[0, 4:8, :] = jnp.broadcast_to(full_row(4), (4, D))
    vec_copy = remote(vecs.at[0], vecs.at[1], s_vec, r_vec, {"dp": partner})

    @pl.when(home)
    def _():
        vec_copy.start()

    def norm_rows(src, row, count, dst_at, slot):
        step = 16

        @pl.loop(0, count // step, unroll=True)
        def _(i):
            at = pl.multiple_of(i * step, step)
            v = src[pl.ds(at, step), :].astype(F32)
            inv = lax.rsqrt(jnp.mean(v * v, axis=-1, keepdims=True) + token_eps)
            normed[pl.ds(dst_at + at, step), :] = (
                v * inv * vecs[slot, 2 + row : 3 + row, :] + vecs[slot, row : row + 1, :]
            ).astype(BF)

    def head_norm(x):
        square = x * x
        high = square.astype(BF)
        low = (square - high.astype(F32)).astype(BF)
        mean = jnp.dot(jnp.concatenate([high, low], axis=1), grp[...], preferred_element_type=F32)
        return x * lax.rsqrt(mean + token_eps)

    def turn(y, cos, sin):
        lane = lax.broadcasted_iota(jnp.int32, y.shape, 1)
        front = lax.rem(lane, head_width // 2) < head_width // 4
        other = jnp.where(
            front,
            pltpu.roll(y, HW - head_width // 4, axis=1),
            pltpu.roll(y, head_width // 4, axis=1),
        )
        return y * cos + other * sin

    def turns_of(k):
        at = pl.ds(pl.multiple_of(peers[k] * R, R), R)
        return turns[0, at, :], turns[1, at, :]

    def project(first, count, plain):
        x = normed[first : first + count, :]
        kk = head_norm(jnp.dot(x, wkv[0], preferred_element_type=F32))
        for h in range(n_head):
            y = kk[:, h * HW : (h + 1) * HW] * k_gain
            if plain:
                kvl[h, first : first + plain, 0:HW] = y[:plain].astype(BF)
            for at in range(plain, count, R):
                kvl[h, first + at : first + at + R, 0:HW] = turn(
                    y[at : at + R], *turns_of((first + at - C) // R)
                ).astype(BF)
        vv = jnp.dot(x, wkv[1], preferred_element_type=F32).astype(BF)
        for h in range(n_head):
            kvl[h, first : first + count, HW:] = vv[:, h * VW : (h + 1) * VW]

    def project_queries(first, last):
        x = normed[C + first * R : C + last * R, :]
        qq = head_norm(jnp.dot(x, wq[...], preferred_element_type=F32))
        for k in range(first, last):
            for h in range(n_head):
                y = qq[(k - first) * R : (k - first + 1) * R, h * HW : (h + 1) * HW] * q_gain
                qown[h, k * R : (k + 1) * R, :] = (
                    turn(y, *turns_of(k)) * (head_width ** -0.5)
                ).astype(BF)

    def split_maps(q, at):
        lane = lax.broadcasted_iota(jnp.int32, q.shape, 1)
        for m in range(2):
            qm[m, at : at + ROWS, :] = jnp.where(lane // head_width == m, q, jnp.zeros_like(q))

    def kv_copy(j, head, at, count):
        there = base + lax.rem(s - base + j, H)
        i = 2 * j + a
        return remote(kvl.at[head, pl.ds(C + at, count)], kvr.at[block, pl.ds(at, count)], s_kv,
                      r_kv.at[i], {"dp": d_ix - core + head, "sp": there})

    def send_block(at, count):
        for j in range(1, H):
            for head in range(2):
                kv_copy(j, head, at, count).start()
        kv_copy(0, 1 - core, at, count).start()

    def ctx_copy(there, head):
        at = pl.ds(pl.multiple_of(s * C, C), C)
        return remote(kvl.at[head, pl.ds(0, C)], kvc.at[at], s_ctx, r_ctx,
                      {"dp": d_ix - core + head, "sp": there})

    def send_ctx():
        @pl.when(home)
        def _():
            for j in range(1, H):
                for head in range(2):
                    ctx_copy(base + lax.rem(s - base + j, H), head).start()
            ctx_copy(s, 1 - core).start()
            kvc[pl.ds(pl.multiple_of(s * C, C), C), :] = kvl[core, 0:C, :]

        @pl.when(away)
        def _():
            for j in range(H):
                for head in range(2):
                    ctx_copy(lax.rem(s_opp + j, H) + H - base, head).start()

    l_ctx.wait()
    norm_rows(ctx, 1, C, 0, 0)
    drain(wkv, loc.at[5])
    drain(turns, loc.at[6])

    @pl.when(home)
    def _():
        norm_rows(lat.at[0], 0, R, C, 0)
        project(0, C + R, C)
        send_block(0, R)
        send_ctx()
        drain(lat.at[1], r_lat.at[4])
        norm_rows(lat.at[1], 0, R, C + R, 0)
        norm_rows(lat.at[2], 0, R, C + 2 * R, 0)
        project(C + R, 2 * R, 0)
        send_block(R, 2 * R)

    @pl.when(jnp.logical_and(home, core == 0))
    def _():
        start(*near_leads)

    @pl.when(away)
    def _():
        project(0, C, C)
        send_ctx()
        pass_on(2)
        pass_on(3)
        start(*lead_f, *near_rests)
        vec_copy.wait_recv()
        norm_rows(lat.at[0], 0, R, C, 1)
        drain(lat.at[1], r_lat.at[4])
        norm_rows(lat.at[1], 0, R, C + R, 1)
        norm_rows(lat.at[2], 0, R, C + 2 * R, 1)
        project(C, 3 * R, 0)
        send_block(0, 3 * R)

    l_wq.wait()
    project_queries(0, 3)
    drain(lat.at[3], r_lat.at[5])
    norm_rows(lat.at[3], 0, R, C + 3 * R, a)
    project(C + 3 * R, R, 0)
    send_block(3 * R, R)

    project_queries(3, 4)
    q_copy = remote(qown.at[1 - core], qin, s_q, r_q, {"dp": partner})
    q_copy.start()
    split_maps(qown[core], 0)

    QB = 4 * R
    lift = lift_r[core]

    def attend(block, at, keys, start_row, count, first, plus):
        k = block[at : at + keys, 0:HW]
        v = block[at : at + keys, HW:]
        vx = jnp.concatenate([v, jnp.ones_like(v)], axis=1)
        for m in range(2):
            for b in range(count // QB):
                rows = slice(start_row + b * QB, start_row + (b + 1) * QB)
                sc = lax.dot_general(
                    qm[m, rows, :], k, (((1,), (1,)), ((), ())), preferred_element_type=F32
                )
                if plus is not None:
                    sc = sc + plus
                p = jnp.exp(sc).astype(BF)
                add = jnp.dot(p, vx, preferred_element_type=F32)
                if first:
                    acc[m, rows, :] = add
                else:
                    acc[m, rows, :] += add

    @pl.when(home)
    def _():
        share_first()
        start(*lead_f)

    @pl.when(jnp.logical_and(home, core == 0))
    def _():
        start(*near_rests)

    attend(kvl.at[core], C, ROWS, 0, ROWS, True, None)

    @pl.when(jnp.logical_and(home, core == 1))
    def _():
        drain(wo.at[3, pl.ds(0, 2 * SH)], r_wo.at[6])
        start(*near_rests)

    q_copy.wait_recv()
    split_maps(qin[...], ROWS)
    attend(kvl.at[core], C, ROWS, ROWS, ROWS, True, None)

    @pl.when(home)
    def _():
        share_second()

    pass_rest()

    @pl.when(jnp.logical_or(away, core == 0))
    def _():
        drain(wo.at[3, pl.ds(0, 2 * SH)], r_wo.at[6])

    share_far()

    def attend_block(slot, i):
        drain(kvr.at[slot], r_kv.at[i])
        attend(kvr.at[slot], 0, ROWS, 0, 2 * ROWS, False, None)

    for j in range(1, H):
        attend_block(base + lax.rem(s - base + H - j, H), 2 * j)

    @pl.when(home)
    def _():
        drain(kvc.at[pl.ds(0, (n_sp - 1) * C)], r_ctx)

    @pl.when(away)
    def _():
        drain(kvc, r_ctx)

    attend(kvc, 0, n_sp * C, 0, 2 * ROWS, False, lift)
    attend_block(other_block, 1 - a)
    for j in range(1, H):
        attend_block(lax.rem(base + lax.rem(s - base + H - j, H) + H, n_sp), 2 * j + 1)

    def ho_copy(q, k):
        lanes = pl.ds(pl.multiple_of(k * n_head * VW + core * VW, VW), VW)
        return remote(mine.at[q, pl.ds(k * R, R)], ho.at[:, lanes], s_ho, r_ho.at[k],
                      {"dp": d_work, "sp": block + q * (other_block - block), "tp": peers[k]})

    for q in (1 - a, a):
        rows = pl.ds(pl.multiple_of(q * ROWS, ROWS), ROWS)
        a0 = acc[0, rows, :]
        a1 = acc[1, rows, :]
        mixed = a0[:, :VW] / a0[:, VW:] - lam_r[core] * (a1[:, :VW] / a1[:, VW:])
        inv = lax.rsqrt(jnp.mean(mixed * mixed, axis=-1, keepdims=True) + head_eps)
        mine[q, :, :] = (mixed * inv * v_gain * head_factor).astype(BF)
        for k in (3, 1, 2):
            ho_copy(q, k).start()
        if q is not a:
            ho_copy(q, 0).start()

    @pl.when(away)
    def _():
        ho_copy(a, 0).start()

    for h in range(2):
        @pl.when(jnp.logical_and(home, core == h))
        def _():
            ho[:, h * VW : (h + 1) * VW] = mine[0, 0:R, :]

    drain(wo.at[1, pl.ds(0, 2 * (QUART - 2 * SH))], r_wo.at[5])
    for k in range(1, 3):
        drain(wo.at[k, pl.ds(0, 2 * SH)], r_wz.at[k - 1])
        dd_copy(k, 0, HALF).start()
    drain(wo.at[3, pl.ds(0, 2 * SH)], r_wz.at[2])
    for q in range(2):
        dd_copy(3, q * QUART, SH).start()
        dd_copy(3, (q + 1) * QUART - SH, SH).start()
    for q in range(2):
        rest_f[q].wait_recv()
        dd_copy(3, q * QUART + SH, QUART - 2 * SH).start()

    for k in range(1, 4):
        drain(wo.at[k, pl.ds(0, HALF)], r_dd.at[k - 1])
        drain(mine.at[0, pl.ds(0, 2 * R)], r_ho.at[k])

    @pl.when(home)
    def _():
        drain(mine.at[0, pl.ds(0, R)], r_ho.at[0])

    @pl.when(away)
    def _():
        drain(mine.at[0, pl.ds(0, 2 * R)], r_ho.at[0])

    weights = wo[...].reshape(-1, D)
    mixture = vecs[0, 4:5, :] * jnp.dot(ho[...], weights, preferred_element_type=F32)

    @pl.when(home)
    def _():
        out_r[...] = (lat[0].astype(F32) + mixture).astype(BF)

    @pl.when(away)
    def _():
        out_r[...] = (own[...].astype(F32) + mixture).astype(BF)

    def sent(ref, sem):
        remote(ref, ref, sem, sem, {"dp": partner}).wait_send()

    sent(mod_in, s_mod)
    sent(mod_full.at[0:3], s_mt)
    sent(lat.at[0:3], s_lat)
    sent(kvr.at[0 : n_sp - 1], s_kv)
    sent(wo.at[0:3, pl.ds(0, 2 * (QUART - SH))], s_wo)
    sent(wo.at[0:3, pl.ds(0, 2 * SH)], s_wz)
    sent(wo.at[0:3, pl.ds(0, HALF)], s_dd)
    q_copy.wait_send()

    @pl.when(home)
    def _():
        vec_copy.wait_send()
        sent(kvc.at[pl.ds(0, (n_sp - 1) * C)], s_ctx)
        sent(qm.at[0, pl.ds(0, 7 * R)], s_ho)

    @pl.when(away)
    def _():
        sent(own, s_swap)
        sent(kvc, s_ctx)
        sent(mine, s_ho)


def on_device(n_sp, n_tp, n_dp, *args):
    (
        latent, context, cond, context_cond, norm_gain, mod_shift, mod_scale, mod_gate,
        w_query, w_key, w_value, query_gain, key_gain, mix_lambda, context_lift, value_gain, w_out,
    ) = args
    R, D = latent.shape
    C = context.shape[0]
    head_width = query_gain.shape[0]
    cos, sin = rope_tables(R * n_sp * n_tp, head_width)
    QW, VWALL = w_query.shape[1], w_value.shape[1]
    heads = mix_lambda.shape[0]
    ROWS = R * n_tp
    HW = 2 * head_width
    KV = (QW + VWALL) // heads
    MC = mod_shift.shape[1]
    vm = pl.BlockSpec(memory_space=pltpu.VMEM)
    anywhere = pl.BlockSpec(memory_space=pl.ANY)
    smem = pl.BlockSpec(memory_space=pltpu.SMEM)
    dma = pltpu.SemaphoreType.DMA
    update = pl.pallas_call(
        functools.partial(kernel, n_sp, n_tp, n_dp, head_width),
        out_shape=pltpu.VMEM((R, D), BF),
        in_specs=[anywhere] * 14 + [smem, smem]
        + [anywhere] * 3,
        out_specs=vm,
        scratch_shapes=[
            pltpu.VMEM(cond.shape, BF),
            pltpu.VMEM(context_cond.shape, BF),
            pltpu.VMEM(norm_gain.shape, F32),
            pltpu.VMEM(query_gain.shape, F32),
            pltpu.VMEM(key_gain.shape, F32),
            pltpu.VMEM(value_gain.shape, F32),
            pltpu.VMEM((R, D), BF),
            pltpu.VMEM((4, R, D), BF),
            pltpu.VMEM((C, D), BF),
            pltpu.VMEM((3,) + mod_shift.shape, BF),
            pltpu.VMEM(w_query.shape, BF),
            pltpu.VMEM((2,) + w_key.shape, BF),
            pltpu.VMEM((4,) + w_out.shape, BF),
            pltpu.VMEM((2, ROWS, HW), F32),
            pltpu.VMEM((8, mod_shift.shape[0]), F32),
            pltpu.VMEM((8, MC), F32),
            pltpu.VMEM((n_sp - 1, 8, MC), F32),
            pltpu.VMEM((8, MC), F32),
            pltpu.VMEM((n_tp, 8, MC), F32),
            pltpu.VMEM((2, 8, D), F32),
            pltpu.VMEM((C + ROWS, D), BF),
            pltpu.VMEM((heads, ROWS, HW), BF),
            pltpu.VMEM((ROWS, HW), BF),
            pltpu.VMEM((2, 2 * ROWS, HW), BF),
            pltpu.VMEM((heads, C + ROWS, KV), BF),
            pltpu.VMEM((n_sp, ROWS, KV), BF),
            pltpu.VMEM((n_sp * C, KV), BF),
            pltpu.VMEM((2, 2 * ROWS, 2 * VWALL // heads), F32),
            pltpu.VMEM((2, ROWS, VWALL // heads), BF),
            pltpu.VMEM((R, n_tp * VWALL), BF),
            pltpu.VMEM((2 * QW, QW), BF),
            dma((13,)),
            dma(()), dma((4,)),
            dma(()), dma((6,)),
            dma(()), dma(()),
            dma(()), dma(()),
            dma(()), dma(()),
            dma(()), dma((n_sp,)),
            dma(()), dma(()),
            dma(()), dma(()),
            dma(()), dma((9,)),
            dma(()), dma((3,)),
            dma(()), dma((3,)),
            dma(()), dma((4,)),
        ],
        compiler_params=pltpu.CompilerParams(
            collective_id=0, has_side_effects=True, vmem_limit_bytes=66_100_000
        ),
        name="block",
    )(
        latent, context, cond, context_cond, norm_gain, mod_shift, mod_scale,
        mod_gate, w_query, w_key, w_value, query_gain, key_gain, value_gain, mix_lambda, context_lift, w_out,
        jnp.asarray(cos), jnp.asarray(sin),
    )
    return update


def solution(mesh):
    placed = (
        P(("dp", "sp", "tp"), None),
        P(("dp", "sp"), None),
        P(("dp", "sp")),
        P("sp"),
        P(),
        P("sp", "tp"),
        P("sp", "tp"),
        P("sp", "tp"),
        P(None, "tp"),
        P(None, "tp"),
        P(None, "tp"),
        P(),
        P(),
        P("tp"),
        P("tp"),
        P(),
        P("tp", None),
    )
    sizes = mesh.shape
    return jax.shard_map(
        functools.partial(on_device, sizes["sp"], sizes["tp"], sizes["dp"]),
        mesh=mesh,
        in_specs=placed,
        out_specs=P(("dp", "sp", "tp"), None),
        check_vma=False,
    )
```

```python
import functools

import jax
import jax.numpy as jnp
import numpy as np
from jax import lax
from jax.experimental import pallas as pl
from jax.experimental.pallas import tpu as pltpu
from jax.sharding import PartitionSpec as P

GRID = 64
token_eps = 0.01
head_eps = 0.001
rope_base = 10000.0
head_factor = 0.8
MESH = pl.DeviceIdType.MESH
BF = jnp.bfloat16
F32 = jnp.float32


def rope_tables(length, width):
    quarter = width // 4
    inverse = (rope_base ** (-np.arange(quarter, dtype=np.float64) / quarter)).astype(np.float32)
    pos = np.arange(length)
    row = (pos // GRID).astype(np.float32)[:, None] * inverse
    col = (pos % GRID).astype(np.float32)[:, None] * inverse
    cos = np.concatenate([np.cos(row), np.cos(row), np.cos(col), np.cos(col)], axis=1)
    sin = np.concatenate([-np.sin(row), np.sin(row), -np.sin(col), np.sin(col)], axis=1)
    return np.tile(cos, (1, 2)).astype(np.float32), np.tile(sin, (1, 2)).astype(np.float32)


def kernel(n_sp, n_tp, n_dp, head_width, *refs):
    (
        lat_h, ctx_h, cond_h, cctx_h, gain_h, ms_h, msc_h, mg_h, wq_h, wk_h, wv_h,
        qg_h, kg_h, vg_h, lam_r, lift_r, wo_h, cos_h, sin_h,
        out_r,
        cond_r, cctx_r, gain_r, qg_r, kg_r, vg_r,
        own, lat, ctx, mw, wq, wkv, wo, turns,
        act, part, mod_in, summed, mod_full, vecs, normed, qown, qin, qm, kvl, kvr, kvc, acc,
        mine, ho, grp, partial,
        loc, s_swap, r_swap, s_lat, r_lat, s_mod, r_mod, s_mt, r_mt, s_vec, r_vec, s_kv, r_kv,
        s_ctx, r_ctx, s_q, r_q, s_wo, r_wo, s_wz, r_wz, s_dd, r_dd, s_ho, r_ho,
    ) = refs
    s = lax.axis_index("sp")
    t = lax.axis_index("tp")
    d_ix = lax.axis_index("dp")
    core = lax.rem(d_ix, 2)
    partner = d_ix + 1 - 2 * core
    t_odd = lax.rem(t, 2)
    nbr1 = t + 1 - 2 * t_odd
    nbr2 = lax.rem(t + 2, 4)
    nbr3 = lax.rem(nbr1 + 2, 4)
    peers = (t, nbr1, nbr2, nbr3)
    H = n_sp // 2
    half = s // H
    base = half * H
    s_opp = lax.rem(s + H, n_sp)
    home = core == half
    away = jnp.not_equal(core, half)
    a = lax.rem(core + half, 2)
    block = s + a * (s_opp - s)
    other_block = s_opp + a * (s - s_opp)
    d_work = d_ix - core + half
    e = lax.rem(s, 2)
    level = s + 1 - 2 * e
    R, D = own.shape
    PR = R // 4
    C = ctx.shape[0]
    QW = wq.shape[1]
    n_head = QW // (2 * head_width)
    HW = 2 * head_width
    VW = wkv.shape[2] // n_head
    ROWS = 4 * R

    bar = pltpu.get_barrier_semaphore()
    greeted = [{"tp": peers[k]} for k in range(1, 4)] + [{"dp": partner}]
    for k in range(1, n_sp):
        there = lax.rem(s + k, n_sp)
        greeted += [{"sp": there}, {"dp": partner, "sp": there}]
    for where in greeted:
        pl.semaphore_signal(bar, inc=1, device_id=where, device_id_type=MESH)

    def local(i, src, dst):
        c = pltpu.make_async_copy(src, dst, loc.at[i])
        c.start()
        return c

    def remote(src, dst, ss, rs, where):
        return pltpu.make_async_remote_copy(
            src_ref=src, dst_ref=dst, send_sem=ss, recv_sem=rs, device_id=where, device_id_type=MESH
        )

    def drain(ref, sem):
        remote(ref, ref, sem, sem, {"dp": partner}).wait_recv()

    @pl.when(home)
    def _():
        local(0, lat_h, lat.at[0])

    @pl.when(away)
    def _():
        local(0, lat_h, own)

    l_one = [local(1, cond_h, cond_r), local(2, cctx_h, cctx_r)]
    for j, h in enumerate((ms_h, msc_h, mg_h)):
        local(3, h, mw.at[j])

    act[...] = jnp.zeros_like(act)
    for row, ref in ((0, cond_r), (1, cctx_r)):
        l_one[row].wait()
        v = ref[...].astype(F32).reshape(1, -1)
        act[row : row + 1, :] = v / (1.0 + jnp.exp(-v))
    acts = act[...].astype(BF)
    part[...] = jnp.zeros_like(part)
    drain(mw, loc.at[3])
    l_wo = local(12, wo_h, wo.at[0])
    for j in range(3):
        res = jnp.dot(acts, mw[j], preferred_element_type=F32)
        part[2 * j : 2 * j + 2, :] = res[0:2]

    drain(own, loc.at[0])
    pl.semaphore_wait(bar, len(greeted))

    def mod_copy(k):
        return remote(part, mod_in.at[k - 1], s_mod, r_mod, {"sp": lax.rem(s + k, n_sp)})

    def piece(j):
        return pl.ds(j * PR, PR)

    def swap(j):
        return remote(own.at[piece(j)], lat.at[0, piece(j)], s_swap, r_swap.at[j],
                      {"dp": partner, "sp": s_opp})

    def along_x(j):
        return remote(lat.at[0, piece(j)], lat.at[1, piece(j)], s_lat, r_lat.at[j if j < 2 else 4],
                      {"tp": nbr1})

    def along_y(j):
        return remote(lat.at[0, piece(j)], lat.at[2, piece(j)], s_lat, r_lat.at[j if j > 1 else 4],
                      {"tp": nbr2})

    def onward(j):
        slot, where = (1, nbr2) if j < 2 else (2, nbr1)
        return remote(lat.at[slot, piece(j)], lat.at[3, piece(j)], s_lat, r_lat.at[5], {"tp": where})

    def pass_on(j):
        (along_x(j) if j < 2 else along_y(j)).wait_recv()
        onward(j).start()

    HALF = wo.shape[1] // 2
    QUART = HALF // 2
    SH = QUART // 4

    def wo_rows(at, count):
        return pl.ds(pl.multiple_of(core * HALF + at, SH), count)

    def wo_copy(i, src_slot, dst_slot, at, count, where):
        rows = wo_rows(at, count)
        return remote(wo.at[src_slot, rows], wo.at[dst_slot, rows], s_wo, r_wo.at[i], {"tp": where})

    def wz_copy(k, q):
        rows = wo_rows(q * QUART + (QUART - SH) * e, SH)
        return remote(wo.at[k, rows], wo.at[k, rows], s_wz, r_wz.at[k - 1], {"sp": level})

    def dd_copy(k, at, count):
        rows = wo_rows(at, count)
        return remote(wo.at[k, rows], wo.at[k, rows], s_dd, r_dd.at[k - 1], {"dp": partner})

    def lead(i, src, dst, q, where):
        return wo_copy(i, src, dst, q * QUART + (QUART - SH) * e, SH, where)

    def rest(i, src, dst, q, where):
        return wo_copy(i, src, dst, q * QUART + SH, QUART - 2 * SH, where)

    lead_x = [lead(0, 0, 1, 0, nbr1), lead(2, 0, 1, 1, nbr1)]
    lead_y = [lead(2, 0, 2, 0, nbr2), lead(1, 0, 2, 1, nbr2)]
    lead_f = [lead(6, 1, 3, 0, nbr2), lead(6, 2, 3, 1, nbr1)]
    rest_x = [rest(3, 0, 1, 0, nbr1), rest(5, 0, 1, 1, nbr1)]
    rest_y = [rest(5, 0, 2, 0, nbr2), rest(4, 0, 2, 1, nbr2)]
    rest_f = [rest(7, 1, 3, 0, nbr2), rest(8, 2, 3, 1, nbr1)]

    def start(*copies):
        for c in copies:
            c.start()

    def share_first():
        lead_x[0].wait_recv()
        wz_copy(1, 0).start()
        lead_y[1].wait_recv()
        wz_copy(2, 1).start()

    def share_second():
        drain(wo.at[1, pl.ds(0, 2 * SH)], r_wo.at[2])
        wz_copy(1, 1).start()
        wz_copy(2, 0).start()

    def share_far():
        wz_copy(3, 0).start()
        wz_copy(3, 1).start()

    def pass_rest():
        rest_x[0].wait_recv()
        rest_f[0].start()
        rest_y[1].wait_recv()
        rest_f[1].start()

    near_leads = (lead_x[0], lead_y[1], lead_x[1], lead_y[0])
    near_rests = (rest_x[0], rest_y[1], rest_x[1], rest_y[0])

    for k in range(1, n_sp):
        mod_copy(k).start()

    @pl.when(home)
    def _():
        for j in range(4):
            along_x(j).start()
            along_y((j + 2) % 4).start()

    @pl.when(away)
    def _():
        for j in range(4):
            swap(j).start()

    l_ctx = local(4, ctx_h, ctx)
    local(5, wk_h, wkv.at[0])
    local(5, wv_h, wkv.at[1])
    at_turns = pl.ds(pl.multiple_of(block * ROWS, ROWS), ROWS)
    local(6, cos_h.at[at_turns], turns.at[0])
    local(6, sin_h.at[at_turns], turns.at[1])
    l_small = [
        local(7 + j, src, dst)
        for j, (src, dst) in enumerate(((gain_h, gain_r), (qg_h, qg_r), (kg_h, kg_r), (vg_h, vg_r)))
    ]
    l_wq = local(11, wq_h, wq)

    l_wo.wait()

    @pl.when(away)
    def _():
        start(*near_leads)

    group = (
        lax.rem(lax.broadcasted_iota(jnp.int32, (2 * QW, QW), 0), QW) // head_width
        == lax.broadcasted_iota(jnp.int32, (2 * QW, QW), 1) // head_width
    )
    grp[...] = jnp.where(group, 1.0 / head_width, 0.0).astype(BF)
    for c in l_small:
        c.wait()
    gain = gain_r[...].reshape(1, -1)
    q_gain = qg_r[...].reshape(1, -1)
    q_gain = jnp.concatenate([q_gain, q_gain], axis=1)
    k_gain = kg_r[...].reshape(1, -1)
    k_gain = jnp.concatenate([k_gain, k_gain], axis=1)
    v_gain = vg_r[...].reshape(1, -1)

    drain(mod_in, r_mod)
    total = part[...]
    for k in range(n_sp - 1):
        total = total + mod_in[k]
    summed[...] = total
    mod_full[t] = total

    def mt_copy(k):
        return remote(summed, mod_full.at[t], s_mt, r_mt, {"tp": peers[k]})

    for k in range(1, 4):
        mt_copy(k).start()

    @pl.when(home)
    def _():
        for j in (0, 2, 1, 3):
            pass_on(j)

    @pl.when(jnp.logical_and(home, core == 1))
    def _():
        start(*near_leads)

    @pl.when(away)
    def _():
        @pl.when(core == 1)
        def _():
            share_first()
            share_second()

        for j in range(4):
            swap(j).wait_recv()
            along_y(j).start()
            along_x(j).start()
            if j == 3:
                @pl.when(core == 0)
                def _():
                    share_first()
                    share_second()

        pass_on(0)
        pass_on(1)

    def full_row(j):
        return jnp.concatenate([mod_full[q, j : j + 1, :] for q in range(n_tp)], axis=1)

    vec_copy = remote(vecs.at[0], vecs.at[1], s_vec, r_vec, {"dp": partner})

    @pl.when(home)
    def _():
        drain(mod_full.at[0:3], r_mt)
        vecs[0, 0:1, :] = full_row(0)
        vecs[0, 1:2, :] = full_row(1)
        vecs[0, 2:3, :] = gain * (1.0 + full_row(2))
        vecs[0, 3:4, :] = gain * (1.0 + full_row(3))
        vecs[0, 4:8, :] = jnp.broadcast_to(full_row(4), (4, D))
        vec_copy.start()

    @pl.when(away)
    def _():
        vec_copy.wait_recv()

    def norm_rows(src, row, count, dst_at, slot):
        step = 16

        @pl.loop(0, count // step, unroll=True)
        def _(i):
            at = pl.multiple_of(i * step, step)
            v = src[pl.ds(at, step), :].astype(F32)
            inv = lax.rsqrt(jnp.mean(v * v, axis=-1, keepdims=True) + token_eps)
            normed[pl.ds(dst_at + at, step), :] = (
                v * inv * vecs[slot, 2 + row : 3 + row, :] + vecs[slot, row : row + 1, :]
            ).astype(BF)

    def head_norm(x):
        square = x * x
        high = square.astype(BF)
        low = (square - high.astype(F32)).astype(BF)
        mean = jnp.dot(jnp.concatenate([high, low], axis=1), grp[...], preferred_element_type=F32)
        return x * lax.rsqrt(mean + token_eps)

    def turn(y, cos, sin):
        lane = lax.broadcasted_iota(jnp.int32, y.shape, 1)
        front = lax.rem(lane, head_width // 2) < head_width // 4
        other = jnp.where(
            front,
            pltpu.roll(y, HW - head_width // 4, axis=1),
            pltpu.roll(y, head_width // 4, axis=1),
        )
        return y * cos + other * sin

    def turns_of(k):
        at = pl.ds(pl.multiple_of(peers[k] * R, R), R)
        return turns[0, at, :], turns[1, at, :]

    def project(first, count, plain):
        x = normed[first : first + count, :]
        kk = head_norm(jnp.dot(x, wkv[0], preferred_element_type=F32))
        for h in range(n_head):
            y = kk[:, h * HW : (h + 1) * HW] * k_gain
            if plain:
                kvl[h, first : first + plain, 0:HW] = y[:plain].astype(BF)
            for at in range(plain, count, R):
                kvl[h, first + at : first + at + R, 0:HW] = turn(
                    y[at : at + R], *turns_of((first + at - C) // R)
                ).astype(BF)
        vv = jnp.dot(x, wkv[1], preferred_element_type=F32).astype(BF)
        for h in range(n_head):
            kvl[h, first : first + count, HW:] = vv[:, h * VW : (h + 1) * VW]

    def project_queries(first, last):
        x = normed[C + first * R : C + last * R, :]
        qq = head_norm(jnp.dot(x, wq[...], preferred_element_type=F32))
        for k in range(first, last):
            for h in range(n_head):
                y = qq[(k - first) * R : (k - first + 1) * R, h * HW : (h + 1) * HW] * q_gain
                qown[h, k * R : (k + 1) * R, :] = (
                    turn(y, *turns_of(k)) * (head_width ** -0.5)
                ).astype(BF)

    def split_maps(q, at):
        lane = lax.broadcasted_iota(jnp.int32, q.shape, 1)
        for m in range(2):
            qm[m, at : at + ROWS, :] = jnp.where(lane // head_width == m, q, jnp.zeros_like(q))

    def kv_copy(j, head, at, count):
        there = base + lax.rem(s - base + j, H)
        i = 2 * j + a
        return remote(kvl.at[head, pl.ds(C + at, count)], kvr.at[block, pl.ds(at, count)], s_kv,
                      r_kv.at[i], {"dp": d_ix - core + head, "sp": there})

    def send_block(at, count):
        for j in range(1, H):
            for head in range(2):
                kv_copy(j, head, at, count).start()
        kv_copy(0, 1 - core, at, count).start()

    def ctx_copy(there, head):
        at = pl.ds(pl.multiple_of(s * C, C), C)
        return remote(kvl.at[head, pl.ds(0, C)], kvc.at[at], s_ctx, r_ctx,
                      {"dp": d_ix - core + head, "sp": there})

    def send_ctx():
        @pl.when(home)
        def _():
            for j in range(1, H):
                for head in range(2):
                    ctx_copy(base + lax.rem(s - base + j, H), head).start()
            ctx_copy(s, 1 - core).start()
            kvc[pl.ds(pl.multiple_of(s * C, C), C), :] = kvl[core, 0:C, :]

        @pl.when(away)
        def _():
            for j in range(H):
                for head in range(2):
                    ctx_copy(lax.rem(s_opp + j, H) + H - base, head).start()

    l_ctx.wait()
    norm_rows(ctx, 1, C, 0, a)
    drain(wkv, loc.at[5])
    drain(turns, loc.at[6])

    @pl.when(home)
    def _():
        norm_rows(lat.at[0], 0, R, C, 0)
        project(0, C + R, C)
        send_block(0, R)
        send_ctx()
        drain(lat.at[1], r_lat.at[4])
        norm_rows(lat.at[1], 0, R, C + R, 0)
        norm_rows(lat.at[2], 0, R, C + 2 * R, 0)
        project(C + R, 2 * R, 0)
        send_block(R, 2 * R)

    @pl.when(jnp.logical_and(home, core == 0))
    def _():
        start(*near_leads)

    @pl.when(away)
    def _():
        project(0, C, C)
        send_ctx()
        pass_on(2)
        pass_on(3)
        start(*lead_f, *near_rests)
        norm_rows(lat.at[0], 0, R, C, 1)
        drain(lat.at[1], r_lat.at[4])
        norm_rows(lat.at[1], 0, R, C + R, 1)
        norm_rows(lat.at[2], 0, R, C + 2 * R, 1)
        project(C, 3 * R, 0)
        send_block(0, 3 * R)

    l_wq.wait()
    project_queries(0, 3)
    drain(lat.at[3], r_lat.at[5])
    norm_rows(lat.at[3], 0, R, C + 3 * R, a)
    project(C + 3 * R, R, 0)
    send_block(3 * R, R)

    project_queries(3, 4)
    q_copy = remote(qown.at[1 - core], qin, s_q, r_q, {"dp": partner})
    q_copy.start()
    split_maps(qown[core], 0)

    QB = 4 * R
    lift = lift_r[core]

    def attend(block, at, keys, start_row, count, first, plus):
        k = block[at : at + keys, 0:HW]
        v = block[at : at + keys, HW:]
        vx = jnp.concatenate([v, jnp.ones_like(v)], axis=1)
        for m in range(2):
            for b in range(count // QB):
                rows = slice(start_row + b * QB, start_row + (b + 1) * QB)
                sc = lax.dot_general(
                    qm[m, rows, :], k, (((1,), (1,)), ((), ())), preferred_element_type=F32
                )
                if plus is not None:
                    sc = sc + plus
                p = jnp.exp(sc).astype(BF)
                add = jnp.dot(p, vx, preferred_element_type=F32)
                if first:
                    acc[m, rows, :] = add
                else:
                    acc[m, rows, :] += add

    @pl.when(home)
    def _():
        share_first()
        start(*lead_f)

    @pl.when(jnp.logical_and(home, core == 0))
    def _():
        start(*near_rests)

    attend(kvl.at[core], C, ROWS, 0, ROWS, True, None)

    @pl.when(jnp.logical_and(home, core == 1))
    def _():
        drain(wo.at[3, pl.ds(0, 2 * SH)], r_wo.at[6])
        start(*near_rests)

    q_copy.wait_recv()
    split_maps(qin[...], ROWS)
    attend(kvl.at[core], C, ROWS, ROWS, ROWS, True, None)

    @pl.when(home)
    def _():
        share_second()

    pass_rest()

    @pl.when(jnp.logical_or(away, core == 0))
    def _():
        drain(wo.at[3, pl.ds(0, 2 * SH)], r_wo.at[6])

    share_far()

    def attend_block(slot, i):
        drain(kvr.at[slot], r_kv.at[i])
        attend(kvr.at[slot], 0, ROWS, 0, 2 * ROWS, False, None)

    for j in range(1, H):
        attend_block(base + lax.rem(s - base + H - j, H), 2 * j)

    @pl.when(home)
    def _():
        drain(kvc.at[pl.ds(0, (n_sp - 1) * C)], r_ctx)

    @pl.when(away)
    def _():
        drain(kvc, r_ctx)

    attend(kvc, 0, n_sp * C, 0, 2 * ROWS, False, lift)
    attend_block(other_block, 1 - a)
    for j in range(1, H):
        attend_block(lax.rem(base + lax.rem(s - base + H - j, H) + H, n_sp), 2 * j + 1)

    @pl.when(away)
    def _():
        drain(mod_full.at[0:3], r_mt)

    def ho_copy(q, k):
        lanes = pl.ds(pl.multiple_of(k * n_head * VW + core * VW, VW), VW)
        return remote(mine.at[q, pl.ds(k * R, R)], ho.at[:, lanes], s_ho, r_ho.at[k],
                      {"dp": d_work, "sp": block + q * (other_block - block), "tp": peers[k]})

    for q in (1 - a, a):
        rows = pl.ds(pl.multiple_of(q * ROWS, ROWS), ROWS)
        a0 = acc[0, rows, :]
        a1 = acc[1, rows, :]
        mixed = a0[:, :VW] / a0[:, VW:] - lam_r[core] * (a1[:, :VW] / a1[:, VW:])
        inv = lax.rsqrt(jnp.mean(mixed * mixed, axis=-1, keepdims=True) + head_eps)
        mine[q, :, :] = (mixed * inv * v_gain * head_factor).astype(BF)
        for k in (3, 2, 1):
            ho_copy(q, k).start()
        if q is not a:
            ho_copy(q, 0).start()

    @pl.when(away)
    def _():
        ho_copy(a, 0).start()

    for h in range(2):
        @pl.when(jnp.logical_and(home, core == h))
        def _():
            ho[:, h * VW : (h + 1) * VW] = mine[0, 0:R, :]

    drain(wo.at[1, pl.ds(0, 2 * (QUART - 2 * SH))], r_wo.at[5])
    for k in range(1, 3):
        drain(wo.at[k, pl.ds(0, 2 * SH)], r_wz.at[k - 1])
        dd_copy(k, 0, HALF).start()
    drain(wo.at[3, pl.ds(0, 2 * SH)], r_wz.at[2])
    for q in range(2):
        dd_copy(3, q * QUART, SH).start()
        dd_copy(3, (q + 1) * QUART - SH, SH).start()
    for q in range(2):
        rest_f[q].wait_recv()
        dd_copy(3, q * QUART + SH, QUART - 2 * SH).start()

    def arrived(k):
        drain(wo.at[k, pl.ds(0, HALF)], r_dd.at[k - 1])
        drain(mine.at[0, pl.ds(0, 2 * R)], r_ho.at[k])

    KW = n_head * VW

    @pl.when(away)
    def _():
        vecs[0, 4:8, :] = jnp.broadcast_to(full_row(4), (4, D))

    arrived(1)
    arrived(2)
    partial[...] = jnp.dot(
        ho[:, KW : 3 * KW], wo[1:3].reshape(-1, D), preferred_element_type=F32
    )
    arrived(3)

    @pl.when(home)
    def _():
        drain(mine.at[0, pl.ds(0, R)], r_ho.at[0])

    @pl.when(away)
    def _():
        drain(mine.at[0, pl.ds(0, 2 * R)], r_ho.at[0])

    late = jnp.dot(ho[:, 0:KW], wo[0], preferred_element_type=F32)
    late += jnp.dot(ho[:, 3 * KW :], wo[3], preferred_element_type=F32)
    mixture = vecs[0, 4:5, :] * (partial[...] + late)

    @pl.when(home)
    def _():
        out_r[...] = (lat[0].astype(F32) + mixture).astype(BF)

    @pl.when(away)
    def _():
        out_r[...] = (own[...].astype(F32) + mixture).astype(BF)

    def sent(ref, sem):
        remote(ref, ref, sem, sem, {"dp": partner}).wait_send()

    sent(mod_in, s_mod)
    sent(mod_full.at[0:3], s_mt)
    sent(lat.at[0:3], s_lat)
    sent(kvr.at[0 : n_sp - 1], s_kv)
    sent(wo.at[0:3, pl.ds(0, 2 * (QUART - SH))], s_wo)
    sent(wo.at[0:3, pl.ds(0, 2 * SH)], s_wz)
    sent(wo.at[0:3, pl.ds(0, HALF)], s_dd)
    q_copy.wait_send()

    @pl.when(home)
    def _():
        vec_copy.wait_send()
        sent(kvc.at[pl.ds(0, (n_sp - 1) * C)], s_ctx)
        sent(qm.at[0, pl.ds(0, 7 * R)], s_ho)

    @pl.when(away)
    def _():
        sent(own, s_swap)
        sent(kvc, s_ctx)
        sent(mine, s_ho)


def on_device(n_sp, n_tp, n_dp, *args):
    (
        latent, context, cond, context_cond, norm_gain, mod_shift, mod_scale, mod_gate,
        w_query, w_key, w_value, query_gain, key_gain, mix_lambda, context_lift, value_gain, w_out,
    ) = args
    R, D = latent.shape
    C = context.shape[0]
    head_width = query_gain.shape[0]
    cos, sin = rope_tables(R * n_sp * n_tp, head_width)
    QW, VWALL = w_query.shape[1], w_value.shape[1]
    heads = mix_lambda.shape[0]
    ROWS = R * n_tp
    HW = 2 * head_width
    KV = (QW + VWALL) // heads
    MC = mod_shift.shape[1]
    vm = pl.BlockSpec(memory_space=pltpu.VMEM)
    anywhere = pl.BlockSpec(memory_space=pl.ANY)
    smem = pl.BlockSpec(memory_space=pltpu.SMEM)
    dma = pltpu.SemaphoreType.DMA
    update = pl.pallas_call(
        functools.partial(kernel, n_sp, n_tp, n_dp, head_width),
        out_shape=pltpu.VMEM((R, D), BF),
        in_specs=[anywhere] * 14 + [smem, smem]
        + [anywhere] * 3,
        out_specs=vm,
        scratch_shapes=[
            pltpu.VMEM(cond.shape, BF),
            pltpu.VMEM(context_cond.shape, BF),
            pltpu.VMEM(norm_gain.shape, F32),
            pltpu.VMEM(query_gain.shape, F32),
            pltpu.VMEM(key_gain.shape, F32),
            pltpu.VMEM(value_gain.shape, F32),
            pltpu.VMEM((R, D), BF),
            pltpu.VMEM((4, R, D), BF),
            pltpu.VMEM((C, D), BF),
            pltpu.VMEM((3,) + mod_shift.shape, BF),
            pltpu.VMEM(w_query.shape, BF),
            pltpu.VMEM((2,) + w_key.shape, BF),
            pltpu.VMEM((4,) + w_out.shape, BF),
            pltpu.VMEM((2, ROWS, HW), F32),
            pltpu.VMEM((8, mod_shift.shape[0]), F32),
            pltpu.VMEM((8, MC), F32),
            pltpu.VMEM((n_sp - 1, 8, MC), F32),
            pltpu.VMEM((8, MC), F32),
            pltpu.VMEM((n_tp, 8, MC), F32),
            pltpu.VMEM((2, 8, D), F32),
            pltpu.VMEM((C + ROWS, D), BF),
            pltpu.VMEM((heads, ROWS, HW), BF),
            pltpu.VMEM((ROWS, HW), BF),
            pltpu.VMEM((2, 2 * ROWS, HW), BF),
            pltpu.VMEM((heads, C + ROWS, KV), BF),
            pltpu.VMEM((n_sp, ROWS, KV), BF),
            pltpu.VMEM((n_sp * C, KV), BF),
            pltpu.VMEM((2, 2 * ROWS, 2 * VWALL // heads), F32),
            pltpu.VMEM((2, ROWS, VWALL // heads), BF),
            pltpu.VMEM((R, n_tp * VWALL), BF),
            pltpu.VMEM((2 * QW, QW), BF),
            pltpu.VMEM((R, D), F32),
            dma((13,)),
            dma(()), dma((4,)),
            dma(()), dma((6,)),
            dma(()), dma(()),
            dma(()), dma(()),
            dma(()), dma(()),
            dma(()), dma((n_sp,)),
            dma(()), dma(()),
            dma(()), dma(()),
            dma(()), dma((9,)),
            dma(()), dma((3,)),
            dma(()), dma((3,)),
            dma(()), dma((4,)),
        ],
        compiler_params=pltpu.CompilerParams(
            collective_id=0, has_side_effects=True, vmem_limit_bytes=66_100_000
        ),
        name="block",
    )(
        latent, context, cond, context_cond, norm_gain, mod_shift, mod_scale,
        mod_gate, w_query, w_key, w_value, query_gain, key_gain, value_gain, mix_lambda, context_lift, w_out,
        jnp.asarray(cos), jnp.asarray(sin),
    )
    return update


def solution(mesh):
    placed = (
        P(("dp", "sp", "tp"), None),
        P(("dp", "sp"), None),
        P(("dp", "sp")),
        P("sp"),
        P(),
        P("sp", "tp"),
        P("sp", "tp"),
        P("sp", "tp"),
        P(None, "tp"),
        P(None, "tp"),
        P(None, "tp"),
        P(),
        P(),
        P("tp"),
        P("tp"),
        P(),
        P("tp", None),
    )
    sizes = mesh.shape
    return jax.shard_map(
        functools.partial(on_device, sizes["sp"], sizes["tp"], sizes["dp"]),
        mesh=mesh,
        in_specs=placed,
        out_specs=P(("dp", "sp", "tp"), None),
        check_vma=False,
    )
```

```python
import functools

import jax
import jax.numpy as jnp
import numpy as np
from jax import lax
from jax.experimental import pallas as pl
from jax.experimental.pallas import tpu as pltpu
from jax.sharding import PartitionSpec as P

GRID = 64
token_eps = 0.01
head_eps = 0.001
rope_base = 10000.0
head_factor = 0.8
MESH = pl.DeviceIdType.MESH
BF = jnp.bfloat16
F32 = jnp.float32


def rope_tables(length, width):
    quarter = width // 4
    inverse = (rope_base ** (-np.arange(quarter, dtype=np.float64) / quarter)).astype(np.float32)
    pos = np.arange(length)
    row = (pos // GRID).astype(np.float32)[:, None] * inverse
    col = (pos % GRID).astype(np.float32)[:, None] * inverse
    cos = np.concatenate([np.cos(row), np.cos(row), np.cos(col), np.cos(col)], axis=1)
    sin = np.concatenate([-np.sin(row), np.sin(row), -np.sin(col), np.sin(col)], axis=1)
    return np.tile(cos, (1, 2)).astype(np.float32), np.tile(sin, (1, 2)).astype(np.float32)


def kernel(n_sp, n_tp, n_dp, head_width, *refs):
    (
        lat_h, ctx_h, cond_h, cctx_h, gain_h, ms_h, msc_h, mg_h, wq_h, wk_h, wv_h,
        qg_h, kg_h, vg_h, lam_r, lift_r, wo_h, cos_h, sin_h,
        out_r,
        cond_r, cctx_r, gain_r, qg_r, kg_r, vg_r,
        own, lat, ctx, mw, wq, wkv, wo, turns,
        act, part, mod_in, summed, mod_full, vecs, normed, qown, qin, qm, kvl, kvr, kvc, acc,
        mine, ho, grp, partial,
        loc, s_swap, r_swap, s_lat, r_lat, s_mod, r_mod, s_mt, r_mt, s_vec, r_vec, s_kv, r_kv,
        s_ctx, r_ctx, s_q, r_q, s_wo, r_wo, s_wz, r_wz, s_dd, r_dd, s_ho, r_ho,
    ) = refs
    s = lax.axis_index("sp")
    t = lax.axis_index("tp")
    d_ix = lax.axis_index("dp")
    core = lax.rem(d_ix, 2)
    partner = d_ix + 1 - 2 * core
    t_odd = lax.rem(t, 2)
    nbr1 = t + 1 - 2 * t_odd
    nbr2 = lax.rem(t + 2, 4)
    nbr3 = lax.rem(nbr1 + 2, 4)
    peers = (t, nbr1, nbr2, nbr3)
    H = n_sp // 2
    half = s // H
    base = half * H
    s_opp = lax.rem(s + H, n_sp)
    home = core == half
    away = jnp.not_equal(core, half)
    a = lax.rem(core + half, 2)
    block = s + a * (s_opp - s)
    other_block = s_opp + a * (s - s_opp)
    d_work = d_ix - core + half
    e = lax.rem(s, 2)
    level = s + 1 - 2 * e
    R, D = own.shape
    PR = R // 4
    C = ctx.shape[0]
    QW = wq.shape[1]
    n_head = QW // (2 * head_width)
    HW = 2 * head_width
    VW = wkv.shape[2] // n_head
    ROWS = 4 * R

    bar = pltpu.get_barrier_semaphore()
    greeted = [{"tp": peers[k]} for k in range(1, 4)] + [{"dp": partner}]
    for k in range(1, n_sp):
        there = lax.rem(s + k, n_sp)
        greeted += [{"sp": there}, {"dp": partner, "sp": there}]
    for where in greeted:
        pl.semaphore_signal(bar, inc=1, device_id=where, device_id_type=MESH)

    def local(i, src, dst):
        c = pltpu.make_async_copy(src, dst, loc.at[i])
        c.start()
        return c

    def remote(src, dst, ss, rs, where):
        return pltpu.make_async_remote_copy(
            src_ref=src, dst_ref=dst, send_sem=ss, recv_sem=rs, device_id=where, device_id_type=MESH
        )

    def drain(ref, sem):
        remote(ref, ref, sem, sem, {"dp": partner}).wait_recv()

    @pl.when(home)
    def _():
        local(0, lat_h, lat.at[0])

    @pl.when(away)
    def _():
        local(0, lat_h, own)

    l_one = [local(1, cond_h, cond_r), local(2, cctx_h, cctx_r)]
    for j, h in enumerate((ms_h, msc_h, mg_h)):
        local(3, h, mw.at[j])

    rows = []
    for row, ref in ((0, cond_r), (1, cctx_r)):
        l_one[row].wait()
        v = ref[...].astype(F32).reshape(1, -1)
        rows.append(v / (1.0 + jnp.exp(-v)))
    acts = jnp.concatenate(rows + [jnp.zeros((6, rows[0].shape[1]), F32)], axis=0).astype(BF)
    drain(mw, loc.at[3])
    l_wo = local(12, wo_h, wo.at[0])
    res = [jnp.dot(acts, mw[j], preferred_element_type=F32) for j in range(3)]
    part[...] = jnp.concatenate([r[0:2] for r in res] + [res[2][6:8]], axis=0)

    drain(own, loc.at[0])
    pl.semaphore_wait(bar, len(greeted))

    def mod_copy(k):
        return remote(part, mod_in.at[k - 1], s_mod, r_mod, {"sp": lax.rem(s + k, n_sp)})

    def piece(j):
        return pl.ds(j * PR, PR)

    def swap(j):
        return remote(own.at[piece(j)], lat.at[0, piece(j)], s_swap, r_swap.at[j],
                      {"dp": partner, "sp": s_opp})

    def along_x(j):
        return remote(lat.at[0, piece(j)], lat.at[1, piece(j)], s_lat, r_lat.at[j if j < 2 else 4],
                      {"tp": nbr1})

    def along_y(j):
        return remote(lat.at[0, piece(j)], lat.at[2, piece(j)], s_lat, r_lat.at[j if j > 1 else 4],
                      {"tp": nbr2})

    def onward(j):
        slot, where = (1, nbr2) if j < 2 else (2, nbr1)
        return remote(lat.at[slot, piece(j)], lat.at[3, piece(j)], s_lat, r_lat.at[5], {"tp": where})

    def pass_on(j):
        (along_x(j) if j < 2 else along_y(j)).wait_recv()
        onward(j).start()

    HALF = wo.shape[1] // 2
    QUART = HALF // 2
    SH = QUART // 4

    def wo_rows(at, count):
        return pl.ds(pl.multiple_of(core * HALF + at, SH), count)

    def wo_copy(i, src_slot, dst_slot, at, count, where):
        rows = wo_rows(at, count)
        return remote(wo.at[src_slot, rows], wo.at[dst_slot, rows], s_wo, r_wo.at[i], {"tp": where})

    def wz_copy(k, q):
        rows = wo_rows(q * QUART + (QUART - SH) * e, SH)
        return remote(wo.at[k, rows], wo.at[k, rows], s_wz, r_wz.at[k - 1], {"sp": level})

    def dd_copy(k, at, count):
        rows = wo_rows(at, count)
        return remote(wo.at[k, rows], wo.at[k, rows], s_dd, r_dd.at[k - 1], {"dp": partner})

    def lead(i, src, dst, q, where):
        return wo_copy(i, src, dst, q * QUART + (QUART - SH) * e, SH, where)

    def rest(i, src, dst, q, where):
        return wo_copy(i, src, dst, q * QUART + SH, QUART - 2 * SH, where)

    lead_x = [lead(0, 0, 1, 0, nbr1), lead(2, 0, 1, 1, nbr1)]
    lead_y = [lead(2, 0, 2, 0, nbr2), lead(1, 0, 2, 1, nbr2)]
    lead_f = [lead(6, 1, 3, 0, nbr2), lead(6, 2, 3, 1, nbr1)]
    rest_x = [rest(3, 0, 1, 0, nbr1), rest(5, 0, 1, 1, nbr1)]
    rest_y = [rest(5, 0, 2, 0, nbr2), rest(4, 0, 2, 1, nbr2)]
    rest_f = [rest(7, 1, 3, 0, nbr2), rest(8, 2, 3, 1, nbr1)]

    def start(*copies):
        for c in copies:
            c.start()

    def share_first():
        lead_x[0].wait_recv()
        wz_copy(1, 0).start()
        lead_y[1].wait_recv()
        wz_copy(2, 1).start()

    def share_second():
        drain(wo.at[1, pl.ds(0, 2 * SH)], r_wo.at[2])
        wz_copy(1, 1).start()
        wz_copy(2, 0).start()

    def share_far():
        wz_copy(3, 0).start()
        wz_copy(3, 1).start()

    def pass_rest():
        rest_x[0].wait_recv()
        rest_f[0].start()
        rest_y[1].wait_recv()
        rest_f[1].start()

    near_leads = (lead_x[0], lead_y[1], lead_x[1], lead_y[0])
    near_rests = (rest_x[0], rest_y[1], rest_x[1], rest_y[0])

    for k in range(1, n_sp):
        mod_copy(k).start()

    @pl.when(home)
    def _():
        for j in range(4):
            along_x(j).start()
            along_y((j + 2) % 4).start()

    @pl.when(away)
    def _():
        for j in range(4):
            swap(j).start()

    l_ctx = local(4, ctx_h, ctx)
    local(5, wk_h, wkv.at[0])
    local(5, wv_h, wkv.at[1])
    at_turns = pl.ds(pl.multiple_of(block * ROWS, ROWS), ROWS)
    local(6, cos_h.at[at_turns], turns.at[0])
    local(6, sin_h.at[at_turns], turns.at[1])
    l_small = [
        local(7 + j, src, dst)
        for j, (src, dst) in enumerate(((gain_h, gain_r), (qg_h, qg_r), (kg_h, kg_r), (vg_h, vg_r)))
    ]
    l_wq = local(11, wq_h, wq)

    l_wo.wait()

    @pl.when(away)
    def _():
        start(*near_leads)

    group = (
        lax.rem(lax.broadcasted_iota(jnp.int32, (2 * QW, QW), 0), QW) // head_width
        == lax.broadcasted_iota(jnp.int32, (2 * QW, QW), 1) // head_width
    )
    grp[...] = jnp.where(group, 1.0 / head_width, 0.0).astype(BF)
    for c in l_small:
        c.wait()
    gain = gain_r[...].reshape(1, -1)
    q_gain = qg_r[...].reshape(1, -1)
    q_gain = jnp.concatenate([q_gain, q_gain], axis=1)
    k_gain = kg_r[...].reshape(1, -1)
    k_gain = jnp.concatenate([k_gain, k_gain], axis=1)
    v_gain = vg_r[...].reshape(1, -1)

    drain(mod_in, r_mod)
    total = part[...]
    for k in range(n_sp - 1):
        total = total + mod_in[k]
    summed[...] = total
    mod_full[t] = total

    def mt_copy(k):
        return remote(summed, mod_full.at[t], s_mt, r_mt, {"tp": peers[k]})

    for k in range(1, 4):
        mt_copy(k).start()

    @pl.when(home)
    def _():
        for j in (0, 2, 1, 3):
            pass_on(j)

    @pl.when(jnp.logical_and(home, core == 1))
    def _():
        start(*near_leads)

    @pl.when(away)
    def _():
        @pl.when(core == 1)
        def _():
            share_first()
            share_second()

        for j in range(4):
            swap(j).wait_recv()
            along_y(j).start()
            along_x(j).start()
            if j == 3:
                @pl.when(core == 0)
                def _():
                    share_first()
                    share_second()

        pass_on(0)
        pass_on(1)

    def full_row(j):
        return jnp.concatenate([mod_full[q, j : j + 1, :] for q in range(n_tp)], axis=1)

    vec_copy = remote(vecs.at[0], vecs.at[1], s_vec, r_vec, {"dp": partner})

    @pl.when(home)
    def _():
        drain(mod_full.at[0:3], r_mt)
        vecs[0, 0:1, :] = full_row(0)
        vecs[0, 1:2, :] = full_row(1)
        vecs[0, 2:3, :] = gain * (1.0 + full_row(2))
        vecs[0, 3:4, :] = gain * (1.0 + full_row(3))
        vecs[0, 4:8, :] = jnp.broadcast_to(full_row(4), (4, D))
        vec_copy.start()

    @pl.when(away)
    def _():
        vec_copy.wait_recv()

    def norm_rows(src, row, count, dst_at, slot):
        step = 16

        @pl.loop(0, count // step, unroll=True)
        def _(i):
            at = pl.multiple_of(i * step, step)
            v = src[pl.ds(at, step), :].astype(F32)
            inv = lax.rsqrt(jnp.mean(v * v, axis=-1, keepdims=True) + token_eps)
            normed[pl.ds(dst_at + at, step), :] = (
                v * inv * vecs[slot, 2 + row : 3 + row, :] + vecs[slot, row : row + 1, :]
            ).astype(BF)

    def head_norm(x):
        square = x * x
        high = square.astype(BF)
        low = (square - high.astype(F32)).astype(BF)
        mean = jnp.dot(jnp.concatenate([high, low], axis=1), grp[...], preferred_element_type=F32)
        return x * lax.rsqrt(mean + token_eps)

    def turn(y, cos, sin):
        lane = lax.broadcasted_iota(jnp.int32, y.shape, 1)
        front = lax.rem(lane, head_width // 2) < head_width // 4
        other = jnp.where(
            front,
            pltpu.roll(y, HW - head_width // 4, axis=1),
            pltpu.roll(y, head_width // 4, axis=1),
        )
        return y * cos + other * sin

    def turns_of(k):
        at = pl.ds(pl.multiple_of(peers[k] * R, R), R)
        return turns[0, at, :], turns[1, at, :]

    def project(first, count, plain):
        x = normed[first : first + count, :]
        kk = head_norm(jnp.dot(x, wkv[0], preferred_element_type=F32))
        for h in range(n_head):
            y = kk[:, h * HW : (h + 1) * HW] * k_gain
            if plain:
                kvl[h, first : first + plain, 0:HW] = y[:plain].astype(BF)
            for at in range(plain, count, R):
                kvl[h, first + at : first + at + R, 0:HW] = turn(
                    y[at : at + R], *turns_of((first + at - C) // R)
                ).astype(BF)
        vv = jnp.dot(x, wkv[1], preferred_element_type=F32).astype(BF)
        for h in range(n_head):
            kvl[h, first : first + count, HW:] = vv[:, h * VW : (h + 1) * VW]

    def project_queries(first, last):
        x = normed[C + first * R : C + last * R, :]
        qq = head_norm(jnp.dot(x, wq[...], preferred_element_type=F32))
        for k in range(first, last):
            for h in range(n_head):
                y = qq[(k - first) * R : (k - first + 1) * R, h * HW : (h + 1) * HW] * q_gain
                qown[h, k * R : (k + 1) * R, :] = (
                    turn(y, *turns_of(k)) * (head_width ** -0.5)
                ).astype(BF)

    def split_maps(q, at):
        lane = lax.broadcasted_iota(jnp.int32, q.shape, 1)
        for m in range(2):
            qm[m, at : at + ROWS, :] = jnp.where(lane // head_width == m, q, jnp.zeros_like(q))

    def kv_copy(j, head, at, count):
        there = base + lax.rem(s - base + j, H)
        i = 2 * j + a
        return remote(kvl.at[head, pl.ds(C + at, count)], kvr.at[block, pl.ds(at, count)], s_kv,
                      r_kv.at[i], {"dp": d_ix - core + head, "sp": there})

    def send_block(at, count):
        for j in range(1, H):
            for head in range(2):
                kv_copy(j, head, at, count).start()
        kv_copy(0, 1 - core, at, count).start()

    def ctx_copy(there, head):
        at = pl.ds(pl.multiple_of(s * C, C), C)
        return remote(kvl.at[head, pl.ds(0, C)], kvc.at[at], s_ctx, r_ctx,
                      {"dp": d_ix - core + head, "sp": there})

    def send_ctx():
        @pl.when(home)
        def _():
            for j in range(1, H):
                for head in range(2):
                    ctx_copy(base + lax.rem(s - base + j, H), head).start()
            ctx_copy(s, 1 - core).start()
            kvc[pl.ds(pl.multiple_of(s * C, C), C), :] = kvl[core, 0:C, :]

        @pl.when(away)
        def _():
            for j in range(H):
                for head in range(2):
                    ctx_copy(lax.rem(s_opp + j, H) + H - base, head).start()

    l_ctx.wait()
    norm_rows(ctx, 1, C, 0, a)
    drain(wkv, loc.at[5])
    drain(turns, loc.at[6])

    @pl.when(home)
    def _():
        norm_rows(lat.at[0], 0, R, C, 0)
        project(0, C + R, C)
        send_block(0, R)
        send_ctx()
        drain(lat.at[1], r_lat.at[4])
        norm_rows(lat.at[1], 0, R, C + R, 0)
        norm_rows(lat.at[2], 0, R, C + 2 * R, 0)
        project(C + R, 2 * R, 0)
        send_block(R, 2 * R)

    @pl.when(jnp.logical_and(home, core == 0))
    def _():
        start(*near_leads)

    @pl.when(away)
    def _():
        project(0, C, C)
        send_ctx()
        pass_on(2)
        pass_on(3)
        start(*lead_f, *near_rests)
        norm_rows(lat.at[0], 0, R, C, 1)
        drain(lat.at[1], r_lat.at[4])
        norm_rows(lat.at[1], 0, R, C + R, 1)
        norm_rows(lat.at[2], 0, R, C + 2 * R, 1)
        project(C, 3 * R, 0)
        send_block(0, 3 * R)

    l_wq.wait()
    project_queries(0, 3)
    drain(lat.at[3], r_lat.at[5])
    norm_rows(lat.at[3], 0, R, C + 3 * R, a)
    project(C + 3 * R, R, 0)
    send_block(3 * R, R)

    project_queries(3, 4)
    q_copy = remote(qown.at[1 - core], qin, s_q, r_q, {"dp": partner})
    q_copy.start()
    split_maps(qown[core], 0)

    QB = 4 * R
    lift = lift_r[core]

    def attend(block, at, keys, start_row, count, first, plus):
        k = block[at : at + keys, 0:HW]
        v = block[at : at + keys, HW:]
        vx = jnp.concatenate([v, jnp.ones_like(v)], axis=1)
        for m in range(2):
            for b in range(count // QB):
                rows = slice(start_row + b * QB, start_row + (b + 1) * QB)
                sc = lax.dot_general(
                    qm[m, rows, :], k, (((1,), (1,)), ((), ())), preferred_element_type=F32
                )
                if plus is not None:
                    sc = sc + plus
                p = jnp.exp(sc).astype(BF)
                add = jnp.dot(p, vx, preferred_element_type=F32)
                if first:
                    acc[m, rows, :] = add
                else:
                    acc[m, rows, :] += add

    @pl.when(home)
    def _():
        share_first()
        start(*lead_f)

    @pl.when(jnp.logical_and(home, core == 0))
    def _():
        start(*near_rests)

    attend(kvl.at[core], C, ROWS, 0, ROWS, True, None)

    @pl.when(jnp.logical_and(home, core == 1))
    def _():
        drain(wo.at[3, pl.ds(0, 2 * SH)], r_wo.at[6])
        start(*near_rests)

    q_copy.wait_recv()
    split_maps(qin[...], ROWS)
    attend(kvl.at[core], C, ROWS, ROWS, ROWS, True, None)

    @pl.when(home)
    def _():
        share_second()

    pass_rest()

    @pl.when(jnp.logical_or(away, core == 0))
    def _():
        drain(wo.at[3, pl.ds(0, 2 * SH)], r_wo.at[6])

    share_far()

    def attend_block(slot, i):
        drain(kvr.at[slot], r_kv.at[i])
        attend(kvr.at[slot], 0, ROWS, 0, 2 * ROWS, False, None)

    for j in range(1, H):
        attend_block(base + lax.rem(s - base + H - j, H), 2 * j)

    @pl.when(home)
    def _():
        drain(kvc.at[pl.ds(0, (n_sp - 1) * C)], r_ctx)

    @pl.when(away)
    def _():
        drain(kvc, r_ctx)

    attend(kvc, 0, n_sp * C, 0, 2 * ROWS, False, lift)
    attend_block(other_block, 1 - a)
    for j in range(1, H):
        attend_block(lax.rem(base + lax.rem(s - base + H - j, H) + H, n_sp), 2 * j + 1)

    @pl.when(away)
    def _():
        drain(mod_full.at[0:3], r_mt)

    def ho_copy(q, k):
        lanes = pl.ds(pl.multiple_of(k * n_head * VW + core * VW, VW), VW)
        return remote(mine.at[q, pl.ds(k * R, R)], ho.at[:, lanes], s_ho, r_ho.at[k],
                      {"dp": d_work, "sp": block + q * (other_block - block), "tp": peers[k]})

    for q in (1 - a, a):
        rows = pl.ds(pl.multiple_of(q * ROWS, ROWS), ROWS)
        a0 = acc[0, rows, :]
        a1 = acc[1, rows, :]
        mixed = a0[:, :VW] / a0[:, VW:] - lam_r[core] * (a1[:, :VW] / a1[:, VW:])
        inv = lax.rsqrt(jnp.mean(mixed * mixed, axis=-1, keepdims=True) + head_eps)
        mine[q, :, :] = (mixed * inv * v_gain * head_factor).astype(BF)
        for k in (3, 2, 1):
            ho_copy(q, k).start()
        if q is not a:
            ho_copy(q, 0).start()

    @pl.when(away)
    def _():
        ho_copy(a, 0).start()

    for h in range(2):
        @pl.when(jnp.logical_and(home, core == h))
        def _():
            ho[:, h * VW : (h + 1) * VW] = mine[0, 0:R, :]

    drain(wo.at[1, pl.ds(0, 2 * (QUART - 2 * SH))], r_wo.at[5])
    for k in range(1, 3):
        drain(wo.at[k, pl.ds(0, 2 * SH)], r_wz.at[k - 1])
        dd_copy(k, 0, HALF).start()
    for q in range(2):
        dd_copy(3, q * QUART + (QUART - SH) * e, SH).start()
    for q in range(2):
        rest_f[q].wait_recv()
        dd_copy(3, q * QUART + SH, QUART - 2 * SH).start()
    drain(wo.at[3, pl.ds(0, 2 * SH)], r_wz.at[2])
    for q in range(2):
        dd_copy(3, q * QUART + (QUART - SH) * (1 - e), SH).start()

    def arrived(k):
        drain(wo.at[k, pl.ds(0, HALF)], r_dd.at[k - 1])
        drain(mine.at[0, pl.ds(0, 2 * R)], r_ho.at[k])

    KW = n_head * VW

    @pl.when(away)
    def _():
        vecs[0, 4:8, :] = jnp.broadcast_to(full_row(4), (4, D))

    arrived(1)
    arrived(2)
    partial[...] = jnp.dot(
        ho[:, KW : 3 * KW], wo[1:3].reshape(-1, D), preferred_element_type=F32
    )
    arrived(3)

    @pl.when(home)
    def _():
        drain(mine.at[0, pl.ds(0, R)], r_ho.at[0])

    @pl.when(away)
    def _():
        drain(mine.at[0, pl.ds(0, 2 * R)], r_ho.at[0])

    late = jnp.dot(ho[:, 0:KW], wo[0], preferred_element_type=F32)
    late += jnp.dot(ho[:, 3 * KW :], wo[3], preferred_element_type=F32)
    mixture = vecs[0, 4:5, :] * (partial[...] + late)

    @pl.when(home)
    def _():
        out_r[...] = (lat[0].astype(F32) + mixture).astype(BF)

    @pl.when(away)
    def _():
        out_r[...] = (own[...].astype(F32) + mixture).astype(BF)

    def sent(ref, sem):
        remote(ref, ref, sem, sem, {"dp": partner}).wait_send()

    sent(mod_in, s_mod)
    sent(mod_full.at[0:3], s_mt)
    sent(lat.at[0:3], s_lat)
    sent(kvr.at[0 : n_sp - 1], s_kv)
    sent(wo.at[0:3, pl.ds(0, 2 * (QUART - SH))], s_wo)
    sent(wo.at[0:3, pl.ds(0, 2 * SH)], s_wz)
    sent(wo.at[0:3, pl.ds(0, HALF)], s_dd)
    q_copy.wait_send()

    @pl.when(home)
    def _():
        vec_copy.wait_send()
        sent(kvc.at[pl.ds(0, (n_sp - 1) * C)], s_ctx)
        sent(qm.at[0, pl.ds(0, 7 * R)], s_ho)

    @pl.when(away)
    def _():
        sent(own, s_swap)
        sent(kvc, s_ctx)
        sent(mine, s_ho)


def on_device(n_sp, n_tp, n_dp, *args):
    (
        latent, context, cond, context_cond, norm_gain, mod_shift, mod_scale, mod_gate,
        w_query, w_key, w_value, query_gain, key_gain, mix_lambda, context_lift, value_gain, w_out,
    ) = args
    R, D = latent.shape
    C = context.shape[0]
    head_width = query_gain.shape[0]
    cos, sin = rope_tables(R * n_sp * n_tp, head_width)
    QW, VWALL = w_query.shape[1], w_value.shape[1]
    heads = mix_lambda.shape[0]
    ROWS = R * n_tp
    HW = 2 * head_width
    KV = (QW + VWALL) // heads
    MC = mod_shift.shape[1]
    vm = pl.BlockSpec(memory_space=pltpu.VMEM)
    anywhere = pl.BlockSpec(memory_space=pl.ANY)
    smem = pl.BlockSpec(memory_space=pltpu.SMEM)
    dma = pltpu.SemaphoreType.DMA
    update = pl.pallas_call(
        functools.partial(kernel, n_sp, n_tp, n_dp, head_width),
        out_shape=pltpu.VMEM((R, D), BF),
        in_specs=[anywhere] * 14 + [smem, smem]
        + [anywhere] * 3,
        out_specs=vm,
        scratch_shapes=[
            pltpu.VMEM(cond.shape, BF),
            pltpu.VMEM(context_cond.shape, BF),
            pltpu.VMEM(norm_gain.shape, F32),
            pltpu.VMEM(query_gain.shape, F32),
            pltpu.VMEM(key_gain.shape, F32),
            pltpu.VMEM(value_gain.shape, F32),
            pltpu.VMEM((R, D), BF),
            pltpu.VMEM((4, R, D), BF),
            pltpu.VMEM((C, D), BF),
            pltpu.VMEM((3,) + mod_shift.shape, BF),
            pltpu.VMEM(w_query.shape, BF),
            pltpu.VMEM((2,) + w_key.shape, BF),
            pltpu.VMEM((4,) + w_out.shape, BF),
            pltpu.VMEM((2, ROWS, HW), F32),
            pltpu.VMEM((8, mod_shift.shape[0]), F32),
            pltpu.VMEM((8, MC), F32),
            pltpu.VMEM((n_sp - 1, 8, MC), F32),
            pltpu.VMEM((8, MC), F32),
            pltpu.VMEM((n_tp, 8, MC), F32),
            pltpu.VMEM((2, 8, D), F32),
            pltpu.VMEM((C + ROWS, D), BF),
            pltpu.VMEM((heads, ROWS, HW), BF),
            pltpu.VMEM((ROWS, HW), BF),
            pltpu.VMEM((2, 2 * ROWS, HW), BF),
            pltpu.VMEM((heads, C + ROWS, KV), BF),
            pltpu.VMEM((n_sp, ROWS, KV), BF),
            pltpu.VMEM((n_sp * C, KV), BF),
            pltpu.VMEM((2, 2 * ROWS, 2 * VWALL // heads), F32),
            pltpu.VMEM((2, ROWS, VWALL // heads), BF),
            pltpu.VMEM((R, n_tp * VWALL), BF),
            pltpu.VMEM((2 * QW, QW), BF),
            pltpu.VMEM((R, D), F32),
            dma((13,)),
            dma(()), dma((4,)),
            dma(()), dma((6,)),
            dma(()), dma(()),
            dma(()), dma(()),
            dma(()), dma(()),
            dma(()), dma((n_sp,)),
            dma(()), dma(()),
            dma(()), dma(()),
            dma(()), dma((9,)),
            dma(()), dma((3,)),
            dma(()), dma((3,)),
            dma(()), dma((4,)),
        ],
        compiler_params=pltpu.CompilerParams(
            collective_id=0, has_side_effects=True, vmem_limit_bytes=66_100_000
        ),
        name="block",
    )(
        latent, context, cond, context_cond, norm_gain, mod_shift, mod_scale,
        mod_gate, w_query, w_key, w_value, query_gain, key_gain, value_gain, mix_lambda, context_lift, w_out,
        jnp.asarray(cos), jnp.asarray(sin),
    )
    return update


def solution(mesh):
    placed = (
        P(("dp", "sp", "tp"), None),
        P(("dp", "sp"), None),
        P(("dp", "sp")),
        P("sp"),
        P(),
        P("sp", "tp"),
        P("sp", "tp"),
        P("sp", "tp"),
        P(None, "tp"),
        P(None, "tp"),
        P(None, "tp"),
        P(),
        P(),
        P("tp"),
        P("tp"),
        P(),
        P("tp", None),
    )
    sizes = mesh.shape
    return jax.shard_map(
        functools.partial(on_device, sizes["sp"], sizes["tp"], sizes["dp"]),
        mesh=mesh,
        in_specs=placed,
        out_specs=P(("dp", "sp", "tp"), None),
        check_vma=False,
    )
```

```python
import functools

import jax
import jax.numpy as jnp
import numpy as np
from jax import lax
from jax.experimental import pallas as pl
from jax.experimental.pallas import tpu as pltpu
from jax.sharding import PartitionSpec as P

GRID = 64
token_eps = 0.01
head_eps = 0.001
rope_base = 10000.0
head_factor = 0.8
MESH = pl.DeviceIdType.MESH
BF = jnp.bfloat16
F32 = jnp.float32


def rope_tables(length, width):
    quarter = width // 4
    inverse = (rope_base ** (-np.arange(quarter, dtype=np.float64) / quarter)).astype(np.float32)
    pos = np.arange(length)
    row = (pos // GRID).astype(np.float32)[:, None] * inverse
    col = (pos % GRID).astype(np.float32)[:, None] * inverse
    cos = np.concatenate([np.cos(row), np.cos(row), np.cos(col), np.cos(col)], axis=1)
    sin = np.concatenate([-np.sin(row), np.sin(row), -np.sin(col), np.sin(col)], axis=1)
    return np.tile(cos, (1, 2)).astype(np.float32), np.tile(sin, (1, 2)).astype(np.float32)


def kernel(n_sp, n_tp, n_dp, head_width, *refs):
    (
        lat_h, ctx_h, cond_h, cctx_h, gain_h, ms_h, msc_h, mg_h, wq_h, wk_h, wv_h,
        qg_h, kg_h, vg_h, lam_r, lift_r, wo_h, cos_h, sin_h,
        out_r,
        cond_r, cctx_r, gain_r, qg_r, kg_r, vg_r,
        own, lat, ctx, mw, wq, wkv, wo, turns,
        act, part, mod_in, summed, mod_full, vecs, normed, qown, qin, qm, kvl, kvr, kvc, acc,
        mine, ho, grp, partial,
        loc, s_swap, r_swap, s_lat, r_lat, s_mod, r_mod, s_mt, r_mt, s_vec, r_vec, s_kv, r_kv,
        s_ctx, r_ctx, s_q, r_q, s_wo, r_wo, s_wz, r_wz, s_dd, r_dd, s_ho, r_ho,
    ) = refs
    s = lax.axis_index("sp")
    t = lax.axis_index("tp")
    d_ix = lax.axis_index("dp")
    core = lax.rem(d_ix, 2)
    partner = d_ix + 1 - 2 * core
    t_odd = lax.rem(t, 2)
    nbr1 = t + 1 - 2 * t_odd
    nbr2 = lax.rem(t + 2, 4)
    nbr3 = lax.rem(nbr1 + 2, 4)
    peers = (t, nbr1, nbr2, nbr3)
    H = n_sp // 2
    half = s // H
    base = half * H
    s_opp = lax.rem(s + H, n_sp)
    home = core == half
    away = jnp.not_equal(core, half)
    a = lax.rem(core + half, 2)
    block = s + a * (s_opp - s)
    other_block = s_opp + a * (s - s_opp)
    d_work = d_ix - core + half
    e = lax.rem(s, 2)
    level = s + 1 - 2 * e
    R, D = own.shape
    PR = R // 4
    C = ctx.shape[0]
    QW = wq.shape[1]
    n_head = QW // (2 * head_width)
    HW = 2 * head_width
    VW = wkv.shape[2] // n_head
    ROWS = 4 * R

    bar = pltpu.get_barrier_semaphore()
    greeted = [{"tp": peers[k]} for k in range(1, 4)] + [{"dp": partner}]
    for k in range(1, n_sp):
        there = lax.rem(s + k, n_sp)
        greeted += [{"sp": there}, {"dp": partner, "sp": there}]
    for where in greeted:
        pl.semaphore_signal(bar, inc=1, device_id=where, device_id_type=MESH)

    def local(i, src, dst):
        c = pltpu.make_async_copy(src, dst, loc.at[i])
        c.start()
        return c

    def remote(src, dst, ss, rs, where):
        return pltpu.make_async_remote_copy(
            src_ref=src, dst_ref=dst, send_sem=ss, recv_sem=rs, device_id=where, device_id_type=MESH
        )

    def drain(ref, sem):
        remote(ref, ref, sem, sem, {"dp": partner}).wait_recv()

    @pl.when(home)
    def _():
        local(0, lat_h, lat.at[0])

    @pl.when(away)
    def _():
        local(0, lat_h, own)

    l_one = [local(1, cond_h, cond_r), local(2, cctx_h, cctx_r)]
    for j, h in enumerate((ms_h, msc_h, mg_h)):
        local(3, h, mw.at[j])

    rows = []
    for row, ref in ((0, cond_r), (1, cctx_r)):
        l_one[row].wait()
        v = ref[...].astype(F32).reshape(1, -1)
        rows.append(v / (1.0 + jnp.exp(-v)))
    acts = jnp.concatenate(rows + [jnp.zeros((6, rows[0].shape[1]), F32)], axis=0).astype(BF)
    drain(mw, loc.at[3])
    l_wo = local(12, wo_h, wo.at[0])
    res = [jnp.dot(acts, mw[j], preferred_element_type=F32) for j in range(3)]
    part[...] = jnp.concatenate([r[0:2] for r in res] + [res[2][6:8]], axis=0)

    drain(own, loc.at[0])
    pl.semaphore_wait(bar, len(greeted))

    def mod_copy(k):
        return remote(part, mod_in.at[k - 1], s_mod, r_mod, {"sp": lax.rem(s + k, n_sp)})

    def piece(j):
        return pl.ds(j * PR, PR)

    def swap(j):
        return remote(own.at[piece(j)], lat.at[0, piece(j)], s_swap, r_swap.at[j],
                      {"dp": partner, "sp": s_opp})

    def along_x(j):
        return remote(lat.at[0, piece(j)], lat.at[1, piece(j)], s_lat, r_lat.at[j if j < 2 else 4],
                      {"tp": nbr1})

    def along_y(j):
        return remote(lat.at[0, piece(j)], lat.at[2, piece(j)], s_lat, r_lat.at[j if j > 1 else 4],
                      {"tp": nbr2})

    def onward(j):
        slot, where = (1, nbr2) if j < 2 else (2, nbr1)
        return remote(lat.at[slot, piece(j)], lat.at[3, piece(j)], s_lat, r_lat.at[5], {"tp": where})

    def pass_on(j):
        (along_x(j) if j < 2 else along_y(j)).wait_recv()
        onward(j).start()

    HALF = wo.shape[1] // 2
    QUART = HALF // 2
    SH = QUART // 4

    def wo_rows(at, count):
        return pl.ds(pl.multiple_of(core * HALF + at, SH), count)

    def wo_copy(i, src_slot, dst_slot, at, count, where):
        rows = wo_rows(at, count)
        return remote(wo.at[src_slot, rows], wo.at[dst_slot, rows], s_wo, r_wo.at[i], {"tp": where})

    def wz_copy(k, q):
        rows = wo_rows(q * QUART + (QUART - SH) * e, SH)
        return remote(wo.at[k, rows], wo.at[k, rows], s_wz, r_wz.at[k - 1], {"sp": level})

    def dd_copy(k, at, count):
        rows = wo_rows(at, count)
        return remote(wo.at[k, rows], wo.at[k, rows], s_dd, r_dd.at[k - 1], {"dp": partner})

    def lead(i, src, dst, q, where):
        return wo_copy(i, src, dst, q * QUART + (QUART - SH) * e, SH, where)

    def rest(i, src, dst, q, where):
        return wo_copy(i, src, dst, q * QUART + SH, QUART - 2 * SH, where)

    lead_x = [lead(0, 0, 1, 0, nbr1), lead(2, 0, 1, 1, nbr1)]
    lead_y = [lead(2, 0, 2, 0, nbr2), lead(1, 0, 2, 1, nbr2)]
    lead_f = [lead(6, 1, 3, 0, nbr2), lead(6, 2, 3, 1, nbr1)]
    rest_x = [rest(3, 0, 1, 0, nbr1), rest(5, 0, 1, 1, nbr1)]
    rest_y = [rest(5, 0, 2, 0, nbr2), rest(4, 0, 2, 1, nbr2)]
    rest_f = [rest(7, 1, 3, 0, nbr2), rest(8, 2, 3, 1, nbr1)]

    def start(*copies):
        for c in copies:
            c.start()

    def share_first():
        lead_x[0].wait_recv()
        wz_copy(1, 0).start()
        lead_y[1].wait_recv()
        wz_copy(2, 1).start()

    def share_second():
        drain(wo.at[1, pl.ds(0, 2 * SH)], r_wo.at[2])
        wz_copy(1, 1).start()
        wz_copy(2, 0).start()

    def share_far():
        wz_copy(3, 0).start()
        wz_copy(3, 1).start()

    def pass_rest():
        rest_x[0].wait_recv()
        rest_f[0].start()
        rest_y[1].wait_recv()
        rest_f[1].start()

    near_leads = (lead_x[0], lead_y[1], lead_x[1], lead_y[0])
    near_rests = (rest_x[0], rest_y[1], rest_x[1], rest_y[0])

    for k in range(1, n_sp):
        mod_copy(k).start()

    @pl.when(home)
    def _():
        for j in range(4):
            along_x(j).start()
            along_y((j + 2) % 4).start()

    @pl.when(away)
    def _():
        for j in range(4):
            swap(j).start()

    l_ctx = local(4, ctx_h, ctx)
    local(5, wk_h, wkv.at[0])
    local(5, wv_h, wkv.at[1])
    at_turns = pl.ds(pl.multiple_of(block * ROWS, ROWS), ROWS)
    local(6, cos_h.at[at_turns], turns.at[0])
    local(6, sin_h.at[at_turns], turns.at[1])
    l_small = [
        local(7 + j, src, dst)
        for j, (src, dst) in enumerate(((gain_h, gain_r), (qg_h, qg_r), (kg_h, kg_r), (vg_h, vg_r)))
    ]
    l_wq = local(11, wq_h, wq)

    l_wo.wait()

    @pl.when(away)
    def _():
        start(*near_leads)

    group = (
        lax.rem(lax.broadcasted_iota(jnp.int32, (2 * QW, QW), 0), QW) // head_width
        == lax.broadcasted_iota(jnp.int32, (2 * QW, QW), 1) // head_width
    )
    grp[...] = jnp.where(group, 1.0 / head_width, 0.0).astype(BF)
    for c in l_small:
        c.wait()
    gain = gain_r[...].reshape(1, -1)
    q_gain = qg_r[...].reshape(1, -1)
    q_gain = jnp.concatenate([q_gain, q_gain], axis=1)
    k_gain = kg_r[...].reshape(1, -1)
    k_gain = jnp.concatenate([k_gain, k_gain], axis=1)
    v_gain = vg_r[...].reshape(1, -1)

    drain(mod_in, r_mod)
    total = part[...]
    for k in range(n_sp - 1):
        total = total + mod_in[k]
    summed[...] = total
    mod_full[t] = total

    def mt_copy(k):
        return remote(summed, mod_full.at[t], s_mt, r_mt, {"tp": peers[k]})

    for k in range(1, 4):
        mt_copy(k).start()

    @pl.when(home)
    def _():
        for j in (0, 2, 1, 3):
            pass_on(j)

    @pl.when(jnp.logical_and(home, core == 1))
    def _():
        start(*near_leads)

    @pl.when(away)
    def _():
        @pl.when(core == 1)
        def _():
            share_first()
            share_second()

        for j in range(4):
            swap(j).wait_recv()
            along_y(j).start()
            along_x(j).start()
            if j == 3:
                @pl.when(core == 0)
                def _():
                    share_first()
                    share_second()

        pass_on(0)
        pass_on(1)

    def full_row(j):
        return jnp.concatenate([mod_full[q, j : j + 1, :] for q in range(n_tp)], axis=1)

    vec_copy = remote(vecs.at[0], vecs.at[1], s_vec, r_vec, {"dp": partner})

    @pl.when(home)
    def _():
        drain(mod_full.at[0:3], r_mt)
        vecs[0, 0:1, :] = full_row(0)
        vecs[0, 1:2, :] = full_row(1)
        vecs[0, 2:3, :] = gain * (1.0 + full_row(2))
        vecs[0, 3:4, :] = gain * (1.0 + full_row(3))
        vecs[0, 4:8, :] = jnp.broadcast_to(full_row(4), (4, D))
        vec_copy.start()

    @pl.when(away)
    def _():
        vec_copy.wait_recv()

    def norm_rows(src, row, count, dst_at, slot):
        step = 16

        @pl.loop(0, count // step, unroll=True)
        def _(i):
            at = pl.multiple_of(i * step, step)
            v = src[pl.ds(at, step), :].astype(F32)
            inv = lax.rsqrt(jnp.mean(v * v, axis=-1, keepdims=True) + token_eps)
            normed[pl.ds(dst_at + at, step), :] = (
                v * inv * vecs[slot, 2 + row : 3 + row, :] + vecs[slot, row : row + 1, :]
            ).astype(BF)

    def head_norm(x):
        square = x * x
        high = square.astype(BF)
        low = (square - high.astype(F32)).astype(BF)
        mean = jnp.dot(jnp.concatenate([high, low], axis=1), grp[...], preferred_element_type=F32)
        return x * lax.rsqrt(mean + token_eps)

    def turn(y, cos, sin):
        lane = lax.broadcasted_iota(jnp.int32, y.shape, 1)
        front = lax.rem(lane, head_width // 2) < head_width // 4
        other = jnp.where(
            front,
            pltpu.roll(y, HW - head_width // 4, axis=1),
            pltpu.roll(y, head_width // 4, axis=1),
        )
        return y * cos + other * sin

    def turns_of(k):
        at = pl.ds(pl.multiple_of(peers[k] * R, R), R)
        return turns[0, at, :], turns[1, at, :]

    def project(first, count, plain):
        x = normed[first : first + count, :]
        kk = head_norm(jnp.dot(x, wkv[0], preferred_element_type=F32))
        for h in range(n_head):
            y = kk[:, h * HW : (h + 1) * HW] * k_gain
            if plain:
                kvl[h, first : first + plain, 0:HW] = y[:plain].astype(BF)
            for at in range(plain, count, R):
                kvl[h, first + at : first + at + R, 0:HW] = turn(
                    y[at : at + R], *turns_of((first + at - C) // R)
                ).astype(BF)
        vv = jnp.dot(x, wkv[1], preferred_element_type=F32).astype(BF)
        for h in range(n_head):
            kvl[h, first : first + count, HW:] = vv[:, h * VW : (h + 1) * VW]

    def project_queries(first, last):
        x = normed[C + first * R : C + last * R, :]
        qq = head_norm(jnp.dot(x, wq[...], preferred_element_type=F32))
        for k in range(first, last):
            for h in range(n_head):
                y = qq[(k - first) * R : (k - first + 1) * R, h * HW : (h + 1) * HW] * q_gain
                qown[h, k * R : (k + 1) * R, :] = (
                    turn(y, *turns_of(k)) * (head_width ** -0.5)
                ).astype(BF)

    def split_maps(q, at):
        lane = lax.broadcasted_iota(jnp.int32, q.shape, 1)
        for m in range(2):
            qm[m, at : at + ROWS, :] = jnp.where(lane // head_width == m, q, jnp.zeros_like(q))

    def kv_copy(j, head, at, count):
        there = base + lax.rem(s - base + j, H)
        i = 2 * j + a
        return remote(kvl.at[head, pl.ds(C + at, count)], kvr.at[block, pl.ds(at, count)], s_kv,
                      r_kv.at[i], {"dp": d_ix - core + head, "sp": there})

    def send_block(at, count):
        for j in range(1, H):
            for head in range(2):
                kv_copy(j, head, at, count).start()
        kv_copy(0, 1 - core, at, count).start()

    def ctx_copy(there, head):
        at = pl.ds(pl.multiple_of(s * C, C), C)
        return remote(kvl.at[head, pl.ds(0, C)], kvc.at[at], s_ctx, r_ctx,
                      {"dp": d_ix - core + head, "sp": there})

    def send_ctx():
        @pl.when(home)
        def _():
            for j in range(1, H):
                for head in range(2):
                    ctx_copy(base + lax.rem(s - base + j, H), head).start()
            ctx_copy(s, 1 - core).start()
            kvc[pl.ds(pl.multiple_of(s * C, C), C), :] = kvl[core, 0:C, :]

        @pl.when(away)
        def _():
            for j in range(H):
                for head in range(2):
                    ctx_copy(lax.rem(s_opp + j, H) + H - base, head).start()

    l_ctx.wait()
    norm_rows(ctx, 1, C, 0, a)
    drain(wkv, loc.at[5])
    drain(turns, loc.at[6])

    @pl.when(home)
    def _():
        norm_rows(lat.at[0], 0, R, C, 0)
        project(0, C + R, C)
        send_block(0, R)
        send_ctx()
        drain(lat.at[1], r_lat.at[4])
        norm_rows(lat.at[1], 0, R, C + R, 0)
        norm_rows(lat.at[2], 0, R, C + 2 * R, 0)
        project(C + R, 2 * R, 0)
        send_block(R, 2 * R)

    @pl.when(jnp.logical_and(home, core == 0))
    def _():
        start(*near_leads)

    @pl.when(away)
    def _():
        project(0, C, C)
        send_ctx()
        pass_on(2)
        pass_on(3)
        start(*lead_f, *near_rests)
        norm_rows(lat.at[0], 0, R, C, 1)
        drain(lat.at[1], r_lat.at[4])
        norm_rows(lat.at[1], 0, R, C + R, 1)
        norm_rows(lat.at[2], 0, R, C + 2 * R, 1)
        project(C, 3 * R, 0)
        send_block(0, 3 * R)

    l_wq.wait()
    project_queries(0, 3)
    drain(lat.at[3], r_lat.at[5])
    norm_rows(lat.at[3], 0, R, C + 3 * R, a)
    project(C + 3 * R, R, 0)
    send_block(3 * R, R)

    @pl.when(jnp.logical_and(home, core == 0))
    def _():
        start(rest_x[0], rest_y[1])


    project_queries(3, 4)
    q_copy = remote(qown.at[1 - core], qin, s_q, r_q, {"dp": partner})
    q_copy.start()
    split_maps(qown[core], 0)

    QB = 4 * R
    lift = lift_r[core]

    def attend(block, at, keys, start_row, count, first, plus):
        k = block[at : at + keys, 0:HW]
        v = block[at : at + keys, HW:]
        vx = jnp.concatenate([v, jnp.ones_like(v)], axis=1)
        for m in range(2):
            for b in range(count // QB):
                rows = slice(start_row + b * QB, start_row + (b + 1) * QB)
                sc = lax.dot_general(
                    qm[m, rows, :], k, (((1,), (1,)), ((), ())), preferred_element_type=F32
                )
                if plus is not None:
                    sc = sc + plus
                p = jnp.exp(sc).astype(BF)
                add = jnp.dot(p, vx, preferred_element_type=F32)
                if first:
                    acc[m, rows, :] = add
                else:
                    acc[m, rows, :] += add

    @pl.when(home)
    def _():
        share_first()
        start(*lead_f)

    @pl.when(jnp.logical_and(home, core == 0))
    def _():
        start(rest_x[1], rest_y[0])

    attend(kvl.at[core], C, ROWS, 0, ROWS, True, None)

    @pl.when(jnp.logical_and(home, core == 1))
    def _():
        drain(wo.at[3, pl.ds(0, 2 * SH)], r_wo.at[6])
        start(*near_rests)

    q_copy.wait_recv()
    split_maps(qin[...], ROWS)
    attend(kvl.at[core], C, ROWS, ROWS, ROWS, True, None)

    @pl.when(home)
    def _():
        share_second()

    pass_rest()

    @pl.when(jnp.logical_or(away, core == 0))
    def _():
        drain(wo.at[3, pl.ds(0, 2 * SH)], r_wo.at[6])

    share_far()

    def attend_block(slot, i):
        drain(kvr.at[slot], r_kv.at[i])
        attend(kvr.at[slot], 0, ROWS, 0, 2 * ROWS, False, None)

    for j in range(1, H):
        attend_block(base + lax.rem(s - base + H - j, H), 2 * j)

    @pl.when(home)
    def _():
        drain(kvc.at[pl.ds(0, (n_sp - 1) * C)], r_ctx)

    @pl.when(away)
    def _():
        drain(kvc, r_ctx)

    attend(kvc, 0, n_sp * C, 0, 2 * ROWS, False, lift)
    attend_block(other_block, 1 - a)
    for j in range(1, H):
        attend_block(lax.rem(base + lax.rem(s - base + H - j, H) + H, n_sp), 2 * j + 1)

    @pl.when(away)
    def _():
        drain(mod_full.at[0:3], r_mt)

    def ho_copy(q, k):
        lanes = pl.ds(pl.multiple_of(k * n_head * VW + core * VW, VW), VW)
        return remote(mine.at[q, pl.ds(k * R, R)], ho.at[:, lanes], s_ho, r_ho.at[k],
                      {"dp": d_work, "sp": block + q * (other_block - block), "tp": peers[k]})

    for q in (1 - a, a):
        rows = pl.ds(pl.multiple_of(q * ROWS, ROWS), ROWS)
        a0 = acc[0, rows, :]
        a1 = acc[1, rows, :]
        mixed = a0[:, :VW] / a0[:, VW:] - lam_r[core] * (a1[:, :VW] / a1[:, VW:])
        inv = lax.rsqrt(jnp.mean(mixed * mixed, axis=-1, keepdims=True) + head_eps)
        mine[q, :, :] = (mixed * inv * v_gain * head_factor).astype(BF)
        for k in (3, 2, 1):
            ho_copy(q, k).start()
        if q is not a:
            ho_copy(q, 0).start()

    @pl.when(away)
    def _():
        ho_copy(a, 0).start()

    for h in range(2):
        @pl.when(jnp.logical_and(home, core == h))
        def _():
            ho[:, h * VW : (h + 1) * VW] = mine[0, 0:R, :]

    drain(wo.at[1, pl.ds(0, 2 * (QUART - 2 * SH))], r_wo.at[5])
    for k in range(1, 3):
        drain(wo.at[k, pl.ds(0, 2 * SH)], r_wz.at[k - 1])
        dd_copy(k, 0, HALF).start()
    for q in range(2):
        dd_copy(3, q * QUART + (QUART - SH) * e, SH).start()
    for q in range(2):
        rest_f[q].wait_recv()
        dd_copy(3, q * QUART + SH, QUART - 2 * SH).start()
    drain(wo.at[3, pl.ds(0, 2 * SH)], r_wz.at[2])
    for q in range(2):
        dd_copy(3, q * QUART + (QUART - SH) * (1 - e), SH).start()

    def arrived(k):
        drain(wo.at[k, pl.ds(0, HALF)], r_dd.at[k - 1])
        drain(mine.at[0, pl.ds(0, 2 * R)], r_ho.at[k])

    KW = n_head * VW

    @pl.when(away)
    def _():
        vecs[0, 4:8, :] = jnp.broadcast_to(full_row(4), (4, D))

    arrived(1)
    arrived(2)
    partial[...] = jnp.dot(
        ho[:, KW : 3 * KW], wo[1:3].reshape(-1, D), preferred_element_type=F32
    )
    arrived(3)

    @pl.when(home)
    def _():
        drain(mine.at[0, pl.ds(0, R)], r_ho.at[0])

    @pl.when(away)
    def _():
        drain(mine.at[0, pl.ds(0, 2 * R)], r_ho.at[0])

    late = jnp.dot(ho[:, 0:KW], wo[0], preferred_element_type=F32)
    late += jnp.dot(ho[:, 3 * KW :], wo[3], preferred_element_type=F32)
    mixture = vecs[0, 4:5, :] * (partial[...] + late)

    @pl.when(home)
    def _():
        out_r[...] = (lat[0].astype(F32) + mixture).astype(BF)

    @pl.when(away)
    def _():
        out_r[...] = (own[...].astype(F32) + mixture).astype(BF)

    def sent(ref, sem):
        remote(ref, ref, sem, sem, {"dp": partner}).wait_send()

    sent(mod_in, s_mod)
    sent(mod_full.at[0:3], s_mt)
    sent(lat.at[0:3], s_lat)
    sent(kvr.at[0 : n_sp - 1], s_kv)
    sent(wo.at[0:3, pl.ds(0, 2 * (QUART - SH))], s_wo)
    sent(wo.at[0:3, pl.ds(0, 2 * SH)], s_wz)
    sent(wo.at[0:3, pl.ds(0, HALF)], s_dd)
    q_copy.wait_send()

    @pl.when(home)
    def _():
        vec_copy.wait_send()
        sent(kvc.at[pl.ds(0, (n_sp - 1) * C)], s_ctx)
        sent(qm.at[0, pl.ds(0, 7 * R)], s_ho)

    @pl.when(away)
    def _():
        sent(own, s_swap)
        sent(kvc, s_ctx)
        sent(mine, s_ho)


def on_device(n_sp, n_tp, n_dp, *args):
    (
        latent, context, cond, context_cond, norm_gain, mod_shift, mod_scale, mod_gate,
        w_query, w_key, w_value, query_gain, key_gain, mix_lambda, context_lift, value_gain, w_out,
    ) = args
    R, D = latent.shape
    C = context.shape[0]
    head_width = query_gain.shape[0]
    cos, sin = rope_tables(R * n_sp * n_tp, head_width)
    QW, VWALL = w_query.shape[1], w_value.shape[1]
    heads = mix_lambda.shape[0]
    ROWS = R * n_tp
    HW = 2 * head_width
    KV = (QW + VWALL) // heads
    MC = mod_shift.shape[1]
    vm = pl.BlockSpec(memory_space=pltpu.VMEM)
    anywhere = pl.BlockSpec(memory_space=pl.ANY)
    smem = pl.BlockSpec(memory_space=pltpu.SMEM)
    dma = pltpu.SemaphoreType.DMA
    update = pl.pallas_call(
        functools.partial(kernel, n_sp, n_tp, n_dp, head_width),
        out_shape=pltpu.VMEM((R, D), BF),
        in_specs=[anywhere] * 14 + [smem, smem]
        + [anywhere] * 3,
        out_specs=vm,
        scratch_shapes=[
            pltpu.VMEM(cond.shape, BF),
            pltpu.VMEM(context_cond.shape, BF),
            pltpu.VMEM(norm_gain.shape, F32),
            pltpu.VMEM(query_gain.shape, F32),
            pltpu.VMEM(key_gain.shape, F32),
            pltpu.VMEM(value_gain.shape, F32),
            pltpu.VMEM((R, D), BF),
            pltpu.VMEM((4, R, D), BF),
            pltpu.VMEM((C, D), BF),
            pltpu.VMEM((3,) + mod_shift.shape, BF),
            pltpu.VMEM(w_query.shape, BF),
            pltpu.VMEM((2,) + w_key.shape, BF),
            pltpu.VMEM((4,) + w_out.shape, BF),
            pltpu.VMEM((2, ROWS, HW), F32),
            pltpu.VMEM((8, mod_shift.shape[0]), F32),
            pltpu.VMEM((8, MC), F32),
            pltpu.VMEM((n_sp - 1, 8, MC), F32),
            pltpu.VMEM((8, MC), F32),
            pltpu.VMEM((n_tp, 8, MC), F32),
            pltpu.VMEM((2, 8, D), F32),
            pltpu.VMEM((C + ROWS, D), BF),
            pltpu.VMEM((heads, ROWS, HW), BF),
            pltpu.VMEM((ROWS, HW), BF),
            pltpu.VMEM((2, 2 * ROWS, HW), BF),
            pltpu.VMEM((heads, C + ROWS, KV), BF),
            pltpu.VMEM((n_sp, ROWS, KV), BF),
            pltpu.VMEM((n_sp * C, KV), BF),
            pltpu.VMEM((2, 2 * ROWS, 2 * VWALL // heads), F32),
            pltpu.VMEM((2, ROWS, VWALL // heads), BF),
            pltpu.VMEM((R, n_tp * VWALL), BF),
            pltpu.VMEM((2 * QW, QW), BF),
            pltpu.VMEM((R, D), F32),
            dma((13,)),
            dma(()), dma((4,)),
            dma(()), dma((6,)),
            dma(()), dma(()),
            dma(()), dma(()),
            dma(()), dma(()),
            dma(()), dma((n_sp,)),
            dma(()), dma(()),
            dma(()), dma(()),
            dma(()), dma((9,)),
            dma(()), dma((3,)),
            dma(()), dma((3,)),
            dma(()), dma((4,)),
        ],
        compiler_params=pltpu.CompilerParams(
            collective_id=0, has_side_effects=True, vmem_limit_bytes=66_100_000
        ),
        name="block",
    )(
        latent, context, cond, context_cond, norm_gain, mod_shift, mod_scale,
        mod_gate, w_query, w_key, w_value, query_gain, key_gain, value_gain, mix_lambda, context_lift, w_out,
        jnp.asarray(cos), jnp.asarray(sin),
    )
    return update


def solution(mesh):
    placed = (
        P(("dp", "sp", "tp"), None),
        P(("dp", "sp"), None),
        P(("dp", "sp")),
        P("sp"),
        P(),
        P("sp", "tp"),
        P("sp", "tp"),
        P("sp", "tp"),
        P(None, "tp"),
        P(None, "tp"),
        P(None, "tp"),
        P(),
        P(),
        P("tp"),
        P("tp"),
        P(),
        P("tp", None),
    )
    sizes = mesh.shape
    return jax.shard_map(
        functools.partial(on_device, sizes["sp"], sizes["tp"], sizes["dp"]),
        mesh=mesh,
        in_specs=placed,
        out_specs=P(("dp", "sp", "tp"), None),
        check_vma=False,
    )
```
